32 devices in a mesh: grp: 2 (over x), sp: 4 (over z), tp: 4 (over y, core).
Axes of the slice: x: 2, y: 2, z: 4, core: 2. Of those that a mesh axis runs over, the one named last changes fastest.
Arguments:
- prompt_layer_input: bfloat16 [24, 512, 2048], P('grp', 'sp'), parts along dimension 0, may hold values from -10 to 10
- next_token_input: bfloat16 [24, 2048], P('grp'), parts along dimension 0, may hold values from -6 to 6
- value_projection: bfloat16 [2048, 2048], P(None, 'tp'), may hold values from -0.125 to 0.125
- output_gate_matrix: bfloat16 [2048, 2048], P(None, 'tp'), may hold values from -0.125 to 0.125
- key_projection: bfloat16 [2048, 256], replicated, may hold values from -0.0390625 to 0.0390625
- query_projection: bfloat16 [2048, 256], replicated, may hold values from -0.125 to 0.125
- step_projection: bfloat16 [2048, 32], replicated, may hold values from -0.125 to 0.125
- value_filter_taps: bfloat16 [4, 2048], replicated, may hold values from -3 to 3
- key_filter_taps: bfloat16 [4, 256], replicated, may hold values from -3 to 3
- query_filter_taps: bfloat16 [4, 256], replicated, may hold values from -3 to 3
- step_size_bias: float32 [32], replicated, may hold values from -4.3 to -0.7
- head_decay_logarithm: float32 [32], replicated, may hold values from -8.5 to -0.5
- direct_path_weight: float32 [32], replicated, may hold values from 0.1 to 1.9
- gated_norm_gain: float32 [32, 64], replicated, may hold values from 0.1 to 1.9
- position_decay_offset: float32 [24, 512, 32], P('grp', 'sp'), parts along dimension 0, may hold values from -2.1 to 0
Outputs:
- state_cache: bfloat16 [24, 32, 64, 128], P('grp', 'tp', 'sp'), parts along dimension 0
- first_read: bfloat16 [24, 32, 64], P('grp', 'tp', 'sp'), parts along dimension 0
The draws below stay inside these ranges and needn't reach their ends.
There are 2 independent parts, one for each index of `grp`. The reference program is written for one: setup_inputs(seed, part) draws one part's arguments, and reference() takes and returns one part's arrays. A program takes and returns all parts, laid end to end along the dimension named above; an argument that names none is the same for every part. Nothing has to cross between parts.
All inputs are finite; a program needn't handle non-finite values.
Results may differ from the reference program's by a relative error of at most 0.011.
Values may be sent and summed in bfloat16 or wider, within the bound.
A program may use at most 64 MiB of HBM per device.

```python
import math
import jax
import jax.numpy as jnp
from jax import lax

D = 2048
HEADS = 32
P_SIZE = 64
GROUPS = 2
STATE = 128
CONV = 4
SPAN = 64
SEQS = 12
LEN = 512


def head_speeds(key, fast_share):
    return jax.random.uniform(jax.random.fold_in(key, 11), (HEADS,), jnp.float32) < fast_share


def draw_step_size_bias(key, part):
    fast_share = 0.5
    fast_heads = head_speeds(key, fast_share)
    jitter = jax.random.uniform(jax.random.fold_in(key, 12), (HEADS,), jnp.float32, -0.3, 0.3)
    return (jnp.where(fast_heads, -1.0, -4.0) + jitter).astype(jnp.float32)


def draw_head_decay_logarithm(key, part):
    fast_share = 0.5
    fast_heads = head_speeds(key, fast_share)
    fraction = jax.random.uniform(jax.random.fold_in(key, 13), (HEADS,), jnp.float32)
    fast_rate = jnp.exp(math.log(0.01) + fraction * math.log(10.0 / 3.0)) / 0.4
    slow_rate = jnp.exp(math.log(0.1 / LEN) + fraction * math.log(6.0)) / 0.035
    return jnp.log(jnp.where(fast_heads, fast_rate, slow_rate)).astype(jnp.float32)


def draw_prompt_layer_input(key, part):
    block_count = LEN // SPAN
    drawn_draw = jnp.clip(jax.random.normal(jax.random.fold_in(key, 21), (SEQS, LEN, D), jnp.float32), -6.0, 6.0)
    spread = jnp.exp(jax.random.uniform(jax.random.fold_in(key, 22), (SEQS, block_count), jnp.float32, math.log(0.6), math.log(1.6)))
    shaped = drawn_draw.reshape(SEQS, block_count, SPAN, D) * spread[:, :, None, None]
    return shaped.reshape(SEQS, LEN, D).astype(jnp.bfloat16)


def draw_position_decay_offset(key, part):
    positions = jax.random.randint(jax.random.fold_in(key, 31), (SEQS, 3, HEADS), 0, LEN)
    strength = jax.random.uniform(jax.random.fold_in(key, 32), (SEQS, 3, HEADS), jnp.float32, math.log(0.5), math.log(0.8))
    places = jnp.arange(LEN, dtype=jnp.int32)
    matched = places[None, :, None, None] == positions[:, None, :, :]
    return jnp.sum(jnp.where(matched, strength[:, None], 0.0), axis=2).astype(jnp.float32)


def steps_of(own_key, dims, cuts, least, top_value):
    loudness = 1.0
    for axis_at, shards_of in cuts:
        heights = jax.random.uniform(jax.random.fold_in(jax.random.fold_in(own_key, 6), axis_at), (shards_of,), jnp.float32, least / len(cuts), top_value / len(cuts))
        loudness = loudness * jnp.repeat(jnp.exp(heights), dims[axis_at] // shards_of).reshape((-1,) + (1,) * (len(dims) - 1 - axis_at))
    return loudness


def gaussian(key, shape, scale, limit, cuts=(), kind=jnp.bfloat16):
    values = scale * jax.random.normal(key, shape, jnp.float32)
    if cuts:
        values = values * steps_of(key, shape, cuts, -0.22, 0.18)
    return jnp.clip(values, -limit, limit).astype(kind)


def setup_inputs(seed: int = 0, part: int = 0) -> dict:
    splits = jax.random.split(jax.random.key(seed), 16)
    part_keys = jax.random.split(jax.random.fold_in(splits[15], part), 16)
    return {
        "prompt_layer_input": draw_prompt_layer_input(jax.random.fold_in(jax.random.fold_in(splits[15], part), 71), part),
        "next_token_input": gaussian(part_keys[1], (SEQS, D), 1.0, 6.0),
        "value_projection": gaussian(splits[2], (D, HEADS * P_SIZE), D ** -0.5, 0.125, ((1, 4),)),
        "output_gate_matrix": gaussian(splits[3], (D, HEADS * P_SIZE), D ** -0.5, 0.125, ((1, 4),)),
        "key_projection": gaussian(splits[4], (D, GROUPS * STATE), (11 * D) ** -0.5, 0.0390625),
        "query_projection": gaussian(splits[5], (D, GROUPS * STATE), D ** -0.5, 0.125),
        "step_projection": gaussian(splits[6], (D, HEADS), D ** -0.5, 0.125),
        "value_filter_taps": gaussian(splits[7], (CONV, HEADS * P_SIZE), 0.5, 3.0),
        "key_filter_taps": gaussian(splits[8], (CONV, GROUPS * STATE), 0.5, 3.0),
        "query_filter_taps": gaussian(splits[9], (CONV, GROUPS * STATE), 0.5, 3.0),
        "step_size_bias": draw_step_size_bias(jax.random.fold_in(splits[15], 71), part),
        "head_decay_logarithm": draw_head_decay_logarithm(jax.random.fold_in(splits[15], 71), part),
        "direct_path_weight": jnp.clip(1.0 + 0.18 * jax.random.normal(splits[12], (HEADS,), jnp.float32), 0.1, 1.9),
        "gated_norm_gain": jnp.clip(1.0 + 0.18 * jax.random.normal(splits[13], (HEADS, P_SIZE), jnp.float32), 0.1, 1.9),
        "position_decay_offset": draw_position_decay_offset(jax.random.fold_in(jax.random.fold_in(splits[15], part), 71), part),
    }


epsilon = 1e-06

def reference(prompt_layer_input, next_token_input, value_projection, output_gate_matrix, key_projection, query_projection, step_projection, value_filter_taps, key_filter_taps, query_filter_taps, step_size_bias, head_decay_logarithm, direct_path_weight, gated_norm_gain, position_decay_offset):
    seq_count, length, width = prompt_layer_input.shape
    feature_cols = HEADS * P_SIZE
    map_cols = GROUPS * STATE
    weights_all = jnp.concatenate([value_projection, key_projection, query_projection], axis=1)
    kernel = jnp.concatenate([value_filter_taps, key_filter_taps, query_filter_taps], axis=1).astype(jnp.float32)
    token_rows = prompt_layer_input.reshape(seq_count * length, width)
    projected = jnp.dot(token_rows, weights_all, preferred_element_type=jnp.float32).astype(jnp.bfloat16)
    projected = projected.reshape(seq_count, length, feature_cols + 2 * map_cols)
    step_raw = jnp.dot(token_rows, step_projection, preferred_element_type=jnp.float32).astype(jnp.bfloat16)
    step_raw = step_raw.reshape(seq_count, length, HEADS)
    padded = jnp.concatenate([jnp.zeros((seq_count, CONV - 1, feature_cols + 2 * map_cols), jnp.bfloat16), projected], axis=1)
    total = padded[:, 0:length].astype(jnp.float32) * kernel[0]
    for tap in range(1, CONV):
        total = total + padded[:, tap:tap + length].astype(jnp.float32) * kernel[tap]
    mixed = jax.nn.silu(total).astype(jnp.bfloat16)
    head_decay_speed = jnp.exp(head_decay_logarithm)
    discrete_step = jax.nn.softplus(step_raw.astype(jnp.float32) + step_size_bias)
    logarithmic_decay = position_decay_offset - head_decay_speed * discrete_step
    head_input = mixed[:, :, :feature_cols].reshape(seq_count, length, HEADS, P_SIZE)
    in_map = mixed[:, :, feature_cols:feature_cols + map_cols].reshape(seq_count, length, GROUPS, STATE)
    block_count = length // SPAN

    def blocks(array):
        return jnp.moveaxis(array.reshape((seq_count, block_count, SPAN) + array.shape[2:]), 1, 0)

    def advance(carry, inputs):
        input_block, map_block, step_block, decay_block = inputs
        cumulative = jnp.cumsum(decay_block, axis=1)
        decay_weight = jnp.exp(cumulative[:, -1:] - cumulative) * step_block
        weighted = (input_block.astype(jnp.float32) * decay_weight[..., None]).astype(jnp.bfloat16)
        head_map = jnp.repeat(map_block, HEADS // GROUPS, axis=2)
        block_state = jnp.einsum('bshp,bshn->bhpn', weighted.astype(jnp.float32), head_map.astype(jnp.float32))
        return (jnp.exp(cumulative[:, -1])[:, :, None, None] * carry + block_state, None)
    final, unused = lax.scan(advance, jnp.zeros((seq_count, HEADS, P_SIZE, STATE), jnp.float32), (blocks(head_input), blocks(in_map), blocks(discrete_step), blocks(logarithmic_decay)))
    state_cache = final.astype(jnp.bfloat16)
    new_raw = jnp.dot(next_token_input, weights_all, preferred_element_type=jnp.float32).astype(jnp.bfloat16)
    new_step = jnp.dot(next_token_input, step_projection, preferred_element_type=jnp.float32).astype(jnp.bfloat16)
    new_gate = jnp.dot(next_token_input, output_gate_matrix, preferred_element_type=jnp.float32).astype(jnp.bfloat16)
    window = jnp.concatenate([projected[:, length - (CONV - 1):], new_raw[:, None]], axis=1)
    new_mixed = jax.nn.silu(lax.optimization_barrier(jnp.sum(window.astype(jnp.float32) * kernel[None], axis=1))).astype(jnp.bfloat16)
    new_input = new_mixed[:, :feature_cols].reshape(seq_count, HEADS, P_SIZE).astype(jnp.float32)
    new_in = jnp.repeat(new_mixed[:, feature_cols:feature_cols + map_cols].reshape(seq_count, GROUPS, STATE), HEADS // GROUPS, axis=1).astype(jnp.float32)
    new_out = jnp.repeat(new_mixed[:, feature_cols + map_cols:].reshape(seq_count, GROUPS, STATE), HEADS // GROUPS, axis=1).astype(jnp.float32)
    new_step_size = jax.nn.softplus(new_step.astype(jnp.float32) + step_size_bias)
    cache_values = lax.optimization_barrier(state_cache).astype(jnp.float32)
    new_state = jnp.exp(-head_decay_speed * new_step_size)[:, :, None, None] * cache_values + (new_step_size[:, :, None] * new_input)[..., None] * new_in[:, :, None, :]
    readout = lax.optimization_barrier(jnp.sum(new_state * new_out[:, :, None, :], axis=-1)) + direct_path_weight[None, :, None] * new_input
    gated = readout * jax.nn.silu(new_gate.astype(jnp.float32).reshape(seq_count, HEADS, P_SIZE))
    scale = lax.rsqrt(lax.optimization_barrier(jnp.mean(gated * gated, axis=(1, 2), keepdims=True)) + epsilon)
    first_read = (gated * scale * gated_norm_gain[None]).astype(jnp.bfloat16)
    return (state_cache, first_read)
```

```python
import jax
import jax.numpy as jnp
from jax import lax
from jax.experimental import pallas as pl
from jax.experimental.pallas import tpu as pltpu
from jax.sharding import PartitionSpec as P

HEADS = 32
P_SIZE = 64
GROUPS = 2
STATE = 128
CONV = 4
SPAN = 64


epsilon = 1e-06


def shifted(block, axis, distance):
    devices = range(lax.axis_size(axis))
    route = [(i - distance, i) for i in devices if i - distance in devices]
    return lax.ppermute(block, axis, route)


def broadcast(value, axis, source):
    kept = jnp.where(lax.axis_index(axis) == source, value, 0).astype(value.dtype)
    return lax.psum(kept, axis)


def prefix(shard, axis, combine, identity):
    length, here = (lax.axis_size(axis), lax.axis_index(axis))
    everything = lax.all_gather(shard, axis)
    start = jnp.broadcast_to(jnp.asarray(identity, shard.dtype), shard.shape)

    def lap(k, before):
        at = length - 1 - k
        reached = at > here
        new = combine(before, everything[at])
        return jnp.where(reached, new, before)

    return lax.fori_loop(0, length, lap, start)


def shards(
    prompt_layer_input,
    next_token_input,
    value_projection,
    output_gate_matrix,
    key_projection,
    query_projection,
    step_projection,
    value_filter_taps,
    key_filter_taps,
    query_filter_taps,
    step_size_bias,
    head_decay_logarithm,
    direct_path_weight,
    gated_norm_gain,
    position_decay_offset,
):
    seq_count, local_len, width = prompt_layer_input.shape
    resident_heads = value_projection.shape[1] // P_SIZE
    feature_cols = resident_heads * P_SIZE
    shard_count = lax.axis_size("sp")
    rows_here = P_SIZE // shard_count
    shard_index = lax.axis_index("sp")
    leading_head = lax.axis_index("tp") * resident_heads
    group_index = leading_head // (HEADS // GROUPS)
    row_first = shard_index * rows_here
    in_cols = lax.dynamic_slice_in_dim(key_projection, group_index * STATE, STATE, 1)
    out_cols = lax.dynamic_slice_in_dim(query_projection, group_index * STATE, STATE, 1)
    weights_here = jnp.concatenate([value_projection, in_cols, out_cols], axis=1)
    step_cols = lax.dynamic_slice_in_dim(step_projection, leading_head, resident_heads, 1)
    kernel = jnp.concatenate(
        [
            lax.dynamic_slice_in_dim(value_filter_taps, leading_head * P_SIZE, feature_cols, 1),
            lax.dynamic_slice_in_dim(key_filter_taps, group_index * STATE, STATE, 1),
            lax.dynamic_slice_in_dim(query_filter_taps, group_index * STATE, STATE, 1),
        ],
        axis=1,
    ).astype(jnp.float32)
    head_decay_speed = jnp.exp(
        lax.dynamic_slice_in_dim(head_decay_logarithm, leading_head, resident_heads, 0)
    )
    bias_here = lax.dynamic_slice_in_dim(step_size_bias, leading_head, resident_heads, 0)
    skip_here = lax.dynamic_slice_in_dim(direct_path_weight, leading_head, resident_heads, 0)
    gain_here = lax.dynamic_slice(
        gated_norm_gain, (leading_head, row_first), (resident_heads, rows_here)
    )
    token_rows = prompt_layer_input.reshape(seq_count * local_len, width)
    projected = jnp.dot(token_rows, weights_here, preferred_element_type=jnp.float32).astype(
        jnp.bfloat16
    )
    projected = projected.reshape(seq_count, local_len, feature_cols + 2 * STATE)
    trailing = projected[:, local_len - (CONV - 1) :]
    before = shifted(trailing, "sp", 1)
    newest = broadcast(trailing, "sp", shard_count - 1)
    padded = jnp.concatenate([before, projected], axis=1)
    total = padded[:, 0:local_len].astype(jnp.float32) * kernel[0]
    for tap in range(1, CONV):
        total = total + padded[:, tap : tap + local_len].astype(jnp.float32) * kernel[tap]
    mixed = jax.nn.silu(total).astype(jnp.bfloat16)
    step_raw = jnp.dot(token_rows, step_cols, preferred_element_type=jnp.float32).astype(
        jnp.bfloat16
    )
    discrete_step = jax.nn.softplus(step_raw.astype(jnp.float32) + bias_here).reshape(
        seq_count, local_len, resident_heads
    )
    decay_spikes = lax.dynamic_slice_in_dim(position_decay_offset, leading_head, resident_heads, 2)
    logarithmic_decay = decay_spikes - head_decay_speed * discrete_step
    block_count = local_len // SPAN
    cumulative = jnp.cumsum(
        logarithmic_decay.reshape(seq_count, block_count, SPAN, resident_heads), axis=2
    )
    decay_weight = jnp.exp(cumulative[:, :, -1:] - cumulative) * discrete_step.reshape(
        seq_count, block_count, SPAN, resident_heads
    )
    head_input = mixed[:, :, :feature_cols].reshape(
        seq_count, block_count, SPAN, resident_heads, P_SIZE
    )
    weighted = (head_input.astype(jnp.float32) * decay_weight[..., None]).astype(jnp.bfloat16)
    in_map = mixed[:, :, feature_cols : feature_cols + STATE].reshape(
        seq_count, block_count, SPAN, STATE
    )
    block_state = jnp.einsum(
        "bcshp,bcsn->bchpn", weighted, in_map, preferred_element_type=jnp.float32
    )
    block_log = cumulative[:, :, -1]
    own_log = jnp.sum(block_log, axis=1)
    after_block = jnp.exp(own_log[:, None] - jnp.cumsum(block_log, axis=1))
    local_state = jnp.sum(after_block[..., None, None] * block_state, axis=1)
    later_log = prefix(own_log, "sp", jnp.add, jnp.zeros_like(own_log))
    scaled = jnp.exp(later_log)[:, :, None, None] * local_state
    own_rows = lax.psum_scatter(scaled, "sp", scatter_dimension=2, tiled=True)
    state_cache = own_rows.astype(jnp.bfloat16)
    new_raw = jnp.dot(next_token_input, weights_here, preferred_element_type=jnp.float32).astype(
        jnp.bfloat16
    )
    new_step = jnp.dot(next_token_input, step_cols, preferred_element_type=jnp.float32).astype(
        jnp.bfloat16
    )
    new_gate = jnp.dot(
        next_token_input, output_gate_matrix, preferred_element_type=jnp.float32
    ).astype(jnp.bfloat16)
    window = jnp.concatenate([newest, new_raw[:, None]], axis=1)
    new_mixed = jax.nn.silu(jnp.sum(window.astype(jnp.float32) * kernel[None], axis=1)).astype(
        jnp.bfloat16
    )
    new_input = lax.dynamic_slice_in_dim(
        new_mixed[:, :feature_cols].reshape(seq_count, resident_heads, P_SIZE),
        row_first,
        rows_here,
        2,
    ).astype(jnp.float32)
    new_in = new_mixed[:, feature_cols : feature_cols + STATE].astype(jnp.float32)
    new_out = new_mixed[:, feature_cols + STATE :].astype(jnp.float32)
    new_step_size = jax.nn.softplus(new_step.astype(jnp.float32) + bias_here)
    cache_values = lax.optimization_barrier(state_cache).astype(jnp.float32)
    new_state = (
        jnp.exp(-head_decay_speed * new_step_size)[:, :, None, None] * cache_values
        + (new_step_size[:, :, None] * new_input)[..., None] * new_in[:, None, None, :]
    )
    readout = (
        jnp.sum(new_state * new_out[:, None, None, :], axis=-1)
        + skip_here[None, :, None] * new_input
    )
    gate_rows = lax.dynamic_slice_in_dim(
        new_gate.reshape(seq_count, resident_heads, P_SIZE), row_first, rows_here, 2
    )
    gated = readout * jax.nn.silu(gate_rows.astype(jnp.float32))
    squares = lax.psum(jnp.sum(gated * gated, axis=(1, 2)), ("sp", "tp"))
    scale = lax.rsqrt(squares / (HEADS * P_SIZE) + epsilon)
    first_read = (gated * scale[:, None, None] * gain_here[None]).astype(jnp.bfloat16)
    return (state_cache, first_read)


F32, BF16 = jnp.float32, jnp.bfloat16
MESH = pl.DeviceIdType.MESH
EXACT = lax.Precision.HIGHEST


def exact_dot(a, b, dims=((1,), (0,))):
    return lax.dot_general(a, b, (dims, ((), ())), precision=EXACT, preferred_element_type=F32)


def softplus(v):
    return jnp.maximum(v, 0.0) + jnp.log1p(jnp.exp(-jnp.abs(v)))


def silu(v):
    return v / (1.0 + jnp.exp(-v))


def ones_where(shape, test, dtype=F32):
    rows = lax.broadcasted_iota(jnp.int32, shape, 0)
    cols = lax.broadcasted_iota(jnp.int32, shape, 1)
    return jnp.where(test(rows, cols), 1.0, 0.0).astype(dtype)


def mixer_kernel(
    dims,
    x_hbm,
    next_ref,
    wv_hbm,
    wg_hbm,
    wk_hbm,
    wq_hbm,
    ws_hbm,
    tv_ref,
    tk_ref,
    tq_ref,
    bias_ref,
    speed_ref,
    skip_ref,
    gain_ref,
    off_hbm,
    cache_hbm,
    read_ref,
    xbuf,
    edge,
    wall,
    wq,
    ws,
    wg,
    off,
    taps,
    pad,
    wsplit,
    halo_out,
    halo_in,
    halo,
    newest,
    heads_t,
    decay,
    log_own,
    log_out,
    log_in,
    own,
    from_left,
    from_right,
    kept_buf,
    sq_out,
    sq_in,
    expand,
    load_sem,
    x_sem,
    halo_sem,
    new_sem,
    st_send,
    st_recv,
    log_send,
    log_recv,
    out_sem,
    sq_send,
    sq_recv,
):
    n, m, S, L, heads, R, G = dims
    F = heads * P_SIZE
    C = F + STATE
    RH = heads * R
    SP = 16
    steps = S // G
    lead_steps = min(LEAD, steps)
    me, tp = lax.axis_index("sp"), lax.axis_index("tp")
    lead = pl.multiple_of(tp * heads, 8)
    group = lax.div(lead, HEADS // GROUPS)
    fcol = pl.multiple_of(tp * F, 128)
    gcol = pl.multiple_of(group * STATE, 128)

    def load(src, dst, k):
        c = pltpu.make_async_copy(src, dst, load_sem.at[k])
        c.start()
        return c

    def load_x(g):
        return pltpu.make_async_copy(
            x_hbm.at[pl.ds(g * G, G)], xbuf.at[pl.ds(g * G, G)], x_sem.at[g]
        )

    first = [
        load(ws_hbm.at[pl.ds(lead, heads), :], ws, 0),
        load(x_hbm.at[:, pl.ds(L - 16, 16)], edge.at[pl.ds(0, S)], 1),
        load(wk_hbm.at[:, pl.ds(gcol, STATE)], wall.at[:, pl.ds(F, STATE)], 2),
        load(wv_hbm, wall.at[:, pl.ds(0, F)], 3),
        load(wq_hbm.at[:, pl.ds(gcol, STATE)], wq, 4),
    ]
    off_load = load(off_hbm.at[:, pl.ds(lead, heads), :], off, 5)
    for g in range(steps):
        load_x(g).start()
    gate_load = load(wg_hbm, wg, 6)

    peers = [(a, b) for a in range(n) for b in range(m) if (a, b) != (0, 0)]

    def at(a, b=0):
        return {"sp": lax.rem(me + a, n), "tp": lax.rem(tp + b, m)}

    barrier = pltpu.get_barrier_semaphore()
    for a, b in peers:
        pl.semaphore_signal(barrier, inc=1, device_id=at(a, b), device_id_type=MESH)

    taps[:, 0:F] = tv_ref[:, pl.ds(fcol, F)].astype(F32)
    taps[:, F:C] = tk_ref[:, pl.ds(gcol, STATE)].astype(F32)
    taps[:, C : C + STATE] = tq_ref[:, pl.ds(gcol, STATE)].astype(F32)
    edge[S] = jnp.zeros(edge.shape[1:], BF16)
    edge[S, 0:S, :] = next_ref[...]
    halo_out[...] = jnp.zeros_like(halo_out)
    head_of = ones_where((heads, F), lambda i, c: i == lax.div(c, P_SIZE))
    expand[...] = jnp.concatenate([head_of, head_of], axis=0).astype(BF16)
    bias = bias_ref[...]
    speed = jnp.exp(speed_ref[...])
    square = jnp.zeros((128, 128 - HEADS), F32)

    def columns(row, k):
        full = jnp.concatenate([jnp.broadcast_to(row, (128, HEADS)), square], axis=1)
        heads_t[k] = full.T[0:HEADS]
        return heads_t[k, pl.ds(lead, heads), :]

    bias_t, speed_t = columns(bias, 0), columns(speed, 1)

    @pl.when(me == 0)
    def _():
        from_left[:, 0] = jnp.zeros((S, RH, STATE), BF16)

    @pl.when(me == n - 1)
    def _():
        from_right[:, n - 1] = jnp.zeros((S, RH, STATE), BF16)
        log_in[...] = jnp.zeros_like(log_in)

    eye = ones_where((heads, 128), lambda i, c: i == c)
    later_ones = ones_where((L, L), lambda u, t: u > t, BF16)

    first[0].wait()
    wall[:, C : C + STATE] = jnp.concatenate(
        [ws[...], jnp.zeros((STATE - heads, ws.shape[1]), BF16)], axis=0
    ).T
    for c in first[1:4]:
        c.wait()
    rows = edge[...].reshape((S + 1) * 16, edge.shape[2])
    eproj = jnp.dot(rows, wall[...], preferred_element_type=F32).astype(BF16).astype(F32)
    e3 = eproj.reshape(S + 1, 16, C + STATE)
    for j in range(CONV - 1):
        halo_out[j, 0:S, :] = e3[0:S, 16 - (CONV - 1) + j, 0:C].astype(BF16)

    pl.semaphore_wait(barrier, len(peers))

    def halo_copy():
        return pltpu.make_async_remote_copy(
            halo_out, halo_in, halo_sem.at[0], halo_sem.at[1], device_id=at(1), device_id_type=MESH
        )

    @pl.when(me < n - 1)
    def _():
        halo_copy().start()

    first[4].wait()
    eq = jnp.dot(rows, wq[...], preferred_element_type=F32).astype(BF16).astype(F32)
    q3 = eq.reshape(S + 1, 16, STATE)
    new_raw = jnp.concatenate([e3[S, :, 0:C], q3[S]], axis=1)
    new_step = e3[S, :, C : C + STATE]

    def newest_copy():
        return pltpu.make_async_remote_copy(
            newest,
            newest,
            new_sem.at[0],
            new_sem.at[1],
            device_id=at(n - 1),
            device_id_type=MESH,
        )

    @pl.when(me == n - 1)
    def _():
        total = jnp.zeros((S, C + STATE), F32)
        for j in range(CONV - 1):
            row = 16 - (CONV - 1) + j
            tail = jnp.concatenate([e3[0:S, row, 0:C], q3[0:S, row, :]], axis=1)
            total = total + tail * taps[j : j + 1, :]
        newest[...] = jnp.zeros_like(newest)
        newest[0:S, :] = total
        newest_copy().start()

    def span(s, right, far):
        if right:
            return (s + 2, n) if far else (s + 1, s + 2)
        return (0, s - 1) if far else (s - 1, s)

    def flow(g, s, right, far):
        lo, hi = span(s, right, far)
        if not (0 <= lo < hi <= n):
            return None
        k = 2 * int(right) + int(far)
        here = (pl.ds(g * G, G), pl.ds(lo, hi - lo))
        return pltpu.make_async_remote_copy(
            own.at[here],
            (from_left if right else from_right).at[here],
            st_send.at[k, g],
            st_recv.at[k, g],
            device_id=at(1 if right else n - 1),
            device_id_type=MESH,
        )

    def begin(g, s, right, far):
        c = flow(g, s, right, far)
        if c is not None:
            c.start()

    def log_copy(g):
        here = pl.ds(g * G, G)
        return pltpu.make_async_remote_copy(
            log_out.at[here],
            log_in.at[here],
            log_send.at[g],
            log_recv.at[g],
            device_id=at(n - 1),
            device_id_type=MESH,
        )

    def project(g):
        load_x(g).wait()
        slot = lax.rem(g, lead_steps)
        xg = xbuf[pl.ds(g * G, G)].reshape(G * L, xbuf.shape[2])
        acc = jnp.dot(xg, wall[...], preferred_element_type=F32).astype(BF16).astype(F32)
        for q in range(G):
            p = g * G + q
            raw = acc[q * L : (q + 1) * L]
            pad[slot, q, 8 : 8 + L, :] = raw[:, 0:C]
            dt = softplus(raw[:, C : C + STATE].T[0:heads] + bias_t)
            ld = off[p] - speed_t * dt
            a = ld.astype(BF16).astype(F32)
            b = (ld - a).astype(BF16).astype(F32)
            parts = jnp.concatenate([a, b, ld - a - b, jnp.zeros_like(a)], axis=0).astype(BF16)
            sums = jnp.dot(parts, later_ones, preferred_element_type=F32)
            suffix = sums[0:heads] + sums[heads : 2 * heads] + sums[2 * heads : 3 * heads]
            whole = jnp.broadcast_to(suffix[:, 0:1] + ld[:, 0:1], (heads, 128))
            decay[p] = jnp.exp(whole)
            log_own[p] = jnp.sum(whole * eye, axis=0, keepdims=True)
            w = dt * jnp.exp(suffix)
            hi = w.astype(BF16).astype(F32)
            wsplit[slot, q] = jnp.concatenate([hi, w - hi], axis=0).astype(BF16)

    def states(g):
        slot = lax.rem(g, lead_steps)
        for q in range(G):
            p = g * G + q
            for j in range(CONV - 1):
                r = 8 - (CONV - 1) + j
                pad[slot, q, r : r + 1, :] = halo[j, pl.ds(p, 1), :]
            wide = lax.dot_general(
                wsplit[slot, q],
                expand[...],
                (((0,), (0,)), ((), ())),
                preferred_element_type=F32,
            )

            def mixed(c):
                s = slice(c, c + 128)
                t = pad[slot, q, 8 - (CONV - 1) : 8 - (CONV - 1) + L, s] * taps[0:1, s]
                for j in range(1, CONV):
                    r = 8 - (CONV - 1) + j
                    t = t + pad[slot, q, r : r + L, s] * taps[j : j + 1, s]
                return silu(t).astype(BF16)

            in_map = mixed(F)
            for c in range(0, F, 128):
                weighted = (mixed(c).astype(F32) * wide[:, c : c + 128]).astype(BF16)
                share = lax.dot_general(
                    weighted, in_map, (((0,), (0,)), ((), ())), preferred_element_type=F32
                ).astype(BF16)
                for hh in range(128 // P_SIZE):
                    h = c // P_SIZE + hh
                    for d in range(n):
                        b = hh * P_SIZE + d * R
                        own[p, d, h * R : (h + 1) * R, :] = share[b : b + R]

    def later_factor(p):
        row = jnp.sum(eye * log_in[p], axis=1, keepdims=True)
        return jnp.exp(jnp.broadcast_to(row, (heads, 128)))

    def relay(g):
        for s in range(1, n - 1):

            @pl.when(me == s)
            def _(s=s):
                if s + 1 < n:
                    flow(g, s - 1, True, True).wait_recv()
                for q in range(G):
                    p = g * G + q
                    factor = decay[p]
                    for d in range(s + 1, n):
                        for h in range(heads):
                            z = (p, d, slice(h * R, (h + 1) * R))
                            got = from_left[z].astype(F32) * factor[h : h + 1, :]
                            own[z] = (own[z].astype(F32) + got).astype(BF16)
                begin(g, s, True, True)
                begin(g, s, True, False)
                log_copy(g).wait_recv()
                for q in range(G):
                    p = g * G + q
                    log_out[p] = log_in[p] + log_own[p]
                log_copy(g).start()
                flow(g, s + 1, False, True).wait_recv()
                for q in range(G):
                    p = g * G + q
                    factor = later_factor(p)
                    for d in range(s):
                        for h in range(heads):
                            z = (p, d, slice(h * R, (h + 1) * R))
                            mine = own[z].astype(F32) * factor[h : h + 1, :]
                            own[z] = (from_right[z].astype(F32) + mine).astype(BF16)
                begin(g, s, False, True)
                begin(g, s, False, False)

    off_load.wait()
    lax.fori_loop(0, lead_steps, lambda g, carry: (project(g), carry)[1], 0)

    @pl.when(me == 0)
    def _():
        halo[...] = jnp.zeros_like(halo)

    @pl.when(me > 0)
    def _():
        halo_copy().wait_recv()
        halo[...] = halo_in[...].astype(F32)

    relay_lag, near_lag = min(RELAY_LAG, steps), min(NEAR_LAG, steps)

    def step(g, carry):
        states(g)

        @pl.when(me == 0)
        def _():
            begin(g, 0, True, True)

        @pl.when(me == n - 1)
        def _():
            for q in range(G):
                log_out[g * G + q] = log_own[g * G + q]
            log_copy(g).start()
            begin(g, n - 1, False, True)

        @pl.when(g >= near_lag)
        def _():
            @pl.when(me == 0)
            def _():
                begin(g - near_lag, 0, True, False)

            @pl.when(me == n - 1)
            def _():
                begin(g - near_lag, n - 1, False, False)

        @pl.when(g + lead_steps < steps)
        def _():
            project(g + lead_steps)

        if n > 2:

            @pl.when((g == min(1, steps - 1)) & (me > 0) & (me < n - 1))
            def _():
                newest_copy().wait_recv()
                newest_copy().start()

        @pl.when(g >= relay_lag)
        def _():
            relay(g - relay_lag)

        return carry

    lax.fori_loop(0, steps, step, 0)
    for g in range(steps - near_lag, steps):

        @pl.when(me == 0)
        def _(g=g):
            begin(g, 0, True, False)

        @pl.when(me == n - 1)
        def _(g=g):
            begin(g, n - 1, False, False)

    head_cols = ones_where((HEADS, RH), lambda i, l: i == lead + lax.div(l, R))
    local_cols = ones_where((128, RH), lambda i, l: i == lax.div(l, R))
    local = ones_where((HEADS, 128), lambda i, c: (i == lead + c) & (c < heads))
    pick = ones_where(
        (F, RH), lambda c, l: c == lax.div(l, R) * P_SIZE + me * R + lax.rem(l, R), BF16
    )
    row_pick = ones_where((P_SIZE, RH), lambda c, l: c == me * R + lax.rem(l, R))
    gate_load.wait()
    gate = jnp.dot(edge[S], wg[...], preferred_element_type=F32).astype(BF16)
    gate_here = silu(jnp.dot(gate, pick, preferred_element_type=F32))
    gain_here = jnp.sum(exact_dot(gain_ref[...], row_pick) * head_cols, axis=0, keepdims=True)
    skip_here = exact_dot(skip_ref[...], head_cols)
    new_dt = softplus(new_step + exact_dot(bias, local))
    dt_here = exact_dot(new_dt, local_cols)
    keep_here = jnp.exp(-exact_dot(exact_dot(speed, local) * new_dt, local_cols))

    @pl.when(me == 0)
    def _():
        newest_copy().wait_recv()

    new_mixed = silu(newest[...] + new_raw * taps[CONV - 1 : CONV, :]).astype(BF16)
    new_input = jnp.dot(new_mixed[:, 0:F], pick, preferred_element_type=F32)
    new_in = new_mixed[:, F:C].astype(F32)
    new_out = new_mixed[:, C : C + STATE]
    both = jnp.sum(new_in * new_out.astype(F32), axis=1, keepdims=True)
    where_row = lax.broadcasted_iota(jnp.int32, (SP, RH), 0)

    def out_copy(g):
        here = pl.ds(g * G, G)
        return pltpu.make_async_copy(kept_buf.at[here], cache_hbm.at[here], out_sem.at[g])

    def finish(g, y):
        for s in range(n):

            @pl.when(me == s)
            def _(s=s):
                if s > 0:
                    flow(g, s - 1, True, False).wait_recv()
                if s == 0:
                    log_copy(g).wait_recv()
                if s < n - 1:
                    flow(g, s + 1, False, False).wait_recv()

        for q in range(G):
            p = g * G + q
            before, after = decay[p], later_factor(p)
            kept = []
            for h in range(heads):
                z = (p, me, slice(h * R, (h + 1) * R))
                t = own[z].astype(F32) + from_left[z].astype(F32) * before[h : h + 1, :]
                t = t * after[h : h + 1, :] + from_right[z].astype(F32)
                kept.append(t.astype(BF16))
            kept = jnp.concatenate(kept, axis=0)
            kept_buf[p] = kept
            part = lax.dot_general(
                new_out, kept, (((1,), (1,)), ((), ())), preferred_element_type=F32
            )
            y = jnp.where(where_row == p, part, y)
        out_copy(g).start()
        return y

    y = jnp.zeros((SP, RH), F32)
    left = list(range(steps - relay_lag, steps))
    done = 0
    for i, g in enumerate(left):
        relay(g)
        upto = max(done, g - 2) if i + 1 < len(left) else steps
        if upto > done:
            y = lax.fori_loop(done, upto, finish, y)
            done = upto

    readout = keep_here * y + dt_here * new_input * both + skip_here * new_input
    gated = readout * gate_here
    square_sum = jnp.broadcast_to(jnp.sum(gated * gated, axis=1, keepdims=True), (SP, 128))
    diagonal = ones_where((SP, 128), lambda i, c: i == c)
    sq = jnp.sum(square_sum * diagonal, axis=0, keepdims=True)
    sq_out[...] = sq

    def sq_copy(i):
        a, b = peers[i]
        return pltpu.make_async_remote_copy(
            sq_out, sq_in.at[i], sq_send.at[i], sq_recv.at[i], device_id=at(a, b), device_id_type=MESH
        )

    for i in range(len(peers)):
        sq_copy(i).start()
    for g in range(steps):
        out_copy(g).wait()
    for s in range(n):

        @pl.when(me == s)
        def _(s=s):
            for g in range(steps):
                for right in (False, True):
                    for far in (False, True):
                        c = flow(g, s, right, far)
                        if c is not None:
                            c.wait_send()
                if s > 0:
                    log_copy(g).wait_send()

    @pl.when(me < n - 1)
    def _():
        halo_copy().wait_send()

    @pl.when(me > 0)
    def _():
        newest_copy().wait_send()

    for i in range(len(peers)):
        sq_copy(i).wait_recv()
        sq = sq + sq_in[i]
    mean = jnp.sum(diagonal * sq, axis=1, keepdims=True) / (HEADS * P_SIZE)
    scale = lax.rsqrt(mean + epsilon)
    read_ref[...] = (gated * scale * gain_here).astype(BF16)[0:S]

    for i in range(len(peers)):
        sq_copy(i).wait_send()


LEAD, RELAY_LAG, NEAR_LAG = 2, 2, 2


def fused(*args):
    x, wv, wk = args[0], args[2], args[4]
    S, L, D = x.shape
    n, m = lax.axis_size("sp"), lax.axis_size("tp")
    F = wv.shape[1]
    heads = F // P_SIZE
    R = P_SIZE // n
    G = next(g for g in (2, 3, 1) if S % g == 0)
    steps = S // G
    slots = min(LEAD, steps)
    C, RH, SP = F + STATE, heads * R, 16
    dims = (n, m, S, L, heads, R, G)
    flat = list(args)
    for i in (10, 11, 12):
        flat[i] = args[i].reshape(1, HEADS)
    flat[6] = args[6].T
    flat[14] = jnp.swapaxes(args[14], 1, 2)
    hbm, vmem = pl.BlockSpec(memory_space=pl.ANY), pl.BlockSpec(memory_space=pltpu.VMEM)
    specs = [hbm, vmem, hbm, hbm, hbm, hbm, hbm] + [vmem] * 7 + [hbm]
    dma = pltpu.SemaphoreType.DMA
    cache, read = pl.pallas_call(
        lambda *refs: mixer_kernel(dims, *refs),
        out_shape=(
            jax.ShapeDtypeStruct((S, RH, STATE), BF16),
            jax.ShapeDtypeStruct((S, RH), BF16),
        ),
        in_specs=specs,
        out_specs=(pl.BlockSpec(memory_space=pltpu.HBM), vmem),
        scratch_shapes=[
            pltpu.VMEM((S, L, D), BF16),
            pltpu.VMEM((S + 1, 16, D), BF16),
            pltpu.VMEM((D, C + STATE), BF16),
            pltpu.VMEM((D, STATE), BF16),
            pltpu.VMEM((heads, D), BF16),
            pltpu.VMEM((D, F), BF16),
            pltpu.VMEM((S, heads, L), F32),
            pltpu.VMEM((CONV, C + STATE), F32),
            pltpu.VMEM((slots, G, 8 + L, C), F32),
            pltpu.VMEM((slots, G, 2 * heads, L), BF16),
            pltpu.VMEM((CONV - 1, SP, C), BF16),
            pltpu.VMEM((CONV - 1, SP, C), BF16),
            pltpu.VMEM((CONV - 1, SP, C), F32),
            pltpu.VMEM((SP, C + STATE), F32),
            pltpu.VMEM((2, HEADS, 128), F32),
            pltpu.VMEM((S, heads, 128), F32),
            pltpu.VMEM((S, 1, 128), F32),
            pltpu.VMEM((S, 1, 128), F32),
            pltpu.VMEM((S, 1, 128), F32),
            pltpu.VMEM((S, n, RH, STATE), BF16),
            pltpu.VMEM((S, n, RH, STATE), BF16),
            pltpu.VMEM((S, n, RH, STATE), BF16),
            pltpu.VMEM((S, RH, STATE), BF16),
            pltpu.VMEM((1, 128), F32),
            pltpu.VMEM((n * m - 1, 1, 128), F32),
            pltpu.VMEM((2 * heads, F), BF16),
            dma((7,)),
            dma((steps,)),
            dma((2,)),
            dma((2,)),
            dma((4, steps)),
            dma((4, steps)),
            dma((steps,)),
            dma((steps,)),
            dma((steps,)),
            dma((n * m,)),
            dma((n * m,)),
        ],
        compiler_params=pltpu.CompilerParams(
            collective_id=0, has_side_effects=True, vmem_limit_bytes=56 * 1024 * 1024
        ),
    )(*flat)
    return cache.reshape(S, heads, R, STATE), read.reshape(S, heads, R)


def fits(n, m, shapes):
    (S, L), F = shapes
    heads, R = F // P_SIZE, P_SIZE // n
    return (
        n > 1
        and F % 128 == 0
        and heads % 8 == 0
        and R % 16 == 0
        and (heads * R) % 128 == 0
        and S <= 16
        and L % 16 == 0
        and L == 128
        and (HEADS // GROUPS) % heads == 0
    )


def part(*args):
    shapes = (args[0].shape[:2], args[2].shape[1])
    if fits(lax.axis_size("sp"), lax.axis_size("tp"), shapes):
        return fused(*args)
    return shards(*args)


def solution(mesh):
    in_specs = (
        P("grp", "sp", None),
        P("grp", None),
        P(None, "tp"),
        P(None, "tp"),
        P(),
        P(),
        P(),
        P(),
        P(),
        P(),
        P(),
        P(),
        P(),
        P(),
        P("grp", "sp", None),
    )
    out_specs = (P("grp", "tp", "sp", None), P("grp", "tp", "sp"))
    return jax.shard_map(part, mesh=mesh, in_specs=in_specs, out_specs=out_specs, check_vma=False)
```

```python
import jax
import jax.numpy as jnp
from jax import lax
from jax.experimental import pallas as pl
from jax.experimental.pallas import tpu as pltpu
from jax.sharding import PartitionSpec as P

HEADS = 32
P_SIZE = 64
GROUPS = 2
STATE = 128
CONV = 4
SPAN = 64


epsilon = 1e-06


def shifted(block, axis, distance):
    devices = range(lax.axis_size(axis))
    route = [(i - distance, i) for i in devices if i - distance in devices]
    return lax.ppermute(block, axis, route)


def broadcast(value, axis, source):
    kept = jnp.where(lax.axis_index(axis) == source, value, 0).astype(value.dtype)
    return lax.psum(kept, axis)


def prefix(shard, axis, combine, identity):
    length, here = (lax.axis_size(axis), lax.axis_index(axis))
    everything = lax.all_gather(shard, axis)
    start = jnp.broadcast_to(jnp.asarray(identity, shard.dtype), shard.shape)

    def lap(k, before):
        at = length - 1 - k
        reached = at > here
        new = combine(before, everything[at])
        return jnp.where(reached, new, before)

    return lax.fori_loop(0, length, lap, start)


def shards(
    prompt_layer_input,
    next_token_input,
    value_projection,
    output_gate_matrix,
    key_projection,
    query_projection,
    step_projection,
    value_filter_taps,
    key_filter_taps,
    query_filter_taps,
    step_size_bias,
    head_decay_logarithm,
    direct_path_weight,
    gated_norm_gain,
    position_decay_offset,
):
    seq_count, local_len, width = prompt_layer_input.shape
    resident_heads = value_projection.shape[1] // P_SIZE
    feature_cols = resident_heads * P_SIZE
    shard_count = lax.axis_size("sp")
    rows_here = P_SIZE // shard_count
    shard_index = lax.axis_index("sp")
    leading_head = lax.axis_index("tp") * resident_heads
    group_index = leading_head // (HEADS // GROUPS)
    row_first = shard_index * rows_here
    in_cols = lax.dynamic_slice_in_dim(key_projection, group_index * STATE, STATE, 1)
    out_cols = lax.dynamic_slice_in_dim(query_projection, group_index * STATE, STATE, 1)
    weights_here = jnp.concatenate([value_projection, in_cols, out_cols], axis=1)
    step_cols = lax.dynamic_slice_in_dim(step_projection, leading_head, resident_heads, 1)
    kernel = jnp.concatenate(
        [
            lax.dynamic_slice_in_dim(value_filter_taps, leading_head * P_SIZE, feature_cols, 1),
            lax.dynamic_slice_in_dim(key_filter_taps, group_index * STATE, STATE, 1),
            lax.dynamic_slice_in_dim(query_filter_taps, group_index * STATE, STATE, 1),
        ],
        axis=1,
    ).astype(jnp.float32)
    head_decay_speed = jnp.exp(
        lax.dynamic_slice_in_dim(head_decay_logarithm, leading_head, resident_heads, 0)
    )
    bias_here = lax.dynamic_slice_in_dim(step_size_bias, leading_head, resident_heads, 0)
    skip_here = lax.dynamic_slice_in_dim(direct_path_weight, leading_head, resident_heads, 0)
    gain_here = lax.dynamic_slice(
        gated_norm_gain, (leading_head, row_first), (resident_heads, rows_here)
    )
    token_rows = prompt_layer_input.reshape(seq_count * local_len, width)
    projected = jnp.dot(token_rows, weights_here, preferred_element_type=jnp.float32).astype(
        jnp.bfloat16
    )
    projected = projected.reshape(seq_count, local_len, feature_cols + 2 * STATE)
    trailing = projected[:, local_len - (CONV - 1) :]
    before = shifted(trailing, "sp", 1)
    newest = broadcast(trailing, "sp", shard_count - 1)
    padded = jnp.concatenate([before, projected], axis=1)
    total = padded[:, 0:local_len].astype(jnp.float32) * kernel[0]
    for tap in range(1, CONV):
        total = total + padded[:, tap : tap + local_len].astype(jnp.float32) * kernel[tap]
    mixed = jax.nn.silu(total).astype(jnp.bfloat16)
    step_raw = jnp.dot(token_rows, step_cols, preferred_element_type=jnp.float32).astype(
        jnp.bfloat16
    )
    discrete_step = jax.nn.softplus(step_raw.astype(jnp.float32) + bias_here).reshape(
        seq_count, local_len, resident_heads
    )
    decay_spikes = lax.dynamic_slice_in_dim(position_decay_offset, leading_head, resident_heads, 2)
    logarithmic_decay = decay_spikes - head_decay_speed * discrete_step
    block_count = local_len // SPAN
    cumulative = jnp.cumsum(
        logarithmic_decay.reshape(seq_count, block_count, SPAN, resident_heads), axis=2
    )
    decay_weight = jnp.exp(cumulative[:, :, -1:] - cumulative) * discrete_step.reshape(
        seq_count, block_count, SPAN, resident_heads
    )
    head_input = mixed[:, :, :feature_cols].reshape(
        seq_count, block_count, SPAN, resident_heads, P_SIZE
    )
    weighted = (head_input.astype(jnp.float32) * decay_weight[..., None]).astype(jnp.bfloat16)
    in_map = mixed[:, :, feature_cols : feature_cols + STATE].reshape(
        seq_count, block_count, SPAN, STATE
    )
    block_state = jnp.einsum(
        "bcshp,bcsn->bchpn", weighted, in_map, preferred_element_type=jnp.float32
    )
    block_log = cumulative[:, :, -1]
    own_log = jnp.sum(block_log, axis=1)
    after_block = jnp.exp(own_log[:, None] - jnp.cumsum(block_log, axis=1))
    local_state = jnp.sum(after_block[..., None, None] * block_state, axis=1)
    later_log = prefix(own_log, "sp", jnp.add, jnp.zeros_like(own_log))
    scaled = jnp.exp(later_log)[:, :, None, None] * local_state
    own_rows = lax.psum_scatter(scaled, "sp", scatter_dimension=2, tiled=True)
    state_cache = own_rows.astype(jnp.bfloat16)
    new_raw = jnp.dot(next_token_input, weights_here, preferred_element_type=jnp.float32).astype(
        jnp.bfloat16
    )
    new_step = jnp.dot(next_token_input, step_cols, preferred_element_type=jnp.float32).astype(
        jnp.bfloat16
    )
    new_gate = jnp.dot(
        next_token_input, output_gate_matrix, preferred_element_type=jnp.float32
    ).astype(jnp.bfloat16)
    window = jnp.concatenate([newest, new_raw[:, None]], axis=1)
    new_mixed = jax.nn.silu(jnp.sum(window.astype(jnp.float32) * kernel[None], axis=1)).astype(
        jnp.bfloat16
    )
    new_input = lax.dynamic_slice_in_dim(
        new_mixed[:, :feature_cols].reshape(seq_count, resident_heads, P_SIZE),
        row_first,
        rows_here,
        2,
    ).astype(jnp.float32)
    new_in = new_mixed[:, feature_cols : feature_cols + STATE].astype(jnp.float32)
    new_out = new_mixed[:, feature_cols + STATE :].astype(jnp.float32)
    new_step_size = jax.nn.softplus(new_step.astype(jnp.float32) + bias_here)
    cache_values = lax.optimization_barrier(state_cache).astype(jnp.float32)
    new_state = (
        jnp.exp(-head_decay_speed * new_step_size)[:, :, None, None] * cache_values
        + (new_step_size[:, :, None] * new_input)[..., None] * new_in[:, None, None, :]
    )
    readout = (
        jnp.sum(new_state * new_out[:, None, None, :], axis=-1)
        + skip_here[None, :, None] * new_input
    )
    gate_rows = lax.dynamic_slice_in_dim(
        new_gate.reshape(seq_count, resident_heads, P_SIZE), row_first, rows_here, 2
    )
    gated = readout * jax.nn.silu(gate_rows.astype(jnp.float32))
    squares = lax.psum(jnp.sum(gated * gated, axis=(1, 2)), ("sp", "tp"))
    scale = lax.rsqrt(squares / (HEADS * P_SIZE) + epsilon)
    first_read = (gated * scale[:, None, None] * gain_here[None]).astype(jnp.bfloat16)
    return (state_cache, first_read)


F32, BF16 = jnp.float32, jnp.bfloat16
MESH = pl.DeviceIdType.MESH
EXACT = lax.Precision.HIGHEST


def exact_dot(a, b, dims=((1,), (0,))):
    return lax.dot_general(a, b, (dims, ((), ())), precision=EXACT, preferred_element_type=F32)


def softplus(v):
    return jnp.maximum(v, 0.0) + jnp.log1p(jnp.exp(-jnp.abs(v)))


def silu(v):
    return v / (1.0 + jnp.exp(-v))


def ones_where(shape, test, dtype=F32):
    rows = lax.broadcasted_iota(jnp.int32, shape, 0)
    cols = lax.broadcasted_iota(jnp.int32, shape, 1)
    return jnp.where(test(rows, cols), 1.0, 0.0).astype(dtype)


def mixer_kernel(
    dims,
    x_hbm,
    next_ref,
    wv_hbm,
    wg_hbm,
    wk_hbm,
    wq_hbm,
    ws_hbm,
    tv_ref,
    tk_ref,
    tq_ref,
    bias_ref,
    speed_ref,
    skip_ref,
    gain_ref,
    off_hbm,
    cache_ref,
    read_ref,
    xbuf,
    edge,
    wall,
    ws,
    wg,
    off,
    taps,
    pad,
    wsplit,
    halo_out,
    halo_in,
    newest,
    heads_t,
    decay,
    log_own,
    log_out,
    log_in,
    own,
    from_left,
    from_right,
    sq_out,
    sq_in,
    expand,
    load_sem,
    x_sem,
    halo_sem,
    new_sem,
    st_send,
    st_recv,
    log_send,
    log_recv,
    sq_send,
    sq_recv,
):
    n, m, S, L, heads, R, G = dims
    F = heads * P_SIZE
    C = F + STATE
    RH = heads * R
    SP = 16
    steps = S // G
    lead_steps = min(LEAD, steps)
    me, tp = lax.axis_index("sp"), lax.axis_index("tp")
    lead = pl.multiple_of(tp * heads, 8)
    group = lax.div(lead, HEADS // GROUPS)
    fcol = pl.multiple_of(tp * F, 128)
    gcol = pl.multiple_of(group * STATE, 128)

    def load(src, dst, k):
        c = pltpu.make_async_copy(src, dst, load_sem.at[k])
        c.start()
        return c

    def load_x(g):
        return pltpu.make_async_copy(
            x_hbm.at[pl.ds(g * G, G)], xbuf.at[pl.ds(g * G, G)], x_sem.at[g]
        )

    peers = [(a, b) for a in range(n) for b in range(m) if (a, b) != (0, 0)]

    def at(a, b=0):
        return {"sp": lax.rem(me + a, n), "tp": lax.rem(tp + b, m)}

    barrier = pltpu.get_barrier_semaphore()
    for a, b in peers:
        pl.semaphore_signal(barrier, inc=1, device_id=at(a, b), device_id_type=MESH)

    first = [
        load(ws_hbm.at[pl.ds(lead, heads), :], ws, 0),
        load(x_hbm.at[:, pl.ds(L - 16, 16)], edge.at[pl.ds(0, S)], 1),
        load(wk_hbm.at[:, pl.ds(gcol, STATE)], wall.at[:, pl.ds(128 + F, STATE)], 2),
        load(wq_hbm.at[:, pl.ds(gcol, STATE)], wall.at[:, pl.ds(128 + C, STATE)], 3),
        load(wv_hbm, wall.at[:, pl.ds(128, F)], 4),
    ]

    taps[:, 0:F] = tv_ref[:, pl.ds(fcol, F)].astype(F32)
    taps[:, F:C] = tk_ref[:, pl.ds(gcol, STATE)].astype(F32)
    taps[:, C : C + STATE] = tq_ref[:, pl.ds(gcol, STATE)].astype(F32)
    edge[S] = jnp.zeros(edge.shape[1:], BF16)
    edge[S, 0:S, :] = next_ref[...]
    head_of = ones_where((heads, F), lambda i, c: i == lax.div(c, P_SIZE))
    expand[...] = jnp.concatenate([head_of, head_of], axis=0).astype(BF16)
    bias = bias_ref[...]
    speed = jnp.exp(speed_ref[...])
    square = jnp.zeros((128, 128 - HEADS), F32)

    def columns(row, k):
        full = jnp.concatenate([jnp.broadcast_to(row, (128, HEADS)), square], axis=1)
        heads_t[k] = full.T[0:HEADS]
        return heads_t[k, pl.ds(lead, heads), :]

    bias_t, speed_t = columns(bias, 0), columns(speed, 1)

    @pl.when(me == 0)
    def _():
        from_left[:, 0] = jnp.zeros((S, RH, STATE), BF16)

    @pl.when(me == n - 1)
    def _():
        from_right[:, n - 1] = jnp.zeros((S, RH, STATE), BF16)
        log_in[...] = jnp.zeros_like(log_in)

    eye = ones_where((heads, 128), lambda i, c: i == c)
    later_ones = ones_where((L, L), lambda u, t: u > t, BF16)

    for c in first[1:4]:
        c.wait()
    load_x(0).start()
    first[4].wait()
    off_load = load(off_hbm.at[:, pl.ds(lead, heads), :], off, 5)
    rows = edge[...].reshape((S + 1) * 16, edge.shape[2])
    eproj = jnp.dot(rows, wall[:, 128:], preferred_element_type=F32).astype(BF16).astype(F32)
    e3 = eproj.reshape(S + 1, 16, C + STATE)
    new_raw = e3[S]
    tail_rows = halo_out.shape[1] - G * (CONV - 1)
    for g in range(steps):
        tails = [e3[g * G + q, 16 - (CONV - 1) :, 0:C] for q in range(G)]
        if tail_rows:
            tails.append(jnp.zeros((tail_rows, C), F32))
        halo_out[g] = jnp.concatenate(tails, axis=0).astype(BF16)

    for g in range(1, steps):
        load_x(g).start()
    gate_load = load(wg_hbm, wg, 6)
    pl.semaphore_wait(barrier, len(peers))

    def halo_copy(k):
        here = pl.ds(0, 1) if k == 0 else pl.ds(1, steps - 1)
        return pltpu.make_async_remote_copy(
            halo_out.at[here],
            halo_in.at[here],
            halo_sem.at[0, k],
            halo_sem.at[1, k],
            device_id=at(1),
            device_id_type=MESH,
        )

    halo_parts = range(2 if steps > 1 else 1)

    @pl.when(me < n - 1)
    def _():
        for k in halo_parts:
            halo_copy(k).start()

    first[0].wait()
    wall[:, 0:128] = jnp.concatenate(
        [ws[...], jnp.zeros((128 - heads, ws.shape[1]), BF16)], axis=0
    ).T

    def newest_copy():
        return pltpu.make_async_remote_copy(
            newest,
            newest,
            new_sem.at[0],
            new_sem.at[1],
            device_id=at(n - 1),
            device_id_type=MESH,
        )

    def span(s, right, far):
        if right:
            return (s + 2, n) if far else (s + 1, s + 2)
        return (0, s - 1) if far else (s - 1, s)

    def flow(p, s, right, far):
        lo, hi = span(s, right, far)
        if not (0 <= lo < hi <= n):
            return None
        k = 2 * int(right) + int(far)
        here = (p, pl.ds(lo, hi - lo))
        return pltpu.make_async_remote_copy(
            own.at[here],
            (from_left if right else from_right).at[here],
            st_send.at[k, p],
            st_recv.at[k, p],
            device_id=at(1 if right else n - 1),
            device_id_type=MESH,
        )

    def begin(p, s, right, far):
        c = flow(p, s, right, far)
        if c is not None:
            c.start()

    def log_copy(p):
        return pltpu.make_async_remote_copy(
            log_out.at[p],
            log_in.at[p],
            log_send.at[p],
            log_recv.at[p],
            device_id=at(n - 1),
            device_id_type=MESH,
        )

    def project(g):
        load_x(g).wait()
        slot = lax.rem(g, lead_steps)
        xg = xbuf[pl.ds(g * G, G)].reshape(G * L, xbuf.shape[2])
        acc = jnp.dot(xg, wall[:, 0 : 128 + C], preferred_element_type=F32).astype(BF16).astype(F32)
        for q in range(G):
            p = g * G + q
            raw = acc[q * L : (q + 1) * L]
            pad[slot, q, 8 : 8 + L, :] = raw[:, 128:]
            dt = softplus(raw[:, 0:128].T[0:heads] + bias_t)
            ld = off[p] - speed_t * dt
            a = ld.astype(BF16).astype(F32)
            b = (ld - a).astype(BF16).astype(F32)
            parts = jnp.concatenate([a, b, ld - a - b, jnp.zeros_like(a)], axis=0).astype(BF16)
            sums = jnp.dot(parts, later_ones, preferred_element_type=F32)
            suffix = sums[0:heads] + sums[heads : 2 * heads] + sums[2 * heads : 3 * heads]
            whole = jnp.broadcast_to(suffix[:, 0:1] + ld[:, 0:1], (heads, 128))
            decay[p] = jnp.exp(whole)
            log_own[p] = jnp.sum(whole * eye, axis=0, keepdims=True)
            w = dt * jnp.exp(suffix)
            hi = w.astype(BF16).astype(F32)
            wsplit[slot, q] = jnp.concatenate([hi, w - hi], axis=0).astype(BF16)

    depth, behind = min(DEPTH, S), min(BEHIND, S)

    def feed(p, s, right):
        if flow(0, s, right, True) is not None:

            @pl.when((p >= depth) & (p < S + depth))
            def _():
                flow(p - depth, s, right, True).wait_send()

            @pl.when(p < S)
            def _():
                begin(p, s, right, True)

        @pl.when(p >= depth + behind)
        def _():
            flow(p - depth - behind, s, right, False).wait_send()

        @pl.when(p >= behind)
        def _():
            begin(p - behind, s, right, False)

    def feed_rest(s, right):
        def one(p, carry):
            feed(p, s, right)
            return carry

        lax.fori_loop(S, S + behind, one, 0)

    def states(g):
        slot = lax.rem(g, lead_steps)
        before = halo_in[g].astype(F32)
        for q in range(G):
            p = g * G + q
            pad[slot, q, 8 - (CONV - 1) : 8, :] = before[q * (CONV - 1) : (q + 1) * (CONV - 1)]
            wide = lax.dot_general(
                wsplit[slot, q],
                expand[...],
                (((0,), (0,)), ((), ())),
                preferred_element_type=F32,
            )

            def mixed(c):
                s = slice(c, c + 128)
                t = pad[slot, q, 8 - (CONV - 1) : 8 - (CONV - 1) + L, s] * taps[0:1, s]
                for j in range(1, CONV):
                    r = 8 - (CONV - 1) + j
                    t = t + pad[slot, q, r : r + L, s] * taps[j : j + 1, s]
                return silu(t).astype(BF16)

            in_map = mixed(F)
            for c in range(0, F, 128):
                weighted = (mixed(c).astype(F32) * wide[:, c : c + 128]).astype(BF16)
                share = lax.dot_general(
                    weighted, in_map, (((0,), (0,)), ((), ())), preferred_element_type=F32
                ).astype(BF16)
                for hh in range(128 // P_SIZE):
                    h = c // P_SIZE + hh
                    for d in range(n):
                        b = hh * P_SIZE + d * R
                        own[p, d, h * R : (h + 1) * R, :] = share[b : b + R]

            @pl.when(me == 0)
            def _(p=p):
                feed(p, 0, True)

            @pl.when(me == n - 1)
            def _(p=p):
                log_out[p] = log_own[p]
                log_copy(p).start()
                feed(p, n - 1, False)

    def later_factor(p):
        row = jnp.sum(eye * log_in[p], axis=1, keepdims=True)
        return jnp.exp(jnp.broadcast_to(row, (heads, 128)))

    def sum_right(p, s):
        flow(p, s - 1, True, True).wait_recv()
        factor = decay[p]
        for d in reversed(range(s + 1, n)):
            for h in range(heads):
                z = (p, d, slice(h * R, (h + 1) * R))
                got = from_left[z].astype(F32) * factor[h : h + 1, :]
                own[z] = (own[z].astype(F32) + got).astype(BF16)
        begin(p, s, True, True)
        begin(p, s, True, False)

    def sum_left(p, s):
        log_copy(p).wait_recv()
        log_out[p] = log_in[p] + log_own[p]
        log_copy(p).start()
        flow(p, s + 1, False, True).wait_recv()
        factor = later_factor(p)
        for d in range(s):
            for h in range(heads):
                z = (p, d, slice(h * R, (h + 1) * R))
                mine = own[z].astype(F32) * factor[h : h + 1, :]
                own[z] = (from_right[z].astype(F32) + mine).astype(BF16)
        begin(p, s, False, True)
        begin(p, s, False, False)

    def relay(g, outer):
        for s in range(1, n - 1):

            @pl.when(me == s)
            def _(s=s):
                for q in range(G):
                    if outer == (s < n - 1 - s):
                        sum_right(g * G + q, s)
                    else:
                        sum_left(g * G + q, s)

    off_load.wait()
    lax.fori_loop(0, lead_steps, lambda g, carry: (project(g), carry)[1], 0)
    @pl.when(me == n - 1)
    def _():
        total = jnp.zeros((S, C + STATE), F32)
        for j in range(CONV - 1):
            row = 16 - (CONV - 1) + j
            total = total + e3[0:S, row, :] * taps[j : j + 1, :]
        newest[...] = jnp.zeros_like(newest)
        newest[0:S, :] = total
        newest_copy().start()

    @pl.when(me == 0)
    def _():
        halo_in[...] = jnp.zeros_like(halo_in)

    @pl.when(me > 0)
    def _():
        halo_copy(0).wait_recv()

    relay_lag = min(RELAY_LAG, steps)

    def step(g, carry):
        if steps > 1:

            @pl.when((g == 1) & (me > 0))
            def _():
                halo_copy(1).wait_recv()

        states(g)

        @pl.when(g + lead_steps < steps)
        def _():
            project(g + lead_steps)

        if n > 2:

            for s in range(1, n - 1):

                @pl.when((g == min(FORWARD_AT * (n - 1 - s), steps - 1)) & (me == s))
                def _():
                    newest_copy().wait_recv()
                    newest_copy().start()

        @pl.when(g >= relay_lag)
        def _():
            relay(g - relay_lag, True)

        @pl.when(g >= relay_lag + 1)
        def _():
            relay(g - relay_lag - 1, False)

        return carry

    lax.fori_loop(0, steps, step, 0)
    head_cols = ones_where((HEADS, RH), lambda i, l: i == lead + lax.div(l, R))
    local_cols = ones_where((128, RH), lambda i, l: i == lax.div(l, R))
    local = ones_where((HEADS, 128), lambda i, c: (i == lead + c) & (c < heads))
    pick = ones_where(
        (F, RH), lambda c, l: c == lax.div(l, R) * P_SIZE + me * R + lax.rem(l, R), BF16
    )
    row_pick = ones_where((P_SIZE, RH), lambda c, l: c == me * R + lax.rem(l, R))
    gate_load.wait()
    gate = jnp.dot(edge[S], wg[...], preferred_element_type=F32).astype(BF16)
    gate_here = silu(jnp.dot(gate, pick, preferred_element_type=F32))
    gain_here = jnp.sum(exact_dot(gain_ref[...], row_pick) * head_cols, axis=0, keepdims=True)
    skip_here = exact_dot(skip_ref[...], head_cols)
    new_step = jnp.dot(edge[S], wall[:, 0:128], preferred_element_type=F32).astype(BF16)
    new_dt = softplus(new_step.astype(F32) + exact_dot(bias, local))
    dt_here = exact_dot(new_dt, local_cols)
    keep_here = jnp.exp(-exact_dot(exact_dot(speed, local) * new_dt, local_cols))

    @pl.when(me == 0)
    def _():
        newest_copy().wait_recv()

    new_mixed = silu(newest[...] + new_raw * taps[CONV - 1 : CONV, :]).astype(BF16)
    new_input = jnp.dot(new_mixed[:, 0:F], pick, preferred_element_type=F32)
    new_in = new_mixed[:, F:C].astype(F32)
    new_out = new_mixed[:, C : C + STATE]
    both = jnp.sum(new_in * new_out.astype(F32), axis=1, keepdims=True)
    where_row = lax.broadcasted_iota(jnp.int32, (SP, RH), 0)

    @pl.when(me == 0)
    def _():
        feed_rest(0, True)

    @pl.when(me == n - 1)
    def _():
        feed_rest(n - 1, False)

    def finish(g, y):
        for s in range(n):

            @pl.when(me == s)
            def _(s=s):
                for q in range(G):
                    p = g * G + q
                    if s > 0:
                        flow(p, s - 1, True, False).wait_recv()
                    if s == 0:
                        log_copy(p).wait_recv()
                    if s < n - 1:
                        flow(p, s + 1, False, False).wait_recv()

        for q in range(G):
            p = g * G + q
            before, after = decay[p], later_factor(p)
            kept = []
            for h in range(heads):
                z = (p, me, slice(h * R, (h + 1) * R))
                t = own[z].astype(F32) + from_left[z].astype(F32) * before[h : h + 1, :]
                t = t * after[h : h + 1, :] + from_right[z].astype(F32)
                kept.append(t.astype(BF16))
            kept = jnp.concatenate(kept, axis=0)
            cache_ref[p] = kept
            part = lax.dot_general(
                new_out, kept, (((1,), (1,)), ((), ())), preferred_element_type=F32
            )
            y = jnp.where(where_row == p, part, y)
        return y

    for g in range(steps - relay_lag, steps):
        relay(g, True)
        if g > 0:
            relay(g - 1, False)
    relay(steps - 1, False)
    y = lax.fori_loop(0, steps, finish, jnp.zeros((SP, RH), F32))

    readout = keep_here * y + dt_here * new_input * both + skip_here * new_input
    gated = readout * gate_here
    square_sum = jnp.broadcast_to(jnp.sum(gated * gated, axis=1, keepdims=True), (SP, 128))
    diagonal = ones_where((SP, 128), lambda i, c: i == c)
    sq = jnp.sum(square_sum * diagonal, axis=0, keepdims=True)
    sq_out[...] = sq

    def sq_copy(i):
        a, b = peers[i]
        return pltpu.make_async_remote_copy(
            sq_out, sq_in.at[i], sq_send.at[i], sq_recv.at[i], device_id=at(a, b), device_id_type=MESH
        )

    for i in range(len(peers)):
        sq_copy(i).start()
    for s in range(n):

        @pl.when(me == s)
        def _(s=s):
            end = s in (0, n - 1)

            def sent(p, carry):
                for right in (False, True):
                    for far in (False, True):
                        c = flow(p, s, right, far)
                        if c is None:
                            continue
                        fed = p < S + min(0, behind - depth) if far else p < S - depth

                        @pl.when(jnp.logical_not(fed & end))
                        def _(c=c):
                            c.wait_send()

                if s > 0:
                    log_copy(p).wait_send()
                return carry

            lax.fori_loop(0, S, sent, 0)

    @pl.when(me < n - 1)
    def _():
        for k in halo_parts:
            halo_copy(k).wait_send()

    @pl.when(me > 0)
    def _():
        newest_copy().wait_send()

    for i in range(len(peers)):
        sq_copy(i).wait_recv()
        sq = sq + sq_in[i]
    mean = jnp.sum(diagonal * sq, axis=1, keepdims=True) / (HEADS * P_SIZE)
    scale = lax.rsqrt(mean + epsilon)
    read_ref[...] = (gated * scale * gain_here).astype(BF16)[0:S]

    for i in range(len(peers)):
        sq_copy(i).wait_send()


def on_chip(array):
    return pltpu.with_memory_space_constraint(array, pltpu.VMEM)


def emit_kernel(dims, cache_ref, read_ref, cache_hbm, out_ref, sem):
    heads, R = dims
    S, RH = read_ref.shape
    copy = pltpu.make_async_copy(cache_ref, cache_hbm, sem)
    copy.start()
    spread = ones_where((heads, RH), lambda h, l: h == lax.div(l, R))
    pick = ones_where((RH, R), lambda l, r: lax.rem(l, R) == r, BF16)
    value = read_ref[...].astype(F32)
    rows = jnp.concatenate([value[p : p + 1] * spread for p in range(S)], axis=0).astype(BF16)
    out = jnp.dot(rows, pick, preferred_element_type=F32)
    out_ref[...] = out.reshape(S, heads, R).astype(BF16)
    copy.wait()


LEAD, RELAY_LAG, FORWARD_AT = 1, 1, 2
DEPTH, BEHIND = 4, 8


def fused(*args):
    x, wv, wk = args[0], args[2], args[4]
    S, L, D = x.shape
    n, m = lax.axis_size("sp"), lax.axis_size("tp")
    F = wv.shape[1]
    heads = F // P_SIZE
    R = P_SIZE // n
    G = next(g for g in (2, 3, 1) if S % g == 0)
    steps = S // G
    slots = min(LEAD, steps)
    halo_rows = -(-G * (CONV - 1) // 8) * 8
    C, RH, SP = F + STATE, heads * R, 16
    dims = (n, m, S, L, heads, R, G)
    flat = list(args)
    for i in (10, 11, 12):
        flat[i] = args[i].reshape(1, HEADS)
    flat[6] = args[6].T
    flat[14] = jnp.swapaxes(args[14], 1, 2)
    hbm, vmem = pl.BlockSpec(memory_space=pl.ANY), pl.BlockSpec(memory_space=pltpu.VMEM)
    specs = [hbm, vmem, hbm, hbm, hbm, hbm, hbm] + [vmem] * 7 + [hbm]
    dma = pltpu.SemaphoreType.DMA
    cache, read = pl.pallas_call(
        lambda *refs: mixer_kernel(dims, *refs),
        out_shape=(
            pltpu.VMEM((S, RH, STATE), BF16),
            pltpu.VMEM((S, RH), BF16),
        ),
        in_specs=specs,
        out_specs=(vmem, vmem),
        scratch_shapes=[
            pltpu.VMEM((S, L, D), BF16),
            pltpu.VMEM((S + 1, 16, D), BF16),
            pltpu.VMEM((D, 128 + C + STATE), BF16),
            pltpu.VMEM((heads, D), BF16),
            pltpu.VMEM((D, F), BF16),
            pltpu.VMEM((S, heads, L), F32),
            pltpu.VMEM((CONV, C + STATE), F32),
            pltpu.VMEM((slots, G, 8 + L, C), F32),
            pltpu.VMEM((slots, G, 2 * heads, L), BF16),
            pltpu.VMEM((steps, halo_rows, C), BF16),
            pltpu.VMEM((steps, halo_rows, C), BF16),
            pltpu.VMEM((SP, C + STATE), F32),
            pltpu.VMEM((2, HEADS, 128), F32),
            pltpu.VMEM((S, heads, 128), F32),
            pltpu.VMEM((S, 1, 128), F32),
            pltpu.VMEM((S, 1, 128), F32),
            pltpu.VMEM((S, 1, 128), F32),
            pltpu.VMEM((S, n, RH, STATE), BF16),
            pltpu.VMEM((S, n, RH, STATE), BF16),
            pltpu.VMEM((S, n, RH, STATE), BF16),
            pltpu.VMEM((1, 128), F32),
            pltpu.VMEM((n * m - 1, 1, 128), F32),
            pltpu.VMEM((2 * heads, F), BF16),
            dma((7,)),
            dma((steps,)),
            dma((2, 2)),
            dma((2,)),
            dma((4, S)),
            dma((4, S)),
            dma((S,)),
            dma((S,)),
            dma((n * m,)),
            dma((n * m,)),
        ],
        compiler_params=pltpu.CompilerParams(
            collective_id=0, has_side_effects=True, vmem_limit_bytes=56 * 1024 * 1024
        ),
    )(*flat)
    cache, read = pl.pallas_call(
        lambda *refs: emit_kernel((heads, R), *refs),
        out_shape=(
            jax.ShapeDtypeStruct((S, RH, STATE), BF16),
            jax.ShapeDtypeStruct((S, heads, R), BF16),
        ),
        in_specs=[vmem, vmem],
        out_specs=(pl.BlockSpec(memory_space=pltpu.HBM), vmem),
        scratch_shapes=[dma],
    )(on_chip(cache), on_chip(read))
    return cache.reshape(S, heads, R, STATE), read


def fits(n, m, shapes):
    (S, L), F = shapes
    heads, R = F // P_SIZE, P_SIZE // n
    return (
        n > 1
        and F % 128 == 0
        and heads % 8 == 0
        and R % 16 == 0
        and (heads * R) % 128 == 0
        and S <= 16
        and L % 16 == 0
        and L == 128
        and (HEADS // GROUPS) % heads == 0
    )


def part(*args):
    shapes = (args[0].shape[:2], args[2].shape[1])
    if fits(lax.axis_size("sp"), lax.axis_size("tp"), shapes):
        return fused(*args)
    return shards(*args)


def solution(mesh):
    in_specs = (
        P("grp", "sp", None),
        P("grp", None),
        P(None, "tp"),
        P(None, "tp"),
        P(),
        P(),
        P(),
        P(),
        P(),
        P(),
        P(),
        P(),
        P(),
        P(),
        P("grp", "sp", None),
    )
    out_specs = (P("grp", "tp", "sp", None), P("grp", "tp", "sp"))
    return jax.shard_map(part, mesh=mesh, in_specs=in_specs, out_specs=out_specs, check_vma=False)
```

```python
import jax
import jax.numpy as jnp
from jax import lax
from jax.experimental import pallas as pl
from jax.experimental.pallas import tpu as pltpu
from jax.sharding import PartitionSpec as P

HEADS = 32
P_SIZE = 64
GROUPS = 2
STATE = 128
CONV = 4
SPAN = 64


epsilon = 1e-06


def shifted(block, axis, distance):
    devices = range(lax.axis_size(axis))
    route = [(i - distance, i) for i in devices if i - distance in devices]
    return lax.ppermute(block, axis, route)


def broadcast(value, axis, source):
    kept = jnp.where(lax.axis_index(axis) == source, value, 0).astype(value.dtype)
    return lax.psum(kept, axis)


def prefix(shard, axis, combine, identity):
    length, here = (lax.axis_size(axis), lax.axis_index(axis))
    everything = lax.all_gather(shard, axis)
    start = jnp.broadcast_to(jnp.asarray(identity, shard.dtype), shard.shape)

    def lap(k, before):
        at = length - 1 - k
        reached = at > here
        new = combine(before, everything[at])
        return jnp.where(reached, new, before)

    return lax.fori_loop(0, length, lap, start)


def shards(
    prompt_layer_input,
    next_token_input,
    value_projection,
    output_gate_matrix,
    key_projection,
    query_projection,
    step_projection,
    value_filter_taps,
    key_filter_taps,
    query_filter_taps,
    step_size_bias,
    head_decay_logarithm,
    direct_path_weight,
    gated_norm_gain,
    position_decay_offset,
):
    seq_count, local_len, width = prompt_layer_input.shape
    resident_heads = value_projection.shape[1] // P_SIZE
    feature_cols = resident_heads * P_SIZE
    shard_count = lax.axis_size("sp")
    rows_here = P_SIZE // shard_count
    shard_index = lax.axis_index("sp")
    leading_head = lax.axis_index("tp") * resident_heads
    group_index = leading_head // (HEADS // GROUPS)
    row_first = shard_index * rows_here
    in_cols = lax.dynamic_slice_in_dim(key_projection, group_index * STATE, STATE, 1)
    out_cols = lax.dynamic_slice_in_dim(query_projection, group_index * STATE, STATE, 1)
    weights_here = jnp.concatenate([value_projection, in_cols, out_cols], axis=1)
    step_cols = lax.dynamic_slice_in_dim(step_projection, leading_head, resident_heads, 1)
    kernel = jnp.concatenate(
        [
            lax.dynamic_slice_in_dim(value_filter_taps, leading_head * P_SIZE, feature_cols, 1),
            lax.dynamic_slice_in_dim(key_filter_taps, group_index * STATE, STATE, 1),
            lax.dynamic_slice_in_dim(query_filter_taps, group_index * STATE, STATE, 1),
        ],
        axis=1,
    ).astype(jnp.float32)
    head_decay_speed = jnp.exp(
        lax.dynamic_slice_in_dim(head_decay_logarithm, leading_head, resident_heads, 0)
    )
    bias_here = lax.dynamic_slice_in_dim(step_size_bias, leading_head, resident_heads, 0)
    skip_here = lax.dynamic_slice_in_dim(direct_path_weight, leading_head, resident_heads, 0)
    gain_here = lax.dynamic_slice(
        gated_norm_gain, (leading_head, row_first), (resident_heads, rows_here)
    )
    token_rows = prompt_layer_input.reshape(seq_count * local_len, width)
    projected = jnp.dot(token_rows, weights_here, preferred_element_type=jnp.float32).astype(
        jnp.bfloat16
    )
    projected = projected.reshape(seq_count, local_len, feature_cols + 2 * STATE)
    trailing = projected[:, local_len - (CONV - 1) :]
    before = shifted(trailing, "sp", 1)
    newest = broadcast(trailing, "sp", shard_count - 1)
    padded = jnp.concatenate([before, projected], axis=1)
    total = padded[:, 0:local_len].astype(jnp.float32) * kernel[0]
    for tap in range(1, CONV):
        total = total + padded[:, tap : tap + local_len].astype(jnp.float32) * kernel[tap]
    mixed = jax.nn.silu(total).astype(jnp.bfloat16)
    step_raw = jnp.dot(token_rows, step_cols, preferred_element_type=jnp.float32).astype(
        jnp.bfloat16
    )
    discrete_step = jax.nn.softplus(step_raw.astype(jnp.float32) + bias_here).reshape(
        seq_count, local_len, resident_heads
    )
    decay_spikes = lax.dynamic_slice_in_dim(position_decay_offset, leading_head, resident_heads, 2)
    logarithmic_decay = decay_spikes - head_decay_speed * discrete_step
    block_count = local_len // SPAN
    cumulative = jnp.cumsum(
        logarithmic_decay.reshape(seq_count, block_count, SPAN, resident_heads), axis=2
    )
    decay_weight = jnp.exp(cumulative[:, :, -1:] - cumulative) * discrete_step.reshape(
        seq_count, block_count, SPAN, resident_heads
    )
    head_input = mixed[:, :, :feature_cols].reshape(
        seq_count, block_count, SPAN, resident_heads, P_SIZE
    )
    weighted = (head_input.astype(jnp.float32) * decay_weight[..., None]).astype(jnp.bfloat16)
    in_map = mixed[:, :, feature_cols : feature_cols + STATE].reshape(
        seq_count, block_count, SPAN, STATE
    )
    block_state = jnp.einsum(
        "bcshp,bcsn->bchpn", weighted, in_map, preferred_element_type=jnp.float32
    )
    block_log = cumulative[:, :, -1]
    own_log = jnp.sum(block_log, axis=1)
    after_block = jnp.exp(own_log[:, None] - jnp.cumsum(block_log, axis=1))
    local_state = jnp.sum(after_block[..., None, None] * block_state, axis=1)
    later_log = prefix(own_log, "sp", jnp.add, jnp.zeros_like(own_log))
    scaled = jnp.exp(later_log)[:, :, None, None] * local_state
    own_rows = lax.psum_scatter(scaled, "sp", scatter_dimension=2, tiled=True)
    state_cache = own_rows.astype(jnp.bfloat16)
    new_raw = jnp.dot(next_token_input, weights_here, preferred_element_type=jnp.float32).astype(
        jnp.bfloat16
    )
    new_step = jnp.dot(next_token_input, step_cols, preferred_element_type=jnp.float32).astype(
        jnp.bfloat16
    )
    new_gate = jnp.dot(
        next_token_input, output_gate_matrix, preferred_element_type=jnp.float32
    ).astype(jnp.bfloat16)
    window = jnp.concatenate([newest, new_raw[:, None]], axis=1)
    new_mixed = jax.nn.silu(jnp.sum(window.astype(jnp.float32) * kernel[None], axis=1)).astype(
        jnp.bfloat16
    )
    new_input = lax.dynamic_slice_in_dim(
        new_mixed[:, :feature_cols].reshape(seq_count, resident_heads, P_SIZE),
        row_first,
        rows_here,
        2,
    ).astype(jnp.float32)
    new_in = new_mixed[:, feature_cols : feature_cols + STATE].astype(jnp.float32)
    new_out = new_mixed[:, feature_cols + STATE :].astype(jnp.float32)
    new_step_size = jax.nn.softplus(new_step.astype(jnp.float32) + bias_here)
    cache_values = lax.optimization_barrier(state_cache).astype(jnp.float32)
    new_state = (
        jnp.exp(-head_decay_speed * new_step_size)[:, :, None, None] * cache_values
        + (new_step_size[:, :, None] * new_input)[..., None] * new_in[:, None, None, :]
    )
    readout = (
        jnp.sum(new_state * new_out[:, None, None, :], axis=-1)
        + skip_here[None, :, None] * new_input
    )
    gate_rows = lax.dynamic_slice_in_dim(
        new_gate.reshape(seq_count, resident_heads, P_SIZE), row_first, rows_here, 2
    )
    gated = readout * jax.nn.silu(gate_rows.astype(jnp.float32))
    squares = lax.psum(jnp.sum(gated * gated, axis=(1, 2)), ("sp", "tp"))
    scale = lax.rsqrt(squares / (HEADS * P_SIZE) + epsilon)
    first_read = (gated * scale[:, None, None] * gain_here[None]).astype(jnp.bfloat16)
    return (state_cache, first_read)


F32, BF16 = jnp.float32, jnp.bfloat16
MESH = pl.DeviceIdType.MESH
EXACT = lax.Precision.HIGHEST


def exact_dot(a, b, dims=((1,), (0,))):
    return lax.dot_general(a, b, (dims, ((), ())), precision=EXACT, preferred_element_type=F32)


def softplus(v):
    return jnp.maximum(v, 0.0) + jnp.log1p(jnp.exp(-jnp.abs(v)))


def silu(v):
    return v / (1.0 + jnp.exp(-v))


def ones_where(shape, test, dtype=F32):
    rows = lax.broadcasted_iota(jnp.int32, shape, 0)
    cols = lax.broadcasted_iota(jnp.int32, shape, 1)
    return jnp.where(test(rows, cols), 1.0, 0.0).astype(dtype)


def mixer_kernel(
    dims,
    x_hbm,
    next_hbm,
    wv_hbm,
    wg_hbm,
    wk_hbm,
    wq_hbm,
    ws_hbm,
    tv_hbm,
    tk_hbm,
    tq_hbm,
    bias_hbm,
    speed_hbm,
    skip_hbm,
    gain_hbm,
    off_hbm,
    cache_ref,
    read_ref,
    next_ref,
    tv_ref,
    tk_ref,
    tq_ref,
    bias_ref,
    speed_ref,
    skip_ref,
    gain_ref,
    xbuf,
    edge,
    wall,
    ws,
    wg,
    off,
    taps,
    pad,
    wsplit,
    halo_out,
    halo_in,
    newest,
    heads_t,
    decay,
    log_own,
    log_out,
    log_in,
    own,
    from_left,
    from_right,
    sq_out,
    sq_in,
    expand,
    load_sem,
    x_sem,
    halo_sem,
    new_sem,
    st_send,
    st_recv,
    near_recv,
    log_send,
    log_recv,
    sq_sem,
):
    n, m, S, L, heads, R, G = dims
    F = heads * P_SIZE
    C = F + STATE
    RH = heads * R
    SP = 16
    steps = S // G
    lead_steps = min(LEAD, steps)
    me, tp = lax.axis_index("sp"), lax.axis_index("tp")
    lead = pl.multiple_of(tp * heads, 8)
    group = lax.div(lead, HEADS // GROUPS)
    fcol = pl.multiple_of(tp * F, 128)
    gcol = pl.multiple_of(group * STATE, 128)

    def load(src, dst, k):
        c = pltpu.make_async_copy(src, dst, load_sem.at[k])
        c.start()
        return c

    def load_x(k):
        here = pl.ds(0, G) if k == 0 else pl.ds(G, S - G)
        return pltpu.make_async_copy(x_hbm.at[here], xbuf.at[here], x_sem.at[k])

    first = [
        load(ws_hbm.at[pl.ds(lead, heads), :], ws, 0),
        load(x_hbm.at[:, pl.ds(L - 16, 16)], edge.at[pl.ds(0, S)], 1),
        load(wk_hbm.at[:, pl.ds(gcol, STATE)], wall.at[:, pl.ds(128 + F, STATE)], 2),
        load(wq_hbm.at[:, pl.ds(gcol, STATE)], wall.at[:, pl.ds(128 + C, STATE)], 3),
    ]
    strips = 2 if F % 512 == 0 else 1
    width = F // strips
    first += [
        load(
            wv_hbm.at[:, pl.ds(k * width, width)],
            wall.at[:, pl.ds(128 + k * width, width)],
            4 + k,
        )
        for k in range(strips)
    ]
    small = [
        load(a, b, 8 + k)
        for k, (a, b) in enumerate(
            [
                (next_hbm, next_ref),
                (tv_hbm, tv_ref),
                (tk_hbm, tk_ref),
                (tq_hbm, tq_ref),
                (bias_hbm, bias_ref),
                (speed_hbm, speed_ref),
                (skip_hbm, skip_ref),
                (gain_hbm, gain_ref),
            ]
        )
    ]

    peers = [(a, b) for a in range(n) for b in range(m) if (a, b) != (0, 0)]

    def at(a, b=0):
        return {"sp": lax.rem(me + a, n), "tp": lax.rem(tp + b, m)}

    barrier = pltpu.get_barrier_semaphore()
    for a, b in peers:
        pl.semaphore_signal(barrier, inc=1, device_id=at(a, b), device_id_type=MESH)

    head_of = ones_where((heads, F), lambda i, c: i == lax.div(c, P_SIZE))
    expand[...] = jnp.concatenate([head_of, head_of], axis=0).astype(BF16)
    @pl.when(me == 0)
    def _():
        from_left[:, 0] = jnp.zeros((S, RH, STATE), BF16)

    @pl.when(me == n - 1)
    def _():
        from_right[:, n - 1] = jnp.zeros((S, RH, STATE), BF16)
        log_in[...] = jnp.zeros_like(log_in)

    eye = ones_where((heads, 128), lambda i, c: i == c)
    later_ones = ones_where((L, L), lambda u, t: u > t, BF16)

    for c in small:
        c.wait()
    taps[:, 0:F] = tv_ref[:, pl.ds(fcol, F)].astype(F32)
    taps[:, F:C] = tk_ref[:, pl.ds(gcol, STATE)].astype(F32)
    taps[:, C : C + STATE] = tq_ref[:, pl.ds(gcol, STATE)].astype(F32)
    edge[S] = jnp.zeros(edge.shape[1:], BF16)
    edge[S, 0:S, :] = next_ref[...]
    bias = bias_ref[...]
    speed = jnp.exp(speed_ref[...])
    square = jnp.zeros((128, 128 - HEADS), F32)

    def columns(row, k):
        full = jnp.concatenate([jnp.broadcast_to(row, (128, HEADS)), square], axis=1)
        heads_t[k] = full.T[0:HEADS]
        return heads_t[k, pl.ds(lead, heads), :]

    bias_t, speed_t = columns(bias, 0), columns(speed, 1)

    for c in first[1:4]:
        c.wait()
    load_x(0).start()
    off_load = load(off_hbm.at[:, pl.ds(lead, heads), :], off, 6)
    rows = edge[...].reshape((S + 1) * 16, edge.shape[2])
    halo_out[...] = jnp.zeros_like(halo_out)
    parts = {}

    def edges(a, b):
        part = jnp.dot(rows, wall[:, 128 + a : 128 + b], preferred_element_type=F32)
        parts[a] = part.astype(BF16).astype(F32).reshape(S + 1, 16, b - a)
        tails(a, range(G))

    def tails(a, prompts):
        c = min(a + parts[a].shape[2], C)
        for p in prompts:
            r = p % G * (CONV - 1)
            tail = parts[a][p, 16 - (CONV - 1) :, 0 : c - a]
            halo_out[p // G, r : r + CONV - 1, a:c] = tail.astype(BF16)

    edges(F, C + STATE)
    for k in range(strips):
        first[4 + k].wait()
        edges(k * width, (k + 1) * width)
    if steps > 1:
        load_x(1).start()
    gate_load = load(wg_hbm, wg, 7)
    pl.semaphore_wait(barrier, len(peers))

    def halo_copy(k):
        here = pl.ds(0, 1) if k == 0 else pl.ds(1, steps - 1)
        return pltpu.make_async_remote_copy(
            halo_out.at[here],
            halo_in.at[here],
            halo_sem.at[0, k],
            halo_sem.at[1, k],
            device_id=at(1),
            device_id_type=MESH,
        )

    halo_parts = range(2 if steps > 1 else 1)

    @pl.when(me < n - 1)
    def _():
        halo_copy(0).start()

    for a in parts:
        tails(a, range(G, S))

    @pl.when(me < n - 1)
    def _():
        for k in halo_parts[1:]:
            halo_copy(k).start()

    def newest_copy():
        return pltpu.make_async_remote_copy(
            newest,
            newest,
            new_sem.at[0],
            new_sem.at[1],
            device_id=at(n - 1),
            device_id_type=MESH,
        )

    order = sorted(parts)
    last = 16 - (CONV - 1)

    @pl.when(me == n - 1)
    def _():
        newest[...] = jnp.zeros_like(newest)
        for a in order:
            b = a + parts[a].shape[2]
            newest[0:S, a:b] = sum(
                parts[a][0:S, last + j, :] * taps[j : j + 1, a:b] for j in range(CONV - 1)
            )
        newest_copy().start()

    new_raw = jnp.concatenate([parts[a][S] for a in order], axis=1)
    first[0].wait()
    wall[:, 0:128] = jnp.concatenate(
        [ws[...], jnp.zeros((128 - heads, ws.shape[1]), BF16)], axis=0
    ).T

    def span(s, right, far):
        if right:
            return (s + 2, n) if far else (s + 1, s + 2)
        return (0, s - 1) if far else (s - 1, s)

    def is_end(s, right):
        return s == (0 if right else n - 1)

    def kinds(s, right):
        if not 0 <= (s + 1 if right else s - 1) < n:
            return ()
        if is_end(s, right):
            return (FAR, NEAR) if n > 2 else (NEAR,)
        return (FINAL,) if (s + 1 == n - 1 if right else s - 1 == 0) else (FAR, NEAR)

    def message(i, s, right, kind):
        lo, hi = span(s, right, kind == FAR)
        here = (pl.ds(i * G, G) if kind == NEAR else i, pl.ds(lo, hi - lo))
        lane = 0 if is_end(s, right) else 1
        return pltpu.make_async_remote_copy(
            own.at[here],
            (from_left if right else from_right).at[here],
            st_send.at[kind, lax.rem(i, RING)],
            (near_recv if kind == NEAR else st_recv).at[lane, i],
            device_id=at(1 if right else n - 1),
            device_id_type=MESH,
        )

    def flight(s, right, kind):
        return END_NEARS if kind == NEAR and is_end(s, right) else RING

    def send(i, s, right, kind):
        depth = flight(s, right, kind)

        @pl.when(i >= depth)
        def _():
            message(i - depth, s, right, kind).wait_send()

        message(i, s, right, kind).start()

    def drain(s, right):
        for kind in kinds(s, right):
            total = steps if kind == NEAR else S
            for i in range(max(0, total - flight(s, right, kind)), total):
                message(i, s, right, kind).wait_send()

    def send_prompt(g, q, s, right):
        behind = END_BEHIND if is_end(s, right) else MID_BEHIND
        for kind in kinds(s, right):
            if kind != NEAR:
                send(g * G + q, s, right, kind)
            elif q == G - 1:

                @pl.when(g >= behind)
                def _():
                    send(g - behind, s, right, NEAR)

    def send_rest(s, right):
        behind = END_BEHIND if is_end(s, right) else MID_BEHIND
        if NEAR in kinds(s, right):

            def one(g, carry):
                send(g, s, right, NEAR)
                return carry

            lax.fori_loop(max(0, steps - behind), steps, one, 0)

    def log_copy(g):
        here = pl.ds(g * G, G)
        return pltpu.make_async_remote_copy(
            log_out.at[here],
            log_in.at[here],
            log_send.at[g],
            log_recv.at[g],
            device_id=at(n - 1),
            device_id_type=MESH,
        )

    def project(g):
        @pl.when(g == 0)
        def _():
            load_x(0).wait()

        if steps > 1:

            @pl.when(g == 1)
            def _():
                load_x(1).wait()

        slot = lax.rem(g, lead_steps)
        xg = xbuf[pl.ds(g * G, G)].reshape(G * L, xbuf.shape[2])
        acc = jnp.dot(xg, wall[:, 0 : 128 + C], preferred_element_type=F32).astype(BF16).astype(F32)
        for q in range(G):
            p = g * G + q
            raw = acc[q * L : (q + 1) * L]
            pad[slot, q, 8 : 8 + L, :] = raw[:, 128:]
            dt = softplus(raw[:, 0:128].T[0:heads] + bias_t)
            ld = off[p] - speed_t * dt
            a = ld.astype(BF16).astype(F32)
            b = (ld - a).astype(BF16).astype(F32)
            parts = jnp.concatenate([a, b, ld - a - b, jnp.zeros_like(a)], axis=0).astype(BF16)
            sums = jnp.dot(parts, later_ones, preferred_element_type=F32)
            suffix = sums[0:heads] + sums[heads : 2 * heads] + sums[2 * heads : 3 * heads]
            whole = jnp.broadcast_to(suffix[:, 0:1] + ld[:, 0:1], (heads, 128))
            decay[p] = jnp.exp(whole)
            log_own[p] = jnp.sum(whole * eye, axis=0, keepdims=True)
            w = dt * jnp.exp(suffix)
            hi = w.astype(BF16).astype(F32)
            wsplit[slot, q] = jnp.concatenate([hi, w - hi], axis=0).astype(BF16)

    def states(g):
        slot = lax.rem(g, lead_steps)
        before = halo_in[g].astype(F32)

        @pl.when(me == n - 1)
        def _():
            for q in range(G):
                log_out[g * G + q] = log_own[g * G + q]
            log_copy(g).start()

        for q in range(G):
            p = g * G + q
            pad[slot, q, 8 - (CONV - 1) : 8, :] = before[q * (CONV - 1) : (q + 1) * (CONV - 1)]
            wide = lax.dot_general(
                wsplit[slot, q],
                expand[...],
                (((0,), (0,)), ((), ())),
                preferred_element_type=F32,
            )

            def mixed(c):
                s = slice(c, c + 128)
                t = pad[slot, q, 8 - (CONV - 1) : 8 - (CONV - 1) + L, s] * taps[0:1, s]
                for j in range(1, CONV):
                    r = 8 - (CONV - 1) + j
                    t = t + pad[slot, q, r : r + L, s] * taps[j : j + 1, s]
                return silu(t).astype(BF16)

            in_map = mixed(F)
            for c in range(0, F, 128):
                weighted = (mixed(c).astype(F32) * wide[:, c : c + 128]).astype(BF16)
                share = lax.dot_general(
                    weighted, in_map, (((0,), (0,)), ((), ())), preferred_element_type=F32
                ).astype(BF16)
                for hh in range(128 // P_SIZE):
                    h = c // P_SIZE + hh
                    for d in range(n):
                        b = hh * P_SIZE + d * R
                        own[p, d, h * R : (h + 1) * R, :] = share[b : b + R]

            @pl.when(me == 0)
            def _(q=q):
                send_prompt(g, q, 0, True)

            @pl.when(me == n - 1)
            def _(q=q):
                send_prompt(g, q, n - 1, False)

    def later_factor(p):
        row = jnp.sum(eye * log_in[p], axis=1, keepdims=True)
        return jnp.exp(jnp.broadcast_to(row, (heads, 128)))

    def sum_right(g, q, s):
        p = g * G + q
        message(p, s - 1, True, FAR).wait_recv()
        factor = decay[p]
        for d in reversed(range(s + 1, n)):
            for h in range(heads):
                z = (p, d, slice(h * R, (h + 1) * R))
                got = from_left[z].astype(F32) * factor[h : h + 1, :]
                own[z] = (own[z].astype(F32) + got).astype(BF16)
        send_prompt(g, q, s, True)

    def sum_left(g, q, s):
        p = g * G + q
        message(p, s + 1, False, FAR).wait_recv()
        factor = later_factor(p)
        for d in range(s):
            for h in range(heads):
                z = (p, d, slice(h * R, (h + 1) * R))
                mine = own[z].astype(F32) * factor[h : h + 1, :]
                own[z] = (from_right[z].astype(F32) + mine).astype(BF16)
        send_prompt(g, q, s, False)

    def pass_log(g):
        log_copy(g).wait_recv()
        for q in range(G):
            log_out[g * G + q] = log_in[g * G + q] + log_own[g * G + q]
        log_copy(g).start()

    def relay(g, outer):
        for s in range(1, n - 1):

            @pl.when(me == s)
            def _(s=s):
                for q in range(G):
                    if outer == (s < n - 1 - s):
                        sum_right(g, q, s)
                    else:
                        sum_left(g, q, s)

    off_load.wait()
    lax.fori_loop(0, lead_steps, lambda g, carry: (project(g), carry)[1], 0)
    @pl.when(me == 0)
    def _():
        halo_in[...] = jnp.zeros_like(halo_in)

    @pl.when(me > 0)
    def _():
        halo_copy(0).wait_recv()

    relay_lag = min(RELAY_LAG, steps)

    def step(g, carry):
        if steps > 1:

            @pl.when((g == 1) & (me > 0))
            def _():
                halo_copy(1).wait_recv()

        states(g)

        @pl.when(g + lead_steps < steps)
        def _():
            project(g + lead_steps)

        if n > 2:

            for s in range(1, n - 1):

                @pl.when((g == min(FORWARD_AT * (n - 1 - s), steps - 1)) & (me == s))
                def _():
                    newest_copy().wait_recv()
                    newest_copy().start()

        for s in range(1, n - 1):

            @pl.when((me == s) & (g >= n - 2 - s))
            def _(s=s):
                pass_log(g - (n - 2 - s))

        @pl.when(g >= relay_lag)
        def _():
            relay(g - relay_lag, True)

        @pl.when(g >= relay_lag + 1)
        def _():
            relay(g - relay_lag - 1, False)

        return carry

    lax.fori_loop(0, steps, step, 0)
    head_cols = ones_where((HEADS, RH), lambda i, l: i == lead + lax.div(l, R))
    local_cols = ones_where((128, RH), lambda i, l: i == lax.div(l, R))
    local = ones_where((HEADS, 128), lambda i, c: (i == lead + c) & (c < heads))
    pick = ones_where(
        (F, RH), lambda c, l: c == lax.div(l, R) * P_SIZE + me * R + lax.rem(l, R), BF16
    )
    row_pick = ones_where((P_SIZE, RH), lambda c, l: c == me * R + lax.rem(l, R))
    gate_load.wait()
    gate = jnp.dot(edge[S], wg[...], preferred_element_type=F32).astype(BF16)
    gate_here = silu(jnp.dot(gate, pick, preferred_element_type=F32))
    gain_here = jnp.sum(exact_dot(gain_ref[...], row_pick) * head_cols, axis=0, keepdims=True)
    skip_here = exact_dot(skip_ref[...], head_cols)
    new_step = jnp.dot(edge[S], wall[:, 0:128], preferred_element_type=F32).astype(BF16)
    new_dt = softplus(new_step.astype(F32) + exact_dot(bias, local))
    dt_here = exact_dot(new_dt, local_cols)
    keep_here = jnp.exp(-exact_dot(exact_dot(speed, local) * new_dt, local_cols))

    @pl.when(me == 0)
    def _():
        newest_copy().wait_recv()

    new_mixed = silu(newest[...] + new_raw * taps[CONV - 1 : CONV, :]).astype(BF16)
    new_input = jnp.dot(new_mixed[:, 0:F], pick, preferred_element_type=F32)
    new_in = new_mixed[:, F:C].astype(F32)
    new_out = new_mixed[:, C : C + STATE]
    both = jnp.sum(new_in * new_out.astype(F32), axis=1, keepdims=True)
    where_row = lax.broadcasted_iota(jnp.int32, (SP, RH), 0)

    def rest(outer):
        for s in range(n):
            for right in (True, False):
                if outer == (is_end(s, right) or (s < n - 1 - s) == right):

                    @pl.when(me == s)
                    def _(s=s, right=right):
                        send_rest(s, right)

    def arrivals(g, s, right):
        if FINAL in kinds(s, right):
            for q in range(G):
                message(g * G + q, s, right, FINAL).wait_recv()
        elif NEAR in kinds(s, right):
            message(g, s, right, NEAR).wait_recv()

    def finish(g, y):
        for s in range(n):

            @pl.when(me == s)
            def _(s=s):
                if s > 0:
                    arrivals(g, s - 1, True)
                if s == 0:
                    log_copy(g).wait_recv()
                if s < n - 1:
                    arrivals(g, s + 1, False)

        for q in range(G):
            p = g * G + q
            before, after = decay[p], later_factor(p)
            kept = []
            for h in range(heads):
                z = (p, me, slice(h * R, (h + 1) * R))
                t = own[z].astype(F32) + from_left[z].astype(F32) * before[h : h + 1, :]
                t = t * after[h : h + 1, :] + from_right[z].astype(F32)
                kept.append(t.astype(BF16))
            kept = jnp.concatenate(kept, axis=0)
            cache_ref[p] = kept
            part = lax.dot_general(
                new_out, kept, (((1,), (1,)), ((), ())), preferred_element_type=F32
            )
            y = jnp.where(where_row == p, part, y)
        return y

    for s in range(1, n - 2):

        @pl.when(me == s)
        def _(s=s):
            for g in range(max(0, steps - (n - 2 - s)), steps):
                pass_log(g)

    for g in range(steps - relay_lag, steps):
        relay(g, True)
        if g > 0:
            relay(g - 1, False)
    rest(True)
    relay(steps - 1, False)
    rest(False)
    y = lax.fori_loop(0, steps, finish, jnp.zeros((SP, RH), F32))

    readout = keep_here * y + dt_here * new_input * both + skip_here * new_input
    gated = readout * gate_here
    square_sum = jnp.broadcast_to(jnp.sum(gated * gated, axis=1, keepdims=True), (SP, 128))
    diagonal = ones_where((SP, 128), lambda i, c: i == c)
    sq = jnp.sum(square_sum * diagonal, axis=0, keepdims=True)
    sq_out[...] = sq

    def sq_copy(i):
        a, b = peers[i]
        return pltpu.make_async_remote_copy(
            sq_out, sq_in.at[i], sq_sem.at[0], sq_sem.at[1], device_id=at(a, b), device_id_type=MESH
        )

    all_squares = pltpu.make_async_remote_copy(
        sq_in, sq_in, sq_sem.at[0], sq_sem.at[1], device_id=at(1), device_id_type=MESH
    )
    for i in range(len(peers)):
        sq_copy(i).start()
    for s in range(n):

        @pl.when(me == s)
        def _(s=s):
            drain(s, True)
            drain(s, False)
            if s > 0:
                for g in range(steps):
                    log_copy(g).wait_send()

    @pl.when(me < n - 1)
    def _():
        for k in halo_parts:
            halo_copy(k).wait_send()

    @pl.when(me > 0)
    def _():
        newest_copy().wait_send()

    all_squares.wait_recv()
    for i in range(len(peers)):
        sq = sq + sq_in[i]
    mean = jnp.sum(diagonal * sq, axis=1, keepdims=True) / (HEADS * P_SIZE)
    scale = lax.rsqrt(mean + epsilon)
    read_ref[...] = (gated * scale * gain_here).astype(BF16)[0:S]

    all_squares.wait_send()


def on_chip(array):
    return pltpu.with_memory_space_constraint(array, pltpu.VMEM)


def emit_kernel(dims, cache_ref, read_ref, cache_hbm, out_hbm, out, sem):
    heads, R = dims
    S, RH = read_ref.shape
    copies = [
        pltpu.make_async_copy(cache_ref, cache_hbm, sem.at[0]),
        pltpu.make_async_copy(out, out_hbm, sem.at[1]),
    ]
    copies[0].start()
    spread = ones_where((heads, RH), lambda h, l: h == lax.div(l, R))
    pick = ones_where((RH, R), lambda l, r: lax.rem(l, R) == r, BF16)
    value = read_ref[...].astype(F32)
    rows = jnp.concatenate([value[p : p + 1] * spread for p in range(S)], axis=0).astype(BF16)
    picked = jnp.dot(rows, pick, preferred_element_type=F32)
    out[...] = picked.reshape(S, heads, R).astype(BF16)
    copies[1].start()
    for c in copies:
        c.wait()


LEAD, RELAY_LAG, FORWARD_AT = 1, 1, 2
FAR, NEAR, FINAL = 0, 1, 2
SMALL = (1, 7, 8, 9, 10, 11, 12, 13)
RING, END_NEARS = 4, 2
END_BEHIND, MID_BEHIND = 5, 2


def fused(*args):
    x, wv, wk = args[0], args[2], args[4]
    S, L, D = x.shape
    n, m = lax.axis_size("sp"), lax.axis_size("tp")
    F = wv.shape[1]
    heads = F // P_SIZE
    R = P_SIZE // n
    G = next(g for g in (2, 3, 1) if S % g == 0)
    steps = S // G
    slots = min(LEAD, steps)
    halo_rows = -(-G * (CONV - 1) // 8) * 8
    C, RH, SP = F + STATE, heads * R, 16
    dims = (n, m, S, L, heads, R, G)
    flat = list(args)
    for i in (10, 11, 12):
        flat[i] = args[i].reshape(1, HEADS)
    flat[6] = args[6].T
    flat[14] = jnp.swapaxes(args[14], 1, 2)
    hbm, vmem = pl.BlockSpec(memory_space=pl.ANY), pl.BlockSpec(memory_space=pltpu.VMEM)
    specs = [hbm] * len(flat)
    dma = pltpu.SemaphoreType.DMA
    cache, read = pl.pallas_call(
        lambda *refs: mixer_kernel(dims, *refs),
        out_shape=(
            pltpu.VMEM((S, RH, STATE), BF16),
            pltpu.VMEM((S, RH), BF16),
        ),
        in_specs=specs,
        out_specs=(vmem, vmem),
        scratch_shapes=[
            *[pltpu.VMEM(flat[i].shape, flat[i].dtype) for i in SMALL],
            pltpu.VMEM((S, L, D), BF16),
            pltpu.VMEM((S + 1, 16, D), BF16),
            pltpu.VMEM((D, 128 + C + STATE), BF16),
            pltpu.VMEM((heads, D), BF16),
            pltpu.VMEM((D, F), BF16),
            pltpu.VMEM((S, heads, L), F32),
            pltpu.VMEM((CONV, C + STATE), F32),
            pltpu.VMEM((slots, G, 8 + L, C), F32),
            pltpu.VMEM((slots, G, 2 * heads, L), BF16),
            pltpu.VMEM((steps, halo_rows, C), BF16),
            pltpu.VMEM((steps, halo_rows, C), BF16),
            pltpu.VMEM((SP, C + STATE), F32),
            pltpu.VMEM((2, HEADS, 128), F32),
            pltpu.VMEM((S, heads, 128), F32),
            pltpu.VMEM((S, 1, 128), F32),
            pltpu.VMEM((S, 1, 128), F32),
            pltpu.VMEM((S, 1, 128), F32),
            pltpu.VMEM((S, n, RH, STATE), BF16),
            pltpu.VMEM((S, n, RH, STATE), BF16),
            pltpu.VMEM((S, n, RH, STATE), BF16),
            pltpu.VMEM((1, 128), F32),
            pltpu.VMEM((n * m - 1, 1, 128), F32),
            pltpu.VMEM((2 * heads, F), BF16),
            dma((16,)),
            dma((2,)),
            dma((2, 2)),
            dma((2,)),
            dma((3, RING)),
            dma((2, S)),
            dma((2, steps)),
            dma((steps,)),
            dma((steps,)),
            dma((2,)),
        ],
        compiler_params=pltpu.CompilerParams(
            collective_id=0, has_side_effects=True, vmem_limit_bytes=56 * 1024 * 1024
        ),
    )(*flat)
    cache, read = pl.pallas_call(
        lambda *refs: emit_kernel((heads, R), *refs),
        out_shape=(
            jax.ShapeDtypeStruct((S, RH, STATE), BF16),
            jax.ShapeDtypeStruct((S, heads, R), BF16),
        ),
        in_specs=[vmem, vmem],
        out_specs=(pl.BlockSpec(memory_space=pltpu.HBM),) * 2,
        scratch_shapes=[pltpu.VMEM((S, heads, R), BF16), dma((2,))],
    )(on_chip(cache), on_chip(read))
    return cache.reshape(S, heads, R, STATE), read


def fits(n, m, shapes):
    (S, L), F = shapes
    heads, R = F // P_SIZE, P_SIZE // n
    return (
        n > 1
        and F % 128 == 0
        and heads % 8 == 0
        and R % 16 == 0
        and (heads * R) % 128 == 0
        and S <= 16
        and L % 16 == 0
        and L == 128
        and (HEADS // GROUPS) % heads == 0
    )


def part(*args):
    shapes = (args[0].shape[:2], args[2].shape[1])
    if fits(lax.axis_size("sp"), lax.axis_size("tp"), shapes):
        return fused(*args)
    return shards(*args)


def solution(mesh):
    in_specs = (
        P("grp", "sp", None),
        P("grp", None),
        P(None, "tp"),
        P(None, "tp"),
        P(),
        P(),
        P(),
        P(),
        P(),
        P(),
        P(),
        P(),
        P(),
        P(),
        P("grp", "sp", None),
    )
    out_specs = (P("grp", "tp", "sp", None), P("grp", "tp", "sp"))
    return jax.shard_map(part, mesh=mesh, in_specs=in_specs, out_specs=out_specs, check_vma=False)
```

```python
import jax
import jax.numpy as jnp
from jax import lax
from jax.experimental import pallas as pl
from jax.experimental.pallas import tpu as pltpu
from jax.sharding import PartitionSpec as P

HEADS = 32
P_SIZE = 64
GROUPS = 2
STATE = 128
CONV = 4
SPAN = 64


epsilon = 1e-06


def shifted(block, axis, distance):
    devices = range(lax.axis_size(axis))
    route = [(i - distance, i) for i in devices if i - distance in devices]
    return lax.ppermute(block, axis, route)


def broadcast(value, axis, source):
    kept = jnp.where(lax.axis_index(axis) == source, value, 0).astype(value.dtype)
    return lax.psum(kept, axis)


def prefix(shard, axis, combine, identity):
    length, here = (lax.axis_size(axis), lax.axis_index(axis))
    everything = lax.all_gather(shard, axis)
    start = jnp.broadcast_to(jnp.asarray(identity, shard.dtype), shard.shape)

    def lap(k, before):
        at = length - 1 - k
        reached = at > here
        new = combine(before, everything[at])
        return jnp.where(reached, new, before)

    return lax.fori_loop(0, length, lap, start)


def shards(
    prompt_layer_input,
    next_token_input,
    value_projection,
    output_gate_matrix,
    key_projection,
    query_projection,
    step_projection,
    value_filter_taps,
    key_filter_taps,
    query_filter_taps,
    step_size_bias,
    head_decay_logarithm,
    direct_path_weight,
    gated_norm_gain,
    position_decay_offset,
):
    seq_count, local_len, width = prompt_layer_input.shape
    resident_heads = value_projection.shape[1] // P_SIZE
    feature_cols = resident_heads * P_SIZE
    shard_count = lax.axis_size("sp")
    rows_here = P_SIZE // shard_count
    shard_index = lax.axis_index("sp")
    leading_head = lax.axis_index("tp") * resident_heads
    group_index = leading_head // (HEADS // GROUPS)
    row_first = shard_index * rows_here
    in_cols = lax.dynamic_slice_in_dim(key_projection, group_index * STATE, STATE, 1)
    out_cols = lax.dynamic_slice_in_dim(query_projection, group_index * STATE, STATE, 1)
    weights_here = jnp.concatenate([value_projection, in_cols, out_cols], axis=1)
    step_cols = lax.dynamic_slice_in_dim(step_projection, leading_head, resident_heads, 1)
    kernel = jnp.concatenate(
        [
            lax.dynamic_slice_in_dim(value_filter_taps, leading_head * P_SIZE, feature_cols, 1),
            lax.dynamic_slice_in_dim(key_filter_taps, group_index * STATE, STATE, 1),
            lax.dynamic_slice_in_dim(query_filter_taps, group_index * STATE, STATE, 1),
        ],
        axis=1,
    ).astype(jnp.float32)
    head_decay_speed = jnp.exp(
        lax.dynamic_slice_in_dim(head_decay_logarithm, leading_head, resident_heads, 0)
    )
    bias_here = lax.dynamic_slice_in_dim(step_size_bias, leading_head, resident_heads, 0)
    skip_here = lax.dynamic_slice_in_dim(direct_path_weight, leading_head, resident_heads, 0)
    gain_here = lax.dynamic_slice(
        gated_norm_gain, (leading_head, row_first), (resident_heads, rows_here)
    )
    token_rows = prompt_layer_input.reshape(seq_count * local_len, width)
    projected = jnp.dot(token_rows, weights_here, preferred_element_type=jnp.float32).astype(
        jnp.bfloat16
    )
    projected = projected.reshape(seq_count, local_len, feature_cols + 2 * STATE)
    trailing = projected[:, local_len - (CONV - 1) :]
    before = shifted(trailing, "sp", 1)
    newest = broadcast(trailing, "sp", shard_count - 1)
    padded = jnp.concatenate([before, projected], axis=1)
    total = padded[:, 0:local_len].astype(jnp.float32) * kernel[0]
    for tap in range(1, CONV):
        total = total + padded[:, tap : tap + local_len].astype(jnp.float32) * kernel[tap]
    mixed = jax.nn.silu(total).astype(jnp.bfloat16)
    step_raw = jnp.dot(token_rows, step_cols, preferred_element_type=jnp.float32).astype(
        jnp.bfloat16
    )
    discrete_step = jax.nn.softplus(step_raw.astype(jnp.float32) + bias_here).reshape(
        seq_count, local_len, resident_heads
    )
    decay_spikes = lax.dynamic_slice_in_dim(position_decay_offset, leading_head, resident_heads, 2)
    logarithmic_decay = decay_spikes - head_decay_speed * discrete_step
    block_count = local_len // SPAN
    cumulative = jnp.cumsum(
        logarithmic_decay.reshape(seq_count, block_count, SPAN, resident_heads), axis=2
    )
    decay_weight = jnp.exp(cumulative[:, :, -1:] - cumulative) * discrete_step.reshape(
        seq_count, block_count, SPAN, resident_heads
    )
    head_input = mixed[:, :, :feature_cols].reshape(
        seq_count, block_count, SPAN, resident_heads, P_SIZE
    )
    weighted = (head_input.astype(jnp.float32) * decay_weight[..., None]).astype(jnp.bfloat16)
    in_map = mixed[:, :, feature_cols : feature_cols + STATE].reshape(
        seq_count, block_count, SPAN, STATE
    )
    block_state = jnp.einsum(
        "bcshp,bcsn->bchpn", weighted, in_map, preferred_element_type=jnp.float32
    )
    block_log = cumulative[:, :, -1]
    own_log = jnp.sum(block_log, axis=1)
    after_block = jnp.exp(own_log[:, None] - jnp.cumsum(block_log, axis=1))
    local_state = jnp.sum(after_block[..., None, None] * block_state, axis=1)
    later_log = prefix(own_log, "sp", jnp.add, jnp.zeros_like(own_log))
    scaled = jnp.exp(later_log)[:, :, None, None] * local_state
    own_rows = lax.psum_scatter(scaled, "sp", scatter_dimension=2, tiled=True)
    state_cache = own_rows.astype(jnp.bfloat16)
    new_raw = jnp.dot(next_token_input, weights_here, preferred_element_type=jnp.float32).astype(
        jnp.bfloat16
    )
    new_step = jnp.dot(next_token_input, step_cols, preferred_element_type=jnp.float32).astype(
        jnp.bfloat16
    )
    new_gate = jnp.dot(
        next_token_input, output_gate_matrix, preferred_element_type=jnp.float32
    ).astype(jnp.bfloat16)
    window = jnp.concatenate([newest, new_raw[:, None]], axis=1)
    new_mixed = jax.nn.silu(jnp.sum(window.astype(jnp.float32) * kernel[None], axis=1)).astype(
        jnp.bfloat16
    )
    new_input = lax.dynamic_slice_in_dim(
        new_mixed[:, :feature_cols].reshape(seq_count, resident_heads, P_SIZE),
        row_first,
        rows_here,
        2,
    ).astype(jnp.float32)
    new_in = new_mixed[:, feature_cols : feature_cols + STATE].astype(jnp.float32)
    new_out = new_mixed[:, feature_cols + STATE :].astype(jnp.float32)
    new_step_size = jax.nn.softplus(new_step.astype(jnp.float32) + bias_here)
    cache_values = lax.optimization_barrier(state_cache).astype(jnp.float32)
    new_state = (
        jnp.exp(-head_decay_speed * new_step_size)[:, :, None, None] * cache_values
        + (new_step_size[:, :, None] * new_input)[..., None] * new_in[:, None, None, :]
    )
    readout = (
        jnp.sum(new_state * new_out[:, None, None, :], axis=-1)
        + skip_here[None, :, None] * new_input
    )
    gate_rows = lax.dynamic_slice_in_dim(
        new_gate.reshape(seq_count, resident_heads, P_SIZE), row_first, rows_here, 2
    )
    gated = readout * jax.nn.silu(gate_rows.astype(jnp.float32))
    squares = lax.psum(jnp.sum(gated * gated, axis=(1, 2)), ("sp", "tp"))
    scale = lax.rsqrt(squares / (HEADS * P_SIZE) + epsilon)
    first_read = (gated * scale[:, None, None] * gain_here[None]).astype(jnp.bfloat16)
    return (state_cache, first_read)


F32, BF16 = jnp.float32, jnp.bfloat16
MESH = pl.DeviceIdType.MESH
EXACT = lax.Precision.HIGHEST


def exact_dot(a, b, dims=((1,), (0,))):
    return lax.dot_general(a, b, (dims, ((), ())), precision=EXACT, preferred_element_type=F32)


def softplus(v):
    return jnp.maximum(v, 0.0) + jnp.log1p(jnp.exp(-jnp.abs(v)))


def silu(v):
    return v / (1.0 + jnp.exp(-v))


def ones_where(shape, test, dtype=F32):
    rows = lax.broadcasted_iota(jnp.int32, shape, 0)
    cols = lax.broadcasted_iota(jnp.int32, shape, 1)
    return jnp.where(test(rows, cols), 1.0, 0.0).astype(dtype)


def mixer_kernel(
    dims,
    x_hbm,
    next_hbm,
    wv_hbm,
    wg_hbm,
    wk_hbm,
    wq_hbm,
    ws_hbm,
    tv_hbm,
    tk_hbm,
    tq_hbm,
    bias_hbm,
    speed_hbm,
    skip_hbm,
    gain_hbm,
    off_hbm,
    cache_ref,
    read_ref,
    next_ref,
    tv_ref,
    tk_ref,
    tq_ref,
    bias_ref,
    speed_ref,
    skip_ref,
    gain_ref,
    xbuf,
    edge,
    wall,
    ws,
    wg,
    off,
    taps,
    pad,
    wsplit,
    halo_out,
    halo_in,
    newest,
    heads_t,
    decay,
    log_own,
    log_out,
    log_in,
    own,
    from_left,
    from_right,
    sq_out,
    sq_in,
    expand,
    load_sem,
    x_sem,
    halo_sem,
    new_sem,
    st_send,
    st_recv,
    near_recv,
    log_send,
    log_recv,
    sq_sem,
):
    n, m, S, L, heads, R, G = dims
    F = heads * P_SIZE
    C = F + STATE
    RH = heads * R
    SP = 16
    steps = S // G
    lead_steps = min(LEAD, steps)
    me, tp = lax.axis_index("sp"), lax.axis_index("tp")
    lead = pl.multiple_of(tp * heads, 8)
    group = lax.div(lead, HEADS // GROUPS)
    fcol = pl.multiple_of(tp * F, 128)
    gcol = pl.multiple_of(group * STATE, 128)

    def load(src, dst, k):
        c = pltpu.make_async_copy(src, dst, load_sem.at[k])
        c.start()
        return c

    def load_x(k):
        here = pl.ds(0, G) if k == 0 else pl.ds(G, S - G)
        return pltpu.make_async_copy(x_hbm.at[here], xbuf.at[here], x_sem.at[k])

    first = [
        load(ws_hbm.at[pl.ds(lead, heads), :], ws, 0),
        load(x_hbm.at[:, pl.ds(L - 16, 16)], edge.at[pl.ds(0, S)], 1),
        load(wk_hbm.at[:, pl.ds(gcol, STATE)], wall.at[:, pl.ds(128 + F, STATE)], 2),
        load(wq_hbm.at[:, pl.ds(gcol, STATE)], wall.at[:, pl.ds(128 + C, STATE)], 3),
        load(wv_hbm, wall.at[:, pl.ds(128, F)], 4),
    ]
    small = [
        load(a, b, 8 + k)
        for k, (a, b) in enumerate(
            [
                (next_hbm, next_ref),
                (tv_hbm, tv_ref),
                (tk_hbm, tk_ref),
                (tq_hbm, tq_ref),
                (bias_hbm, bias_ref),
                (speed_hbm, speed_ref),
                (skip_hbm, skip_ref),
                (gain_hbm, gain_ref),
            ]
        )
    ]

    peers = [(a, b) for a in range(n) for b in range(m) if (a, b) != (0, 0)]

    def at(a, b=0):
        return {"sp": lax.rem(me + a, n), "tp": lax.rem(tp + b, m)}

    barrier = pltpu.get_barrier_semaphore()
    for a, b in peers:
        pl.semaphore_signal(barrier, inc=1, device_id=at(a, b), device_id_type=MESH)

    head_of = ones_where((heads, F), lambda i, c: i == lax.div(c, P_SIZE))
    expand[...] = jnp.concatenate([head_of, head_of], axis=0).astype(BF16)
    @pl.when(me == 0)
    def _():
        from_left[:, 0] = jnp.zeros((S, RH, STATE), BF16)

    @pl.when(me == n - 1)
    def _():
        from_right[:, n - 1] = jnp.zeros((S, RH, STATE), BF16)
        log_in[...] = jnp.zeros_like(log_in)

    eye = ones_where((heads, 128), lambda i, c: i == c)
    later_ones = ones_where((L, L), lambda u, t: u > t, BF16)

    for c in small:
        c.wait()
    taps[:, 0:F] = tv_ref[:, pl.ds(fcol, F)].astype(F32)
    taps[:, F:C] = tk_ref[:, pl.ds(gcol, STATE)].astype(F32)
    taps[:, C : C + STATE] = tq_ref[:, pl.ds(gcol, STATE)].astype(F32)
    edge[S] = jnp.zeros(edge.shape[1:], BF16)
    edge[S, 0:S, :] = next_ref[...]
    bias = bias_ref[...]
    speed = jnp.exp(speed_ref[...])
    square = jnp.zeros((128, 128 - HEADS), F32)

    def columns(row, k):
        full = jnp.concatenate([jnp.broadcast_to(row, (128, HEADS)), square], axis=1)
        heads_t[k] = full.T[0:HEADS]
        return heads_t[k, pl.ds(lead, heads), :]

    bias_t, speed_t = columns(bias, 0), columns(speed, 1)

    for c in first[1:4]:
        c.wait()
    load_x(0).start()
    off_load = load(off_hbm.at[:, pl.ds(lead, heads), :], off, 6)
    rows = edge[...].reshape((S + 1) * 16, edge.shape[2])
    halo_out[...] = jnp.zeros_like(halo_out)
    first[4].wait()
    part = jnp.dot(rows, wall[:, 128:], preferred_element_type=F32)
    edge_rows = part.astype(BF16).astype(F32).reshape(S + 1, 16, C + STATE)

    def tails(prompts):
        for p in prompts:
            r = p % G * (CONV - 1)
            tail = edge_rows[p, 16 - (CONV - 1) :, 0:C]
            halo_out[p // G, r : r + CONV - 1, :] = tail.astype(BF16)

    tails(range(G))
    if steps > 1:
        load_x(1).start()
    gate_load = load(wg_hbm, wg, 7)
    pl.semaphore_wait(barrier, len(peers))

    def halo_copy(k):
        here = pl.ds(0, 1) if k == 0 else pl.ds(1, steps - 1)
        return pltpu.make_async_remote_copy(
            halo_out.at[here],
            halo_in.at[here],
            halo_sem.at[0, k],
            halo_sem.at[1, k],
            device_id=at(1),
            device_id_type=MESH,
        )

    halo_parts = range(2 if steps > 1 else 1)

    @pl.when(me < n - 1)
    def _():
        halo_copy(0).start()

    tails(range(G, S))

    @pl.when(me < n - 1)
    def _():
        for k in halo_parts[1:]:
            halo_copy(k).start()

    def newest_copy():
        return pltpu.make_async_remote_copy(
            newest,
            newest,
            new_sem.at[0],
            new_sem.at[1],
            device_id=at(n - 1),
            device_id_type=MESH,
        )

    last = 16 - (CONV - 1)

    @pl.when(me == n - 1)
    def _():
        newest[...] = jnp.zeros_like(newest)
        newest[0:S, :] = sum(
            edge_rows[0:S, last + j, :] * taps[j : j + 1, :] for j in range(CONV - 1)
        )
        newest_copy().start()

    new_raw = edge_rows[S]
    first[0].wait()
    wall[:, 0:128] = jnp.concatenate(
        [ws[...], jnp.zeros((128 - heads, ws.shape[1]), BF16)], axis=0
    ).T

    def span(s, right, far):
        if right:
            return (s + 2, n) if far else (s + 1, s + 2)
        return (0, s - 1) if far else (s - 1, s)

    def is_end(s, right):
        return s == (0 if right else n - 1)

    def kinds(s, right):
        if not 0 <= (s + 1 if right else s - 1) < n:
            return ()
        if is_end(s, right):
            return (FAR, NEAR) if n > 2 else (NEAR,)
        return (FINAL,) if (s + 1 == n - 1 if right else s - 1 == 0) else (FAR, NEAR)

    def message(i, s, right, kind):
        lo, hi = span(s, right, kind == FAR)
        here = (pl.ds(i * G, G) if kind == NEAR else i, pl.ds(lo, hi - lo))
        lane = 0 if is_end(s, right) else 1
        return pltpu.make_async_remote_copy(
            own.at[here],
            (from_left if right else from_right).at[here],
            st_send.at[kind, lax.rem(i, RING)],
            (near_recv if kind == NEAR else st_recv).at[lane, i],
            device_id=at(1 if right else n - 1),
            device_id_type=MESH,
        )

    def flight(s, right, kind):
        return END_NEARS if kind == NEAR and is_end(s, right) else RING

    def send(i, s, right, kind):
        depth = flight(s, right, kind)

        @pl.when(i >= depth)
        def _():
            message(i - depth, s, right, kind).wait_send()

        message(i, s, right, kind).start()

    def drain(s, right):
        for kind in kinds(s, right):
            total = steps if kind == NEAR else S
            for i in range(max(0, total - flight(s, right, kind)), total):
                message(i, s, right, kind).wait_send()

    def send_prompt(g, q, s, right):
        behind = END_BEHIND if is_end(s, right) else MID_BEHIND
        for kind in kinds(s, right):
            if kind != NEAR:
                send(g * G + q, s, right, kind)
            elif q == G - 1:

                @pl.when(g >= behind)
                def _():
                    send(g - behind, s, right, NEAR)

    def send_rest(s, right):
        behind = END_BEHIND if is_end(s, right) else MID_BEHIND
        if NEAR in kinds(s, right):

            def one(g, carry):
                send(g, s, right, NEAR)
                return carry

            lax.fori_loop(max(0, steps - behind), steps, one, 0)

    def log_copy(g):
        here = pl.ds(g * G, G)
        return pltpu.make_async_remote_copy(
            log_out.at[here],
            log_in.at[here],
            log_send.at[g],
            log_recv.at[g],
            device_id=at(n - 1),
            device_id_type=MESH,
        )

    def project(g):
        @pl.when(g == 0)
        def _():
            load_x(0).wait()

        if steps > 1:

            @pl.when(g == 1)
            def _():
                load_x(1).wait()

        slot = lax.rem(g, lead_steps)
        xg = xbuf[pl.ds(g * G, G)].reshape(G * L, xbuf.shape[2])
        acc = jnp.dot(xg, wall[:, 0 : 128 + C], preferred_element_type=F32).astype(BF16).astype(F32)
        for q in range(G):
            p = g * G + q
            raw = acc[q * L : (q + 1) * L]
            pad[slot, q, 8 : 8 + L, :] = raw[:, 128:]
            dt = softplus(raw[:, 0:128].T[0:heads] + bias_t)
            ld = off[p] - speed_t * dt
            a = ld.astype(BF16).astype(F32)
            b = (ld - a).astype(BF16).astype(F32)
            parts = jnp.concatenate([a, b, ld - a - b, jnp.zeros_like(a)], axis=0).astype(BF16)
            sums = jnp.dot(parts, later_ones, preferred_element_type=F32)
            suffix = sums[0:heads] + sums[heads : 2 * heads] + sums[2 * heads : 3 * heads]
            whole = jnp.broadcast_to(suffix[:, 0:1] + ld[:, 0:1], (heads, 128))
            decay[p] = jnp.exp(whole)
            log_own[p] = jnp.sum(whole * eye, axis=0, keepdims=True)
            w = dt * jnp.exp(suffix)
            hi = w.astype(BF16).astype(F32)
            wsplit[slot, q] = jnp.concatenate([hi, w - hi], axis=0).astype(BF16)

    def states(g):
        slot = lax.rem(g, lead_steps)

        @pl.when(me == n - 1)
        def _():
            for q in range(G):
                log_out[g * G + q] = log_own[g * G + q]
            log_copy(g).start()

        for q in range(G):
            p = g * G + q
            wide = lax.dot_general(
                wsplit[slot, q],
                expand[...],
                (((0,), (0,)), ((), ())),
                preferred_element_type=F32,
            )

            def mixed(c, a, b):
                s = slice(c, c + 128)
                t = jnp.zeros((b - a, 128), F32)
                for j in range(CONV):
                    r = 8 - (CONV - 1) + j
                    t = t + pad[slot, q, r + a : r + b, s] * taps[j : j + 1, s]
                return silu(t).astype(BF16).astype(F32)

            columns = range(0, C, 128)
            later = [mixed(c, 8, L) for c in columns]
            if q == 0:
                for k in halo_parts:

                    @pl.when((g == k) & (me > 0))
                    def _(k=k):
                        halo_copy(k).wait_recv()

            r = q * (CONV - 1)
            pad[slot, q, 8 - (CONV - 1) : 8, :] = halo_in[g, r : r + CONV - 1, :].astype(F32)
            whole = [
                jnp.concatenate([mixed(c, 0, 8), late], axis=0)
                for c, late in zip(columns, later)
            ]
            in_map = whole[-1].astype(BF16)
            for c in range(0, F, 128):
                weighted = (whole[c // 128] * wide[:, c : c + 128]).astype(BF16)
                share = lax.dot_general(
                    weighted, in_map, (((0,), (0,)), ((), ())), preferred_element_type=F32
                ).astype(BF16)
                for hh in range(128 // P_SIZE):
                    h = c // P_SIZE + hh
                    for d in range(n):
                        b = hh * P_SIZE + d * R
                        own[p, d, h * R : (h + 1) * R, :] = share[b : b + R]

            @pl.when(me == 0)
            def _(q=q):
                send_prompt(g, q, 0, True)

            @pl.when(me == n - 1)
            def _(q=q):
                send_prompt(g, q, n - 1, False)

    def later_factor(p):
        row = jnp.sum(eye * log_in[p], axis=1, keepdims=True)
        return jnp.exp(jnp.broadcast_to(row, (heads, 128)))

    def sum_right(g, q, s):
        p = g * G + q
        message(p, s - 1, True, FAR).wait_recv()
        factor = decay[p]
        for d in reversed(range(s + 1, n)):
            for h in range(heads):
                z = (p, d, slice(h * R, (h + 1) * R))
                got = from_left[z].astype(F32) * factor[h : h + 1, :]
                own[z] = (own[z].astype(F32) + got).astype(BF16)
        send_prompt(g, q, s, True)

    def sum_left(g, q, s):
        p = g * G + q
        message(p, s + 1, False, FAR).wait_recv()
        factor = later_factor(p)
        for d in range(s):
            for h in range(heads):
                z = (p, d, slice(h * R, (h + 1) * R))
                mine = own[z].astype(F32) * factor[h : h + 1, :]
                own[z] = (from_right[z].astype(F32) + mine).astype(BF16)
        send_prompt(g, q, s, False)

    def pass_log(g):
        log_copy(g).wait_recv()
        for q in range(G):
            log_out[g * G + q] = log_in[g * G + q] + log_own[g * G + q]
        log_copy(g).start()

    def relay(g, outer):
        for s in range(1, n - 1):

            @pl.when(me == s)
            def _(s=s):
                for q in range(G):
                    if outer == (s < n - 1 - s):
                        sum_right(g, q, s)
                    else:
                        sum_left(g, q, s)

    off_load.wait()
    lax.fori_loop(0, lead_steps, lambda g, carry: (project(g), carry)[1], 0)
    @pl.when(me == 0)
    def _():
        halo_in[...] = jnp.zeros_like(halo_in)

    relay_lag = min(RELAY_LAG, steps)

    def step(g, carry):
        states(g)

        @pl.when(g + lead_steps < steps)
        def _():
            project(g + lead_steps)

        if n > 2:

            for s in range(1, n - 1):

                @pl.when((g == min(FORWARD_AT * (n - 1 - s), steps - 1)) & (me == s))
                def _():
                    newest_copy().wait_recv()
                    newest_copy().start()

        for s in range(1, n - 1):

            @pl.when((me == s) & (g >= n - 2 - s))
            def _(s=s):
                pass_log(g - (n - 2 - s))

        @pl.when(g >= relay_lag)
        def _():
            relay(g - relay_lag, True)

        @pl.when(g >= relay_lag + 1)
        def _():
            relay(g - relay_lag - 1, False)

        return carry

    lax.fori_loop(0, steps, step, 0)
    head_cols = ones_where((HEADS, RH), lambda i, l: i == lead + lax.div(l, R))
    local_cols = ones_where((128, RH), lambda i, l: i == lax.div(l, R))
    local = ones_where((HEADS, 128), lambda i, c: (i == lead + c) & (c < heads))
    pick = ones_where(
        (F, RH), lambda c, l: c == lax.div(l, R) * P_SIZE + me * R + lax.rem(l, R), BF16
    )
    row_pick = ones_where((P_SIZE, RH), lambda c, l: c == me * R + lax.rem(l, R))
    gate_load.wait()
    gate = jnp.dot(edge[S], wg[...], preferred_element_type=F32).astype(BF16)
    gate_here = silu(jnp.dot(gate, pick, preferred_element_type=F32))
    gain_here = jnp.sum(exact_dot(gain_ref[...], row_pick) * head_cols, axis=0, keepdims=True)
    skip_here = exact_dot(skip_ref[...], head_cols)
    new_step = jnp.dot(edge[S], wall[:, 0:128], preferred_element_type=F32).astype(BF16)
    new_dt = softplus(new_step.astype(F32) + exact_dot(bias, local))
    dt_here = exact_dot(new_dt, local_cols)
    keep_here = jnp.exp(-exact_dot(exact_dot(speed, local) * new_dt, local_cols))

    @pl.when(me == 0)
    def _():
        newest_copy().wait_recv()

    new_mixed = silu(newest[...] + new_raw * taps[CONV - 1 : CONV, :]).astype(BF16)
    new_input = jnp.dot(new_mixed[:, 0:F], pick, preferred_element_type=F32)
    new_in = new_mixed[:, F:C].astype(F32)
    new_out = new_mixed[:, C : C + STATE]
    both = jnp.sum(new_in * new_out.astype(F32), axis=1, keepdims=True)
    where_row = lax.broadcasted_iota(jnp.int32, (SP, RH), 0)

    def rest(outer):
        for s in range(n):
            for right in (True, False):
                if outer == (is_end(s, right) or (s < n - 1 - s) == right):

                    @pl.when(me == s)
                    def _(s=s, right=right):
                        send_rest(s, right)

    def arrivals(g, s, right):
        if FINAL in kinds(s, right):
            for q in range(G):
                message(g * G + q, s, right, FINAL).wait_recv()
        elif NEAR in kinds(s, right):
            message(g, s, right, NEAR).wait_recv()

    def finish(g, y):
        for s in range(n):

            @pl.when(me == s)
            def _(s=s):
                if s > 0:
                    arrivals(g, s - 1, True)
                if s == 0:
                    log_copy(g).wait_recv()
                if s < n - 1:
                    arrivals(g, s + 1, False)

        for q in range(G):
            p = g * G + q
            before, after = decay[p], later_factor(p)
            kept = []
            for h in range(heads):
                z = (p, me, slice(h * R, (h + 1) * R))
                t = own[z].astype(F32) + from_left[z].astype(F32) * before[h : h + 1, :]
                t = t * after[h : h + 1, :] + from_right[z].astype(F32)
                kept.append(t.astype(BF16))
            kept = jnp.concatenate(kept, axis=0)
            cache_ref[p] = kept
            part = lax.dot_general(
                new_out, kept, (((1,), (1,)), ((), ())), preferred_element_type=F32
            )
            y = jnp.where(where_row == p, part, y)
        return y

    for s in range(1, n - 2):

        @pl.when(me == s)
        def _(s=s):
            for g in range(max(0, steps - (n - 2 - s)), steps):
                pass_log(g)

    for g in range(steps - relay_lag, steps):
        relay(g, True)
        if g > 0:
            relay(g - 1, False)
    rest(True)
    relay(steps - 1, False)
    rest(False)
    y = lax.fori_loop(0, steps, finish, jnp.zeros((SP, RH), F32))

    readout = keep_here * y + dt_here * new_input * both + skip_here * new_input
    gated = readout * gate_here
    square_sum = jnp.broadcast_to(jnp.sum(gated * gated, axis=1, keepdims=True), (SP, 128))
    diagonal = ones_where((SP, 128), lambda i, c: i == c)
    sq = jnp.sum(square_sum * diagonal, axis=0, keepdims=True)
    sq_out[...] = sq

    def sq_copy(i):
        a, b = peers[i]
        return pltpu.make_async_remote_copy(
            sq_out, sq_in.at[i], sq_sem.at[0], sq_sem.at[1], device_id=at(a, b), device_id_type=MESH
        )

    all_squares = pltpu.make_async_remote_copy(
        sq_in, sq_in, sq_sem.at[0], sq_sem.at[1], device_id=at(1), device_id_type=MESH
    )
    for i in range(len(peers)):
        sq_copy(i).start()
    for s in range(n):

        @pl.when(me == s)
        def _(s=s):
            drain(s, True)
            drain(s, False)
            if s > 0:
                for g in range(steps):
                    log_copy(g).wait_send()

    @pl.when(me < n - 1)
    def _():
        for k in halo_parts:
            halo_copy(k).wait_send()

    @pl.when(me > 0)
    def _():
        newest_copy().wait_send()

    all_squares.wait_recv()
    for i in range(len(peers)):
        sq = sq + sq_in[i]
    mean = jnp.sum(diagonal * sq, axis=1, keepdims=True) / (HEADS * P_SIZE)
    scale = lax.rsqrt(mean + epsilon)
    read_ref[...] = (gated * scale * gain_here).astype(BF16)[0:S]

    all_squares.wait_send()


def on_chip(array):
    return pltpu.with_memory_space_constraint(array, pltpu.VMEM)


def emit_kernel(dims, cache_ref, read_ref, cache_hbm, out_hbm, out, sem):
    heads, R = dims
    S, RH = read_ref.shape
    copies = [
        pltpu.make_async_copy(cache_ref, cache_hbm, sem.at[0]),
        pltpu.make_async_copy(out, out_hbm, sem.at[1]),
    ]
    copies[0].start()
    spread = ones_where((heads, RH), lambda h, l: h == lax.div(l, R))
    pick = ones_where((RH, R), lambda l, r: lax.rem(l, R) == r, BF16)
    value = read_ref[...].astype(F32)
    rows = jnp.concatenate([value[p : p + 1] * spread for p in range(S)], axis=0).astype(BF16)
    picked = jnp.dot(rows, pick, preferred_element_type=F32)
    out[...] = picked.reshape(S, heads, R).astype(BF16)
    copies[1].start()
    for c in copies:
        c.wait()


LEAD, RELAY_LAG, FORWARD_AT = 1, 1, 2
FAR, NEAR, FINAL = 0, 1, 2
SMALL = (1, 7, 8, 9, 10, 11, 12, 13)
RING, END_NEARS = 4, 2
END_BEHIND, MID_BEHIND = 5, 2


def fused(*args):
    x, wv, wk = args[0], args[2], args[4]
    S, L, D = x.shape
    n, m = lax.axis_size("sp"), lax.axis_size("tp")
    F = wv.shape[1]
    heads = F // P_SIZE
    R = P_SIZE // n
    G = next(g for g in (2, 3, 1) if S % g == 0)
    steps = S // G
    slots = min(LEAD, steps)
    halo_rows = -(-G * (CONV - 1) // 8) * 8
    C, RH, SP = F + STATE, heads * R, 16
    dims = (n, m, S, L, heads, R, G)
    flat = list(args)
    for i in (10, 11, 12):
        flat[i] = args[i].reshape(1, HEADS)
    flat[6] = args[6].T
    flat[14] = jnp.swapaxes(args[14], 1, 2)
    hbm, vmem = pl.BlockSpec(memory_space=pl.ANY), pl.BlockSpec(memory_space=pltpu.VMEM)
    specs = [hbm] * len(flat)
    dma = pltpu.SemaphoreType.DMA
    cache, read = pl.pallas_call(
        lambda *refs: mixer_kernel(dims, *refs),
        out_shape=(
            pltpu.VMEM((S, RH, STATE), BF16),
            pltpu.VMEM((S, RH), BF16),
        ),
        in_specs=specs,
        out_specs=(vmem, vmem),
        scratch_shapes=[
            *[pltpu.VMEM(flat[i].shape, flat[i].dtype) for i in SMALL],
            pltpu.VMEM((S, L, D), BF16),
            pltpu.VMEM((S + 1, 16, D), BF16),
            pltpu.VMEM((D, 128 + C + STATE), BF16),
            pltpu.VMEM((heads, D), BF16),
            pltpu.VMEM((D, F), BF16),
            pltpu.VMEM((S, heads, L), F32),
            pltpu.VMEM((CONV, C + STATE), F32),
            pltpu.VMEM((slots, G, 8 + L, C), F32),
            pltpu.VMEM((slots, G, 2 * heads, L), BF16),
            pltpu.VMEM((steps, halo_rows, C), BF16),
            pltpu.VMEM((steps, halo_rows, C), BF16),
            pltpu.VMEM((SP, C + STATE), F32),
            pltpu.VMEM((2, HEADS, 128), F32),
            pltpu.VMEM((S, heads, 128), F32),
            pltpu.VMEM((S, 1, 128), F32),
            pltpu.VMEM((S, 1, 128), F32),
            pltpu.VMEM((S, 1, 128), F32),
            pltpu.VMEM((S, n, RH, STATE), BF16),
            pltpu.VMEM((S, n, RH, STATE), BF16),
            pltpu.VMEM((S, n, RH, STATE), BF16),
            pltpu.VMEM((1, 128), F32),
            pltpu.VMEM((n * m - 1, 1, 128), F32),
            pltpu.VMEM((2 * heads, F), BF16),
            dma((16,)),
            dma((2,)),
            dma((2, 2)),
            dma((2,)),
            dma((3, RING)),
            dma((2, S)),
            dma((2, steps)),
            dma((steps,)),
            dma((steps,)),
            dma((2,)),
        ],
        compiler_params=pltpu.CompilerParams(
            collective_id=0, has_side_effects=True, vmem_limit_bytes=56 * 1024 * 1024
        ),
    )(*flat)
    cache, read = pl.pallas_call(
        lambda *refs: emit_kernel((heads, R), *refs),
        out_shape=(
            jax.ShapeDtypeStruct((S, RH, STATE), BF16),
            jax.ShapeDtypeStruct((S, heads, R), BF16),
        ),
        in_specs=[vmem, vmem],
        out_specs=(pl.BlockSpec(memory_space=pltpu.HBM),) * 2,
        scratch_shapes=[pltpu.VMEM((S, heads, R), BF16), dma((2,))],
    )(on_chip(cache), on_chip(read))
    return cache.reshape(S, heads, R, STATE), read


def fits(n, m, shapes):
    (S, L), F = shapes
    heads, R = F // P_SIZE, P_SIZE // n
    return (
        n > 1
        and F % 128 == 0
        and heads % 8 == 0
        and R % 16 == 0
        and (heads * R) % 128 == 0
        and S <= 16
        and L % 16 == 0
        and L == 128
        and (HEADS // GROUPS) % heads == 0
    )


def part(*args):
    shapes = (args[0].shape[:2], args[2].shape[1])
    if fits(lax.axis_size("sp"), lax.axis_size("tp"), shapes):
        return fused(*args)
    return shards(*args)


def solution(mesh):
    in_specs = (
        P("grp", "sp", None),
        P("grp", None),
        P(None, "tp"),
        P(None, "tp"),
        P(),
        P(),
        P(),
        P(),
        P(),
        P(),
        P(),
        P(),
        P(),
        P(),
        P("grp", "sp", None),
    )
    out_specs = (P("grp", "tp", "sp", None), P("grp", "tp", "sp"))
    return jax.shard_map(part, mesh=mesh, in_specs=in_specs, out_specs=out_specs, check_vma=False)
```

```python
import jax
import jax.numpy as jnp
from jax import lax
from jax.experimental import pallas as pl
from jax.experimental.pallas import tpu as pltpu
from jax.sharding import PartitionSpec as P

HEADS = 32
P_SIZE = 64
GROUPS = 2
STATE = 128
CONV = 4
SPAN = 64


epsilon = 1e-06


def shifted(block, axis, distance):
    devices = range(lax.axis_size(axis))
    route = [(i - distance, i) for i in devices if i - distance in devices]
    return lax.ppermute(block, axis, route)


def broadcast(value, axis, source):
    kept = jnp.where(lax.axis_index(axis) == source, value, 0).astype(value.dtype)
    return lax.psum(kept, axis)


def prefix(shard, axis, combine, identity):
    length, here = (lax.axis_size(axis), lax.axis_index(axis))
    everything = lax.all_gather(shard, axis)
    start = jnp.broadcast_to(jnp.asarray(identity, shard.dtype), shard.shape)

    def lap(k, before):
        at = length - 1 - k
        reached = at > here
        new = combine(before, everything[at])
        return jnp.where(reached, new, before)

    return lax.fori_loop(0, length, lap, start)


def shards(
    prompt_layer_input,
    next_token_input,
    value_projection,
    output_gate_matrix,
    key_projection,
    query_projection,
    step_projection,
    value_filter_taps,
    key_filter_taps,
    query_filter_taps,
    step_size_bias,
    head_decay_logarithm,
    direct_path_weight,
    gated_norm_gain,
    position_decay_offset,
):
    seq_count, local_len, width = prompt_layer_input.shape
    resident_heads = value_projection.shape[1] // P_SIZE
    feature_cols = resident_heads * P_SIZE
    shard_count = lax.axis_size("sp")
    rows_here = P_SIZE // shard_count
    shard_index = lax.axis_index("sp")
    leading_head = lax.axis_index("tp") * resident_heads
    group_index = leading_head // (HEADS // GROUPS)
    row_first = shard_index * rows_here
    in_cols = lax.dynamic_slice_in_dim(key_projection, group_index * STATE, STATE, 1)
    out_cols = lax.dynamic_slice_in_dim(query_projection, group_index * STATE, STATE, 1)
    weights_here = jnp.concatenate([value_projection, in_cols, out_cols], axis=1)
    step_cols = lax.dynamic_slice_in_dim(step_projection, leading_head, resident_heads, 1)
    kernel = jnp.concatenate(
        [
            lax.dynamic_slice_in_dim(value_filter_taps, leading_head * P_SIZE, feature_cols, 1),
            lax.dynamic_slice_in_dim(key_filter_taps, group_index * STATE, STATE, 1),
            lax.dynamic_slice_in_dim(query_filter_taps, group_index * STATE, STATE, 1),
        ],
        axis=1,
    ).astype(jnp.float32)
    head_decay_speed = jnp.exp(
        lax.dynamic_slice_in_dim(head_decay_logarithm, leading_head, resident_heads, 0)
    )
    bias_here = lax.dynamic_slice_in_dim(step_size_bias, leading_head, resident_heads, 0)
    skip_here = lax.dynamic_slice_in_dim(direct_path_weight, leading_head, resident_heads, 0)
    gain_here = lax.dynamic_slice(
        gated_norm_gain, (leading_head, row_first), (resident_heads, rows_here)
    )
    token_rows = prompt_layer_input.reshape(seq_count * local_len, width)
    projected = jnp.dot(token_rows, weights_here, preferred_element_type=jnp.float32).astype(
        jnp.bfloat16
    )
    projected = projected.reshape(seq_count, local_len, feature_cols + 2 * STATE)
    trailing = projected[:, local_len - (CONV - 1) :]
    before = shifted(trailing, "sp", 1)
    newest = broadcast(trailing, "sp", shard_count - 1)
    padded = jnp.concatenate([before, projected], axis=1)
    total = padded[:, 0:local_len].astype(jnp.float32) * kernel[0]
    for tap in range(1, CONV):
        total = total + padded[:, tap : tap + local_len].astype(jnp.float32) * kernel[tap]
    mixed = jax.nn.silu(total).astype(jnp.bfloat16)
    step_raw = jnp.dot(token_rows, step_cols, preferred_element_type=jnp.float32).astype(
        jnp.bfloat16
    )
    discrete_step = jax.nn.softplus(step_raw.astype(jnp.float32) + bias_here).reshape(
        seq_count, local_len, resident_heads
    )
    decay_spikes = lax.dynamic_slice_in_dim(position_decay_offset, leading_head, resident_heads, 2)
    logarithmic_decay = decay_spikes - head_decay_speed * discrete_step
    block_count = local_len // SPAN
    cumulative = jnp.cumsum(
        logarithmic_decay.reshape(seq_count, block_count, SPAN, resident_heads), axis=2
    )
    decay_weight = jnp.exp(cumulative[:, :, -1:] - cumulative) * discrete_step.reshape(
        seq_count, block_count, SPAN, resident_heads
    )
    head_input = mixed[:, :, :feature_cols].reshape(
        seq_count, block_count, SPAN, resident_heads, P_SIZE
    )
    weighted = (head_input.astype(jnp.float32) * decay_weight[..., None]).astype(jnp.bfloat16)
    in_map = mixed[:, :, feature_cols : feature_cols + STATE].reshape(
        seq_count, block_count, SPAN, STATE
    )
    block_state = jnp.einsum(
        "bcshp,bcsn->bchpn", weighted, in_map, preferred_element_type=jnp.float32
    )
    block_log = cumulative[:, :, -1]
    own_log = jnp.sum(block_log, axis=1)
    after_block = jnp.exp(own_log[:, None] - jnp.cumsum(block_log, axis=1))
    local_state = jnp.sum(after_block[..., None, None] * block_state, axis=1)
    later_log = prefix(own_log, "sp", jnp.add, jnp.zeros_like(own_log))
    scaled = jnp.exp(later_log)[:, :, None, None] * local_state
    own_rows = lax.psum_scatter(scaled, "sp", scatter_dimension=2, tiled=True)
    state_cache = own_rows.astype(jnp.bfloat16)
    new_raw = jnp.dot(next_token_input, weights_here, preferred_element_type=jnp.float32).astype(
        jnp.bfloat16
    )
    new_step = jnp.dot(next_token_input, step_cols, preferred_element_type=jnp.float32).astype(
        jnp.bfloat16
    )
    new_gate = jnp.dot(
        next_token_input, output_gate_matrix, preferred_element_type=jnp.float32
    ).astype(jnp.bfloat16)
    window = jnp.concatenate([newest, new_raw[:, None]], axis=1)
    new_mixed = jax.nn.silu(jnp.sum(window.astype(jnp.float32) * kernel[None], axis=1)).astype(
        jnp.bfloat16
    )
    new_input = lax.dynamic_slice_in_dim(
        new_mixed[:, :feature_cols].reshape(seq_count, resident_heads, P_SIZE),
        row_first,
        rows_here,
        2,
    ).astype(jnp.float32)
    new_in = new_mixed[:, feature_cols : feature_cols + STATE].astype(jnp.float32)
    new_out = new_mixed[:, feature_cols + STATE :].astype(jnp.float32)
    new_step_size = jax.nn.softplus(new_step.astype(jnp.float32) + bias_here)
    cache_values = lax.optimization_barrier(state_cache).astype(jnp.float32)
    new_state = (
        jnp.exp(-head_decay_speed * new_step_size)[:, :, None, None] * cache_values
        + (new_step_size[:, :, None] * new_input)[..., None] * new_in[:, None, None, :]
    )
    readout = (
        jnp.sum(new_state * new_out[:, None, None, :], axis=-1)
        + skip_here[None, :, None] * new_input
    )
    gate_rows = lax.dynamic_slice_in_dim(
        new_gate.reshape(seq_count, resident_heads, P_SIZE), row_first, rows_here, 2
    )
    gated = readout * jax.nn.silu(gate_rows.astype(jnp.float32))
    squares = lax.psum(jnp.sum(gated * gated, axis=(1, 2)), ("sp", "tp"))
    scale = lax.rsqrt(squares / (HEADS * P_SIZE) + epsilon)
    first_read = (gated * scale[:, None, None] * gain_here[None]).astype(jnp.bfloat16)
    return (state_cache, first_read)


F32, BF16 = jnp.float32, jnp.bfloat16
MESH = pl.DeviceIdType.MESH
EXACT = lax.Precision.HIGHEST


def exact_dot(a, b, dims=((1,), (0,))):
    return lax.dot_general(a, b, (dims, ((), ())), precision=EXACT, preferred_element_type=F32)


def softplus(v):
    return jnp.maximum(v, 0.0) + jnp.log1p(jnp.exp(-jnp.abs(v)))


def silu(v):
    return v / (1.0 + jnp.exp(-v))


def ones_where(shape, test, dtype=F32):
    rows = lax.broadcasted_iota(jnp.int32, shape, 0)
    cols = lax.broadcasted_iota(jnp.int32, shape, 1)
    return jnp.where(test(rows, cols), 1.0, 0.0).astype(dtype)


def mixer_kernel(
    dims,
    x_hbm,
    next_hbm,
    wv_hbm,
    wg_hbm,
    wk_hbm,
    wq_hbm,
    ws_hbm,
    tv_hbm,
    tk_hbm,
    tq_hbm,
    bias_hbm,
    speed_hbm,
    skip_hbm,
    gain_hbm,
    off_hbm,
    cache_ref,
    read_ref,
    next_ref,
    tv_ref,
    tk_ref,
    tq_ref,
    bias_ref,
    speed_ref,
    skip_ref,
    gain_ref,
    xbuf,
    edge,
    early,
    wall,
    ws,
    wg,
    off,
    taps,
    pad,
    wsplit,
    halo_out,
    halo_in,
    newest,
    heads_t,
    decay,
    log_own,
    log_out,
    log_in,
    own,
    from_left,
    from_right,
    sq_out,
    sq_in,
    expand,
    load_sem,
    halo_sem,
    new_sem,
    st_send,
    st_recv,
    near_recv,
    log_send,
    log_recv,
    sq_sem,
):
    n, m, S, L, heads, R, G = dims
    F = heads * P_SIZE
    C = F + STATE
    RH = heads * R
    SP = 16
    steps = S // G
    lead_steps = min(LEAD, steps)
    me, tp = lax.axis_index("sp"), lax.axis_index("tp")
    lead = pl.multiple_of(tp * heads, 8)
    group = lax.div(lead, HEADS // GROUPS)
    fcol = pl.multiple_of(tp * F, 128)
    gcol = pl.multiple_of(group * STATE, 128)

    def load(src, dst, k):
        c = pltpu.make_async_copy(src, dst, load_sem.at[k])
        c.start()
        return c

    def load_x(k):
        here = pl.ds(0, G) if k == 0 else pl.ds(G, S - G)
        return pltpu.make_async_copy(x_hbm.at[here], xbuf.at[here], load_sem.at[k])

    half = x_hbm.shape[2] // 2

    def weights(k):
        rows = pl.ds(k * half, half)
        maps = pl.ds(gcol, STATE)
        return [
            load(wk_hbm.at[rows, maps], wall.at[rows, pl.ds(128 + F, STATE)], 10 + 3 * k),
            load(wq_hbm.at[rows, maps], wall.at[rows, pl.ds(128 + C, STATE)], 11 + 3 * k),
            load(wv_hbm.at[rows], wall.at[rows, pl.ds(128, F)], 12 + 3 * k),
        ]

    first = [
        load(next_hbm, next_ref, 0),
        load(ws_hbm.at[pl.ds(lead, heads), :], ws, 8),
        load(x_hbm.at[:, pl.ds(L - 16, 16)], edge.at[pl.ds(0, S)], 9),
    ]
    first += weights(0)
    second = weights(1)
    small = [
        load(a, b, 1 + k)
        for k, (a, b) in enumerate(
            [
                (tv_hbm, tv_ref),
                (tk_hbm, tk_ref),
                (tq_hbm, tq_ref),
                (bias_hbm, bias_ref),
                (speed_hbm, speed_ref),
                (skip_hbm, skip_ref),
                (gain_hbm, gain_ref),
            ]
        )
    ]

    peers = [(a, b) for a in range(n) for b in range(m) if (a, b) != (0, 0)]

    def at(a, b=0):
        return {"sp": lax.rem(me + a, n), "tp": lax.rem(tp + b, m)}

    barrier = pltpu.get_barrier_semaphore()
    for a, b in peers:
        pl.semaphore_signal(barrier, inc=1, device_id=at(a, b), device_id_type=MESH)

    head_of = ones_where((heads, F), lambda i, c: i == lax.div(c, P_SIZE))
    expand[...] = jnp.concatenate([head_of, head_of], axis=0).astype(BF16)
    @pl.when(me == 0)
    def _():
        from_left[:, 0] = jnp.zeros((S, RH, STATE), BF16)

    @pl.when(me == n - 1)
    def _():
        from_right[:, n - 1] = jnp.zeros((S, RH, STATE), BF16)
        log_in[...] = jnp.zeros_like(log_in)

    eye = ones_where((heads, 128), lambda i, c: i == c)
    later_ones = ones_where((L, L), lambda u, t: u > t, BF16)

    for c in first:
        c.wait()
    edge[S] = jnp.zeros(edge.shape[1:], BF16)
    edge[S, 0:S, :] = next_ref[...]
    rows = edge[...].reshape((S + 1) * 16, edge.shape[2])
    halo_out[...] = jnp.zeros_like(halo_out)
    early[...] = jnp.dot(rows[:, 0:half], wall[0:half, 128:], preferred_element_type=F32)
    for c in second + small:
        c.wait()
    load_x(0).start()
    off_load = load(off_hbm.at[:, pl.ds(lead, heads), :], off, 2)
    late = jnp.dot(rows[:, half:], wall[half:, 128:], preferred_element_type=F32)
    part = early[...] + late
    edge_rows = part.astype(BF16).astype(F32).reshape(S + 1, 16, C + STATE)

    def tails(prompts):
        for p in prompts:
            r = p % G * (CONV - 1)
            tail = edge_rows[p, 16 - (CONV - 1) :, 0:C]
            halo_out[p // G, r : r + CONV - 1, :] = tail.astype(BF16)

    tails(range(G))
    if steps > 1:
        load_x(1).start()
    gate_load = load(wg_hbm, wg, 3)
    pl.semaphore_wait(barrier, len(peers))

    def halo_copy(k):
        here = pl.ds(0, 1) if k == 0 else pl.ds(1, steps - 1)
        return pltpu.make_async_remote_copy(
            halo_out.at[here],
            halo_in.at[here],
            halo_sem.at[0, k],
            halo_sem.at[1, k],
            device_id=at(1),
            device_id_type=MESH,
        )

    halo_parts = range(2 if steps > 1 else 1)

    @pl.when(me < n - 1)
    def _():
        halo_copy(0).start()

    taps[:, 0:F] = tv_ref[:, pl.ds(fcol, F)].astype(F32)
    taps[:, F:C] = tk_ref[:, pl.ds(gcol, STATE)].astype(F32)
    taps[:, C : C + STATE] = tq_ref[:, pl.ds(gcol, STATE)].astype(F32)
    bias = bias_ref[...]
    speed = jnp.exp(speed_ref[...])
    square = jnp.zeros((128, 128 - HEADS), F32)

    def columns(row, k):
        full = jnp.concatenate([jnp.broadcast_to(row, (128, HEADS)), square], axis=1)
        heads_t[k] = full.T[0:HEADS]
        return heads_t[k, pl.ds(lead, heads), :]

    bias_t, speed_t = columns(bias, 0), columns(speed, 1)
    tails(range(G, S))

    @pl.when(me < n - 1)
    def _():
        for k in halo_parts[1:]:
            halo_copy(k).start()

    def newest_copy():
        return pltpu.make_async_remote_copy(
            newest,
            newest,
            new_sem.at[0],
            new_sem.at[1],
            device_id=at(n - 1),
            device_id_type=MESH,
        )

    last = 16 - (CONV - 1)

    @pl.when(me == n - 1)
    def _():
        newest[...] = jnp.zeros_like(newest)
        newest[0:S, :] = sum(
            edge_rows[0:S, last + j, :] * taps[j : j + 1, :] for j in range(CONV - 1)
        )
        newest_copy().start()

    new_raw = edge_rows[S]
    wall[:, 0:128] = jnp.concatenate(
        [ws[...], jnp.zeros((128 - heads, ws.shape[1]), BF16)], axis=0
    ).T

    def span(s, right, far):
        if right:
            return (s + 2, n) if far else (s + 1, s + 2)
        return (0, s - 1) if far else (s - 1, s)

    def is_end(s, right):
        return s == (0 if right else n - 1)

    def kinds(s, right):
        if not 0 <= (s + 1 if right else s - 1) < n:
            return ()
        if is_end(s, right):
            return (FAR, NEAR) if n > 2 else (NEAR,)
        return (FINAL,) if (s + 1 == n - 1 if right else s - 1 == 0) else (FAR, NEAR)

    def message(i, s, right, kind):
        lo, hi = span(s, right, kind == FAR)
        here = (pl.ds(i * G, G) if kind == NEAR else i, pl.ds(lo, hi - lo))
        lane = 0 if is_end(s, right) else 1
        return pltpu.make_async_remote_copy(
            own.at[here],
            (from_left if right else from_right).at[here],
            st_send.at[kind, lax.rem(i, RING)],
            (near_recv if kind == NEAR else st_recv).at[lane, i],
            device_id=at(1 if right else n - 1),
            device_id_type=MESH,
        )

    def flight(s, right, kind):
        return END_NEARS if kind == NEAR and is_end(s, right) else RING

    def send(i, s, right, kind):
        depth = flight(s, right, kind)

        @pl.when(i >= depth)
        def _():
            message(i - depth, s, right, kind).wait_send()

        message(i, s, right, kind).start()

    def drain(s, right):
        for kind in kinds(s, right):
            total = steps if kind == NEAR else S
            for i in range(max(0, total - flight(s, right, kind)), total):
                message(i, s, right, kind).wait_send()

    def send_prompt(g, q, s, right):
        behind = END_BEHIND if is_end(s, right) else MID_BEHIND
        for kind in kinds(s, right):
            if kind != NEAR:
                send(g * G + q, s, right, kind)
            elif q == G - 1:

                @pl.when(g >= behind)
                def _():
                    send(g - behind, s, right, NEAR)

    def send_rest(s, right):
        behind = END_BEHIND if is_end(s, right) else MID_BEHIND
        if NEAR in kinds(s, right):

            def one(g, carry):
                send(g, s, right, NEAR)
                return carry

            lax.fori_loop(max(0, steps - behind), steps, one, 0)

    def log_copy(g):
        here = pl.ds(g * G, G)
        return pltpu.make_async_remote_copy(
            log_out.at[here],
            log_in.at[here],
            log_send.at[0],
            log_recv.at[g],
            device_id=at(n - 1),
            device_id_type=MESH,
        )

    def last_log_left(g):
        @pl.when(g >= 1)
        def _():
            log_copy(g - 1).wait_send()

    def project(g):
        @pl.when(g == 0)
        def _():
            load_x(0).wait()

        if steps > 1:

            @pl.when(g == 1)
            def _():
                load_x(1).wait()

        slot = lax.rem(g, lead_steps)
        xg = xbuf[pl.ds(g * G, G)].reshape(G * L, xbuf.shape[2])
        acc = jnp.dot(xg, wall[:, 0 : 128 + C], preferred_element_type=F32).astype(BF16).astype(F32)
        for q in range(G):
            p = g * G + q
            raw = acc[q * L : (q + 1) * L]
            pad[slot, q, 8 : 8 + L, :] = raw[:, 128:]
            dt = softplus(raw[:, 0:128].T[0:heads] + bias_t)
            ld = off[p] - speed_t * dt
            a = ld.astype(BF16).astype(F32)
            b = (ld - a).astype(BF16).astype(F32)
            parts = jnp.concatenate([a, b, ld - a - b, jnp.zeros_like(a)], axis=0).astype(BF16)
            sums = jnp.dot(parts, later_ones, preferred_element_type=F32)
            suffix = sums[0:heads] + sums[heads : 2 * heads] + sums[2 * heads : 3 * heads]
            whole = jnp.broadcast_to(suffix[:, 0:1] + ld[:, 0:1], (heads, 128))
            decay[p] = jnp.exp(whole)
            log_own[p] = jnp.sum(whole * eye, axis=0, keepdims=True)
            w = dt * jnp.exp(suffix)
            hi = w.astype(BF16).astype(F32)
            wsplit[slot, q] = jnp.concatenate([hi, w - hi], axis=0).astype(BF16)

    def states(g):
        slot = lax.rem(g, lead_steps)

        @pl.when(me == n - 1)
        def _():
            for q in range(G):
                log_out[g * G + q] = log_own[g * G + q]
            last_log_left(g)
            log_copy(g).start()

        for q in range(G):
            p = g * G + q
            wide = lax.dot_general(
                wsplit[slot, q],
                expand[...],
                (((0,), (0,)), ((), ())),
                preferred_element_type=F32,
            )

            def mixed(c, a, b):
                s = slice(c, c + 128)
                t = jnp.zeros((b - a, 128), F32)
                for j in range(CONV):
                    r = 8 - (CONV - 1) + j
                    t = t + pad[slot, q, r + a : r + b, s] * taps[j : j + 1, s]
                return silu(t).astype(BF16).astype(F32)

            columns = range(0, C, 128)
            later = [mixed(c, 8, L) for c in columns]
            if q == 0:
                for k in halo_parts:

                    @pl.when((g == k) & (me > 0))
                    def _(k=k):
                        halo_copy(k).wait_recv()

            r = q * (CONV - 1)
            pad[slot, q, 8 - (CONV - 1) : 8, :] = halo_in[g, r : r + CONV - 1, :].astype(F32)
            whole = [
                jnp.concatenate([mixed(c, 0, 8), late], axis=0)
                for c, late in zip(columns, later)
            ]
            in_map = whole[-1].astype(BF16)
            for c in range(0, F, 128):
                weighted = (whole[c // 128] * wide[:, c : c + 128]).astype(BF16)
                share = lax.dot_general(
                    weighted, in_map, (((0,), (0,)), ((), ())), preferred_element_type=F32
                ).astype(BF16)
                for hh in range(128 // P_SIZE):
                    h = c // P_SIZE + hh
                    for d in range(n):
                        b = hh * P_SIZE + d * R
                        own[p, d, h * R : (h + 1) * R, :] = share[b : b + R]

            @pl.when(me == 0)
            def _(q=q):
                send_prompt(g, q, 0, True)

            @pl.when(me == n - 1)
            def _(q=q):
                send_prompt(g, q, n - 1, False)

    def later_factor(p):
        row = jnp.sum(eye * log_in[p], axis=1, keepdims=True)
        return jnp.exp(jnp.broadcast_to(row, (heads, 128)))

    def sum_right(g, q, s):
        p = g * G + q
        message(p, s - 1, True, FAR).wait_recv()
        factor = decay[p]
        for d in reversed(range(s + 1, n)):
            for h in range(heads):
                z = (p, d, slice(h * R, (h + 1) * R))
                got = from_left[z].astype(F32) * factor[h : h + 1, :]
                own[z] = (own[z].astype(F32) + got).astype(BF16)
        send_prompt(g, q, s, True)

    def sum_left(g, q, s):
        p = g * G + q
        message(p, s + 1, False, FAR).wait_recv()
        factor = later_factor(p)
        for d in range(s):
            for h in range(heads):
                z = (p, d, slice(h * R, (h + 1) * R))
                mine = own[z].astype(F32) * factor[h : h + 1, :]
                own[z] = (from_right[z].astype(F32) + mine).astype(BF16)
        send_prompt(g, q, s, False)

    def pass_log(g):
        log_copy(g).wait_recv()
        last_log_left(g)
        for q in range(G):
            log_out[g * G + q] = log_in[g * G + q] + log_own[g * G + q]
        log_copy(g).start()

    def relay(g, outer):
        for s in range(1, n - 1):

            @pl.when(me == s)
            def _(s=s):
                for q in range(G):
                    if outer == (s < n - 1 - s):
                        sum_right(g, q, s)
                    else:
                        sum_left(g, q, s)

    off_load.wait()
    lax.fori_loop(0, lead_steps, lambda g, carry: (project(g), carry)[1], 0)
    @pl.when(me == 0)
    def _():
        halo_in[...] = jnp.zeros_like(halo_in)

    relay_lag = min(RELAY_LAG, steps)

    def step(g, carry):
        states(g)

        @pl.when(g + lead_steps < steps)
        def _():
            project(g + lead_steps)

        if n > 2:

            for s in range(1, n - 1):

                @pl.when((g == min(FORWARD_AT * (n - 1 - s), steps - 1)) & (me == s))
                def _():
                    newest_copy().wait_recv()
                    newest_copy().start()

        for s in range(1, n - 1):

            @pl.when((me == s) & (g >= n - 2 - s))
            def _(s=s):
                pass_log(g - (n - 2 - s))

        @pl.when(g >= relay_lag)
        def _():
            relay(g - relay_lag, True)

        @pl.when(g >= relay_lag + 1)
        def _():
            relay(g - relay_lag - 1, False)

        return carry

    lax.fori_loop(0, steps, step, 0)
    head_cols = ones_where((HEADS, RH), lambda i, l: i == lead + lax.div(l, R))
    local_cols = ones_where((128, RH), lambda i, l: i == lax.div(l, R))
    local = ones_where((HEADS, 128), lambda i, c: (i == lead + c) & (c < heads))
    pick = ones_where(
        (F, RH), lambda c, l: c == lax.div(l, R) * P_SIZE + me * R + lax.rem(l, R), BF16
    )
    row_pick = ones_where((P_SIZE, RH), lambda c, l: c == me * R + lax.rem(l, R))
    gate_load.wait()
    gate = jnp.dot(edge[S], wg[...], preferred_element_type=F32).astype(BF16)
    gate_here = silu(jnp.dot(gate, pick, preferred_element_type=F32))
    gain_here = jnp.sum(exact_dot(gain_ref[...], row_pick) * head_cols, axis=0, keepdims=True)
    skip_here = exact_dot(skip_ref[...], head_cols)
    new_step = jnp.dot(edge[S], wall[:, 0:128], preferred_element_type=F32).astype(BF16)
    new_dt = softplus(new_step.astype(F32) + exact_dot(bias, local))
    dt_here = exact_dot(new_dt, local_cols)
    keep_here = jnp.exp(-exact_dot(exact_dot(speed, local) * new_dt, local_cols))

    @pl.when(me == 0)
    def _():
        newest_copy().wait_recv()

    new_mixed = silu(newest[...] + new_raw * taps[CONV - 1 : CONV, :]).astype(BF16)
    new_input = jnp.dot(new_mixed[:, 0:F], pick, preferred_element_type=F32)
    new_in = new_mixed[:, F:C].astype(F32)
    new_out = new_mixed[:, C : C + STATE]
    both = jnp.sum(new_in * new_out.astype(F32), axis=1, keepdims=True)
    where_row = lax.broadcasted_iota(jnp.int32, (SP, RH), 0)

    def rest(outer):
        for s in range(n):
            for right in (True, False):
                if outer == (is_end(s, right) or (s < n - 1 - s) == right):

                    @pl.when(me == s)
                    def _(s=s, right=right):
                        send_rest(s, right)

    def arrivals(g, s, right):
        if FINAL in kinds(s, right):
            for q in range(G):
                message(g * G + q, s, right, FINAL).wait_recv()
        elif NEAR in kinds(s, right):
            message(g, s, right, NEAR).wait_recv()

    def finish(g, y):
        for s in range(n):

            @pl.when(me == s)
            def _(s=s):
                if s > 0:
                    arrivals(g, s - 1, True)
                if s == 0:
                    log_copy(g).wait_recv()
                if s < n - 1:
                    arrivals(g, s + 1, False)

        for q in range(G):
            p = g * G + q
            before, after = decay[p], later_factor(p)
            kept = []
            for h in range(heads):
                z = (p, me, slice(h * R, (h + 1) * R))
                t = own[z].astype(F32) + from_left[z].astype(F32) * before[h : h + 1, :]
                t = t * after[h : h + 1, :] + from_right[z].astype(F32)
                kept.append(t.astype(BF16))
            kept = jnp.concatenate(kept, axis=0)
            cache_ref[p] = kept
            part = lax.dot_general(
                new_out, kept, (((1,), (1,)), ((), ())), preferred_element_type=F32
            )
            y = jnp.where(where_row == p, part, y)
        return y

    for s in range(1, n - 2):

        @pl.when(me == s)
        def _(s=s):
            for g in range(max(0, steps - (n - 2 - s)), steps):
                pass_log(g)

    for g in range(steps - relay_lag, steps):
        relay(g, True)
        if g > 0:
            relay(g - 1, False)
    rest(True)
    relay(steps - 1, False)
    rest(False)
    y = lax.fori_loop(0, steps, finish, jnp.zeros((SP, RH), F32))

    readout = keep_here * y + dt_here * new_input * both + skip_here * new_input
    gated = readout * gate_here
    square_sum = jnp.broadcast_to(jnp.sum(gated * gated, axis=1, keepdims=True), (SP, 128))
    diagonal = ones_where((SP, 128), lambda i, c: i == c)
    sq = jnp.sum(square_sum * diagonal, axis=0, keepdims=True)
    sq_out[...] = sq

    def sq_copy(i):
        a, b = peers[i]
        return pltpu.make_async_remote_copy(
            sq_out, sq_in.at[i], sq_sem.at[0], sq_sem.at[1], device_id=at(a, b), device_id_type=MESH
        )

    all_squares = pltpu.make_async_remote_copy(
        sq_in, sq_in, sq_sem.at[0], sq_sem.at[1], device_id=at(1), device_id_type=MESH
    )
    for i in range(len(peers)):
        sq_copy(i).start()
    for s in range(n):

        @pl.when(me == s)
        def _(s=s):
            drain(s, True)
            drain(s, False)
            if s > 0:
                log_copy(steps - 1).wait_send()

    @pl.when(me < n - 1)
    def _():
        for k in halo_parts:
            halo_copy(k).wait_send()

    @pl.when(me > 0)
    def _():
        newest_copy().wait_send()

    all_squares.wait_recv()
    for i in range(len(peers)):
        sq = sq + sq_in[i]
    mean = jnp.sum(diagonal * sq, axis=1, keepdims=True) / (HEADS * P_SIZE)
    scale = lax.rsqrt(mean + epsilon)
    read_ref[...] = (gated * scale * gain_here).astype(BF16)[0:S]

    all_squares.wait_send()


def on_chip(array):
    return pltpu.with_memory_space_constraint(array, pltpu.VMEM)


def emit_kernel(dims, cache_ref, read_ref, cache_hbm, out_hbm, out, sem):
    heads, R = dims
    S, RH = read_ref.shape
    copies = [
        pltpu.make_async_copy(cache_ref, cache_hbm, sem.at[0]),
        pltpu.make_async_copy(out, out_hbm, sem.at[1]),
    ]
    copies[0].start()
    spread = ones_where((heads, RH), lambda h, l: h == lax.div(l, R))
    pick = ones_where((RH, R), lambda l, r: lax.rem(l, R) == r, BF16)
    value = read_ref[...].astype(F32)
    rows = jnp.concatenate([value[p : p + 1] * spread for p in range(S)], axis=0).astype(BF16)
    picked = jnp.dot(rows, pick, preferred_element_type=F32)
    out[...] = picked.reshape(S, heads, R).astype(BF16)
    copies[1].start()
    for c in copies:
        c.wait()


LEAD, RELAY_LAG, FORWARD_AT = 1, 1, 2
FAR, NEAR, FINAL = 0, 1, 2
SMALL = (1, 7, 8, 9, 10, 11, 12, 13)
RING, END_NEARS = 4, 2
END_BEHIND, MID_BEHIND = 5, 2


def fused(*args):
    x, wv, wk = args[0], args[2], args[4]
    S, L, D = x.shape
    n, m = lax.axis_size("sp"), lax.axis_size("tp")
    F = wv.shape[1]
    heads = F // P_SIZE
    R = P_SIZE // n
    G = next(g for g in (2, 3, 1) if S % g == 0)
    steps = S // G
    slots = min(LEAD, steps)
    halo_rows = -(-G * (CONV - 1) // 8) * 8
    C, RH, SP = F + STATE, heads * R, 16
    dims = (n, m, S, L, heads, R, G)
    flat = list(args)
    for i in (10, 11, 12):
        flat[i] = args[i].reshape(1, HEADS)
    flat[6] = args[6].T
    flat[14] = jnp.swapaxes(args[14], 1, 2)
    hbm, vmem = pl.BlockSpec(memory_space=pl.ANY), pl.BlockSpec(memory_space=pltpu.VMEM)
    specs = [hbm] * len(flat)
    dma = pltpu.SemaphoreType.DMA
    cache, read = pl.pallas_call(
        lambda *refs: mixer_kernel(dims, *refs),
        out_shape=(
            pltpu.VMEM((S, RH, STATE), BF16),
            pltpu.VMEM((S, RH), BF16),
        ),
        in_specs=specs,
        out_specs=(vmem, vmem),
        scratch_shapes=[
            *[pltpu.VMEM(flat[i].shape, flat[i].dtype) for i in SMALL],
            pltpu.VMEM((S, L, D), BF16),
            pltpu.VMEM((S + 1, 16, D), BF16),
            pltpu.VMEM(((S + 1) * 16, C + STATE), F32),
            pltpu.VMEM((D, 128 + C + STATE), BF16),
            pltpu.VMEM((heads, D), BF16),
            pltpu.VMEM((D, F), BF16),
            pltpu.VMEM((S, heads, L), F32),
            pltpu.VMEM((CONV, C + STATE), F32),
            pltpu.VMEM((slots, G, 8 + L, C), F32),
            pltpu.VMEM((slots, G, 2 * heads, L), BF16),
            pltpu.VMEM((steps, halo_rows, C), BF16),
            pltpu.VMEM((steps, halo_rows, C), BF16),
            pltpu.VMEM((SP, C + STATE), F32),
            pltpu.VMEM((2, HEADS, 128), F32),
            pltpu.VMEM((S, heads, 128), F32),
            pltpu.VMEM((S, 1, 128), F32),
            pltpu.VMEM((S, 1, 128), F32),
            pltpu.VMEM((S, 1, 128), F32),
            pltpu.VMEM((S, n, RH, STATE), BF16),
            pltpu.VMEM((S, n, RH, STATE), BF16),
            pltpu.VMEM((S, n, RH, STATE), BF16),
            pltpu.VMEM((1, 128), F32),
            pltpu.VMEM((n * m - 1, 1, 128), F32),
            pltpu.VMEM((2 * heads, F), BF16),
            dma((16,)),
            dma((2, 2)),
            dma((2,)),
            dma((3, RING)),
            dma((2, S)),
            dma((2, steps)),
            dma((1,)),
            dma((steps,)),
            dma((2,)),
        ],
        compiler_params=pltpu.CompilerParams(
            collective_id=0, has_side_effects=True, vmem_limit_bytes=56 * 1024 * 1024
        ),
    )(*flat)
    cache, read = pl.pallas_call(
        lambda *refs: emit_kernel((heads, R), *refs),
        out_shape=(
            jax.ShapeDtypeStruct((S, RH, STATE), BF16),
            jax.ShapeDtypeStruct((S, heads, R), BF16),
        ),
        in_specs=[vmem, vmem],
        out_specs=(pl.BlockSpec(memory_space=pltpu.HBM),) * 2,
        scratch_shapes=[pltpu.VMEM((S, heads, R), BF16), dma((2,))],
    )(on_chip(cache), on_chip(read))
    return cache.reshape(S, heads, R, STATE), read


def fits(n, m, shapes):
    (S, L), F = shapes
    heads, R = F // P_SIZE, P_SIZE // n
    return (
        n > 1
        and F % 128 == 0
        and heads % 8 == 0
        and R % 16 == 0
        and (heads * R) % 128 == 0
        and S <= 16
        and L % 16 == 0
        and L == 128
        and (HEADS // GROUPS) % heads == 0
    )


def part(*args):
    shapes = (args[0].shape[:2], args[2].shape[1])
    if fits(lax.axis_size("sp"), lax.axis_size("tp"), shapes):
        return fused(*args)
    return shards(*args)


def solution(mesh):
    in_specs = (
        P("grp", "sp", None),
        P("grp", None),
        P(None, "tp"),
        P(None, "tp"),
        P(),
        P(),
        P(),
        P(),
        P(),
        P(),
        P(),
        P(),
        P(),
        P(),
        P("grp", "sp", None),
    )
    out_specs = (P("grp", "tp", "sp", None), P("grp", "tp", "sp"))
    return jax.shard_map(part, mesh=mesh, in_specs=in_specs, out_specs=out_specs, check_vma=False)
```

```python
import jax
import jax.numpy as jnp
from jax import lax
from jax.experimental import pallas as pl
from jax.experimental.pallas import tpu as pltpu
from jax.sharding import PartitionSpec as P

HEADS = 32
P_SIZE = 64
GROUPS = 2
STATE = 128
CONV = 4
SPAN = 64


epsilon = 1e-06


def shifted(block, axis, distance):
    devices = range(lax.axis_size(axis))
    route = [(i - distance, i) for i in devices if i - distance in devices]
    return lax.ppermute(block, axis, route)


def broadcast(value, axis, source):
    kept = jnp.where(lax.axis_index(axis) == source, value, 0).astype(value.dtype)
    return lax.psum(kept, axis)


def prefix(shard, axis, combine, identity):
    length, here = (lax.axis_size(axis), lax.axis_index(axis))
    everything = lax.all_gather(shard, axis)
    start = jnp.broadcast_to(jnp.asarray(identity, shard.dtype), shard.shape)

    def lap(k, before):
        at = length - 1 - k
        reached = at > here
        new = combine(before, everything[at])
        return jnp.where(reached, new, before)

    return lax.fori_loop(0, length, lap, start)


def shards(
    prompt_layer_input,
    next_token_input,
    value_projection,
    output_gate_matrix,
    key_projection,
    query_projection,
    step_projection,
    value_filter_taps,
    key_filter_taps,
    query_filter_taps,
    step_size_bias,
    head_decay_logarithm,
    direct_path_weight,
    gated_norm_gain,
    position_decay_offset,
):
    seq_count, local_len, width = prompt_layer_input.shape
    resident_heads = value_projection.shape[1] // P_SIZE
    feature_cols = resident_heads * P_SIZE
    shard_count = lax.axis_size("sp")
    rows_here = P_SIZE // shard_count
    shard_index = lax.axis_index("sp")
    leading_head = lax.axis_index("tp") * resident_heads
    group_index = leading_head // (HEADS // GROUPS)
    row_first = shard_index * rows_here
    in_cols = lax.dynamic_slice_in_dim(key_projection, group_index * STATE, STATE, 1)
    out_cols = lax.dynamic_slice_in_dim(query_projection, group_index * STATE, STATE, 1)
    weights_here = jnp.concatenate([value_projection, in_cols, out_cols], axis=1)
    step_cols = lax.dynamic_slice_in_dim(step_projection, leading_head, resident_heads, 1)
    kernel = jnp.concatenate(
        [
            lax.dynamic_slice_in_dim(value_filter_taps, leading_head * P_SIZE, feature_cols, 1),
            lax.dynamic_slice_in_dim(key_filter_taps, group_index * STATE, STATE, 1),
            lax.dynamic_slice_in_dim(query_filter_taps, group_index * STATE, STATE, 1),
        ],
        axis=1,
    ).astype(jnp.float32)
    head_decay_speed = jnp.exp(
        lax.dynamic_slice_in_dim(head_decay_logarithm, leading_head, resident_heads, 0)
    )
    bias_here = lax.dynamic_slice_in_dim(step_size_bias, leading_head, resident_heads, 0)
    skip_here = lax.dynamic_slice_in_dim(direct_path_weight, leading_head, resident_heads, 0)
    gain_here = lax.dynamic_slice(
        gated_norm_gain, (leading_head, row_first), (resident_heads, rows_here)
    )
    token_rows = prompt_layer_input.reshape(seq_count * local_len, width)
    projected = jnp.dot(token_rows, weights_here, preferred_element_type=jnp.float32).astype(
        jnp.bfloat16
    )
    projected = projected.reshape(seq_count, local_len, feature_cols + 2 * STATE)
    trailing = projected[:, local_len - (CONV - 1) :]
    before = shifted(trailing, "sp", 1)
    newest = broadcast(trailing, "sp", shard_count - 1)
    padded = jnp.concatenate([before, projected], axis=1)
    total = padded[:, 0:local_len].astype(jnp.float32) * kernel[0]
    for tap in range(1, CONV):
        total = total + padded[:, tap : tap + local_len].astype(jnp.float32) * kernel[tap]
    mixed = jax.nn.silu(total).astype(jnp.bfloat16)
    step_raw = jnp.dot(token_rows, step_cols, preferred_element_type=jnp.float32).astype(
        jnp.bfloat16
    )
    discrete_step = jax.nn.softplus(step_raw.astype(jnp.float32) + bias_here).reshape(
        seq_count, local_len, resident_heads
    )
    decay_spikes = lax.dynamic_slice_in_dim(position_decay_offset, leading_head, resident_heads, 2)
    logarithmic_decay = decay_spikes - head_decay_speed * discrete_step
    block_count = local_len // SPAN
    cumulative = jnp.cumsum(
        logarithmic_decay.reshape(seq_count, block_count, SPAN, resident_heads), axis=2
    )
    decay_weight = jnp.exp(cumulative[:, :, -1:] - cumulative) * discrete_step.reshape(
        seq_count, block_count, SPAN, resident_heads
    )
    head_input = mixed[:, :, :feature_cols].reshape(
        seq_count, block_count, SPAN, resident_heads, P_SIZE
    )
    weighted = (head_input.astype(jnp.float32) * decay_weight[..., None]).astype(jnp.bfloat16)
    in_map = mixed[:, :, feature_cols : feature_cols + STATE].reshape(
        seq_count, block_count, SPAN, STATE
    )
    block_state = jnp.einsum(
        "bcshp,bcsn->bchpn", weighted, in_map, preferred_element_type=jnp.float32
    )
    block_log = cumulative[:, :, -1]
    own_log = jnp.sum(block_log, axis=1)
    after_block = jnp.exp(own_log[:, None] - jnp.cumsum(block_log, axis=1))
    local_state = jnp.sum(after_block[..., None, None] * block_state, axis=1)
    later_log = prefix(own_log, "sp", jnp.add, jnp.zeros_like(own_log))
    scaled = jnp.exp(later_log)[:, :, None, None] * local_state
    own_rows = lax.psum_scatter(scaled, "sp", scatter_dimension=2, tiled=True)
    state_cache = own_rows.astype(jnp.bfloat16)
    new_raw = jnp.dot(next_token_input, weights_here, preferred_element_type=jnp.float32).astype(
        jnp.bfloat16
    )
    new_step = jnp.dot(next_token_input, step_cols, preferred_element_type=jnp.float32).astype(
        jnp.bfloat16
    )
    new_gate = jnp.dot(
        next_token_input, output_gate_matrix, preferred_element_type=jnp.float32
    ).astype(jnp.bfloat16)
    window = jnp.concatenate([newest, new_raw[:, None]], axis=1)
    new_mixed = jax.nn.silu(jnp.sum(window.astype(jnp.float32) * kernel[None], axis=1)).astype(
        jnp.bfloat16
    )
    new_input = lax.dynamic_slice_in_dim(
        new_mixed[:, :feature_cols].reshape(seq_count, resident_heads, P_SIZE),
        row_first,
        rows_here,
        2,
    ).astype(jnp.float32)
    new_in = new_mixed[:, feature_cols : feature_cols + STATE].astype(jnp.float32)
    new_out = new_mixed[:, feature_cols + STATE :].astype(jnp.float32)
    new_step_size = jax.nn.softplus(new_step.astype(jnp.float32) + bias_here)
    cache_values = lax.optimization_barrier(state_cache).astype(jnp.float32)
    new_state = (
        jnp.exp(-head_decay_speed * new_step_size)[:, :, None, None] * cache_values
        + (new_step_size[:, :, None] * new_input)[..., None] * new_in[:, None, None, :]
    )
    readout = (
        jnp.sum(new_state * new_out[:, None, None, :], axis=-1)
        + skip_here[None, :, None] * new_input
    )
    gate_rows = lax.dynamic_slice_in_dim(
        new_gate.reshape(seq_count, resident_heads, P_SIZE), row_first, rows_here, 2
    )
    gated = readout * jax.nn.silu(gate_rows.astype(jnp.float32))
    squares = lax.psum(jnp.sum(gated * gated, axis=(1, 2)), ("sp", "tp"))
    scale = lax.rsqrt(squares / (HEADS * P_SIZE) + epsilon)
    first_read = (gated * scale[:, None, None] * gain_here[None]).astype(jnp.bfloat16)
    return (state_cache, first_read)


F32, BF16 = jnp.float32, jnp.bfloat16
MESH = pl.DeviceIdType.MESH
EXACT = lax.Precision.HIGHEST


def exact_dot(a, b, dims=((1,), (0,))):
    return lax.dot_general(a, b, (dims, ((), ())), precision=EXACT, preferred_element_type=F32)


def softplus(v):
    return jnp.maximum(v, 0.0) + jnp.log1p(jnp.exp(-jnp.abs(v)))


def silu(v):
    return v / (1.0 + jnp.exp(-v))


def ones_where(shape, test, dtype=F32):
    rows = lax.broadcasted_iota(jnp.int32, shape, 0)
    cols = lax.broadcasted_iota(jnp.int32, shape, 1)
    return jnp.where(test(rows, cols), 1.0, 0.0).astype(dtype)


def mixer_kernel(
    dims,
    x_hbm,
    next_hbm,
    wv_hbm,
    wg_hbm,
    wk_hbm,
    wq_hbm,
    ws_hbm,
    tv_hbm,
    tk_hbm,
    tq_hbm,
    bias_hbm,
    speed_hbm,
    skip_hbm,
    gain_hbm,
    off_hbm,
    cache_ref,
    read_ref,
    next_ref,
    tv_ref,
    tk_ref,
    tq_ref,
    bias_ref,
    speed_ref,
    skip_ref,
    gain_ref,
    xbuf,
    edge,
    early,
    wall,
    ws,
    wg,
    off,
    taps,
    pad,
    wsplit,
    halo_out,
    halo_in,
    newest,
    heads_t,
    decay,
    log_own,
    log_out,
    log_in,
    own,
    from_left,
    from_right,
    sq_out,
    sq_in,
    expand,
    load_sem,
    halo_sem,
    new_sem,
    st_send,
    st_recv,
    near_recv,
    log_send,
    log_recv,
    sq_sem,
):
    n, m, S, L, heads, R, G = dims
    F = heads * P_SIZE
    C = F + STATE
    RH = heads * R
    SP = 16
    steps = S // G
    lead_steps = min(LEAD, steps)
    me, tp = lax.axis_index("sp"), lax.axis_index("tp")
    lead = pl.multiple_of(tp * heads, 8)
    group = lax.div(lead, HEADS // GROUPS)
    fcol = pl.multiple_of(tp * F, 128)
    gcol = pl.multiple_of(group * STATE, 128)

    def load(src, dst, k):
        c = pltpu.make_async_copy(src, dst, load_sem.at[k])
        c.start()
        return c

    def load_x(k):
        here = pl.ds(0, G) if k == 0 else pl.ds(G, S - G)
        return pltpu.make_async_copy(x_hbm.at[here], xbuf.at[here], load_sem.at[k])

    half = x_hbm.shape[2] // 2

    def weights(k):
        rows = pl.ds(k * half, half)
        maps = pl.ds(gcol, STATE)
        return [
            load(wk_hbm.at[rows, maps], wall.at[rows, pl.ds(128 + F, STATE)], 10 + 3 * k),
            load(wq_hbm.at[rows, maps], wall.at[rows, pl.ds(128 + C, STATE)], 11 + 3 * k),
            load(wv_hbm.at[rows], wall.at[rows, pl.ds(128, F)], 12 + 3 * k),
        ]

    first = [
        load(next_hbm, next_ref, 0),
        load(ws_hbm.at[pl.ds(lead, heads), :], ws, 8),
        load(x_hbm.at[:, pl.ds(L - 16, 16)], edge.at[pl.ds(0, S)], 9),
    ]
    first += weights(0)
    second = weights(1)
    small = [
        load(a, b, 1 + k)
        for k, (a, b) in enumerate(
            [
                (tv_hbm, tv_ref),
                (tk_hbm, tk_ref),
                (tq_hbm, tq_ref),
                (bias_hbm, bias_ref),
                (speed_hbm, speed_ref),
                (skip_hbm, skip_ref),
                (gain_hbm, gain_ref),
            ]
        )
    ]

    peers = [(a, b) for a in range(n) for b in range(m) if (a, b) != (0, 0)]

    def at(a, b=0):
        return {"sp": lax.rem(me + a, n), "tp": lax.rem(tp + b, m)}

    barrier = pltpu.get_barrier_semaphore()
    for a, b in peers:
        pl.semaphore_signal(barrier, inc=1, device_id=at(a, b), device_id_type=MESH)

    head_of = ones_where((heads, F), lambda i, c: i == lax.div(c, P_SIZE))
    expand[...] = jnp.concatenate([head_of, head_of], axis=0).astype(BF16)
    @pl.when(me == 0)
    def _():
        from_left[:, 0] = jnp.zeros((S, RH, STATE), BF16)

    @pl.when(me == n - 1)
    def _():
        from_right[:, n - 1] = jnp.zeros((S, RH, STATE), BF16)
        log_in[...] = jnp.zeros_like(log_in)

    eye = ones_where((heads, 128), lambda i, c: i == c)
    later_ones = ones_where((L, L), lambda u, t: u > t, BF16)

    for c in first:
        c.wait()
    edge[S] = jnp.zeros(edge.shape[1:], BF16)
    edge[S, 0:S, :] = next_ref[...]
    rows = edge[...].reshape((S + 1) * 16, edge.shape[2])
    halo_out[...] = jnp.zeros_like(halo_out)
    early[...] = jnp.dot(rows[:, 0:half], wall[0:half, 128:], preferred_element_type=F32)
    for c in second + small:
        c.wait()
    load_x(0).start()
    off_load = load(off_hbm.at[:, pl.ds(lead, heads), :], off, 2)
    late = jnp.dot(rows[:, half:], wall[half:, 128:], preferred_element_type=F32)
    part = early[...] + late
    edge_rows = part.astype(BF16).astype(F32).reshape(S + 1, 16, C + STATE)

    def tails(prompts):
        for p in prompts:
            r = p % G * (CONV - 1)
            tail = edge_rows[p, 16 - (CONV - 1) :, 0:C]
            halo_out[p // G, r : r + CONV - 1, :] = tail.astype(BF16)

    tails(range(G))
    if steps > 1:
        load_x(1).start()
    gate_load = load(wg_hbm, wg, 3)
    pl.semaphore_wait(barrier, len(peers))

    def halo_copy(k):
        here = pl.ds(0, 1) if k == 0 else pl.ds(1, steps - 1)
        return pltpu.make_async_remote_copy(
            halo_out.at[here],
            halo_in.at[here],
            halo_sem.at[0, k],
            halo_sem.at[1, k],
            device_id=at(1),
            device_id_type=MESH,
        )

    halo_parts = range(2 if steps > 1 else 1)

    @pl.when(me < n - 1)
    def _():
        halo_copy(0).start()

    taps[:, 0:F] = tv_ref[:, pl.ds(fcol, F)].astype(F32)
    taps[:, F:C] = tk_ref[:, pl.ds(gcol, STATE)].astype(F32)
    taps[:, C : C + STATE] = tq_ref[:, pl.ds(gcol, STATE)].astype(F32)
    bias = bias_ref[...]
    speed = jnp.exp(speed_ref[...])
    square = jnp.zeros((128, 128 - HEADS), F32)

    def columns(row, k):
        full = jnp.concatenate([jnp.broadcast_to(row, (128, HEADS)), square], axis=1)
        heads_t[k] = full.T[0:HEADS]
        return heads_t[k, pl.ds(lead, heads), :]

    bias_t, speed_t = columns(bias, 0), columns(speed, 1)
    tails(range(G, S))

    @pl.when(me < n - 1)
    def _():
        for k in halo_parts[1:]:
            halo_copy(k).start()

    def newest_copy():
        return pltpu.make_async_remote_copy(
            newest,
            newest,
            new_sem.at[0],
            new_sem.at[1],
            device_id=at(n - 1),
            device_id_type=MESH,
        )

    last = 16 - (CONV - 1)

    @pl.when(me == n - 1)
    def _():
        newest[...] = jnp.zeros_like(newest)
        newest[0:S, :] = sum(
            edge_rows[0:S, last + j, :] * taps[j : j + 1, :] for j in range(CONV - 1)
        )
        newest_copy().start()

    new_raw = edge_rows[S]
    wall[:, 0:128] = jnp.concatenate(
        [ws[...], jnp.zeros((128 - heads, ws.shape[1]), BF16)], axis=0
    ).T

    def span(s, right, far):
        if right:
            return (s + 2, n) if far else (s + 1, s + 2)
        return (0, s - 1) if far else (s - 1, s)

    def is_end(s, right):
        return s == (0 if right else n - 1)

    def kinds(s, right):
        if not 0 <= (s + 1 if right else s - 1) < n:
            return ()
        if is_end(s, right):
            return (FAR, NEAR) if n > 2 else (NEAR,)
        return (FINAL,) if (s + 1 == n - 1 if right else s - 1 == 0) else (FAR, NEAR)

    def message(i, s, right, kind):
        lo, hi = span(s, right, kind == FAR)
        here = (pl.ds(i * G, G) if kind == NEAR else i, pl.ds(lo, hi - lo))
        lane = 0 if is_end(s, right) else 1
        return pltpu.make_async_remote_copy(
            own.at[here],
            (from_left if right else from_right).at[here],
            st_send.at[kind, lax.rem(i, RING)],
            (near_recv if kind == NEAR else st_recv).at[lane, i],
            device_id=at(1 if right else n - 1),
            device_id_type=MESH,
        )

    def flight(s, right, kind):
        return END_NEARS if kind == NEAR and is_end(s, right) else RING

    def send(i, s, right, kind):
        depth = flight(s, right, kind)

        @pl.when(i >= depth)
        def _():
            message(i - depth, s, right, kind).wait_send()

        message(i, s, right, kind).start()

    def drain(s, right):
        for kind in kinds(s, right):
            total = steps if kind == NEAR else S
            for i in range(max(0, total - flight(s, right, kind)), total):
                message(i, s, right, kind).wait_send()

    def send_prompt(g, q, s, right):
        behind = END_BEHIND if is_end(s, right) else MID_BEHIND
        for kind in kinds(s, right):
            if kind != NEAR:
                send(g * G + q, s, right, kind)
            elif q == G - 1:

                @pl.when(g >= behind)
                def _():
                    send(g - behind, s, right, NEAR)

    def send_rest(s, right):
        behind = END_BEHIND if is_end(s, right) else MID_BEHIND
        if NEAR in kinds(s, right):

            def one(g, carry):
                send(g, s, right, NEAR)
                return carry

            lax.fori_loop(max(0, steps - behind), steps, one, 0)

    def log_copy(g):
        here = pl.ds(g * G, G)
        return pltpu.make_async_remote_copy(
            log_out.at[here],
            log_in.at[here],
            log_send.at[0],
            log_recv.at[g],
            device_id=at(n - 1),
            device_id_type=MESH,
        )

    def last_log_left(g):
        @pl.when(g >= 1)
        def _():
            log_copy(g - 1).wait_send()

    def project(g):
        @pl.when(g == 0)
        def _():
            load_x(0).wait()

        if steps > 1:

            @pl.when(g == 1)
            def _():
                load_x(1).wait()

        slot = lax.rem(g, lead_steps)
        xg = xbuf[pl.ds(g * G, G)].reshape(G * L, xbuf.shape[2])
        acc = jnp.dot(xg, wall[:, 0 : 128 + C], preferred_element_type=F32).astype(BF16).astype(F32)
        for q in range(G):
            p = g * G + q
            raw = acc[q * L : (q + 1) * L]
            pad[slot, q, 8 : 8 + L, :] = raw[:, 128:]
            dt = softplus(raw[:, 0:128].T[0:heads] + bias_t)
            ld = off[p] - speed_t * dt
            a = ld.astype(BF16).astype(F32)
            b = (ld - a).astype(BF16).astype(F32)
            parts = jnp.concatenate([a, b, ld - a - b, jnp.zeros_like(a)], axis=0).astype(BF16)
            sums = jnp.dot(parts, later_ones, preferred_element_type=F32)
            suffix = sums[0:heads] + sums[heads : 2 * heads] + sums[2 * heads : 3 * heads]
            whole = jnp.broadcast_to(suffix[:, 0:1] + ld[:, 0:1], (heads, 128))
            decay[p] = jnp.exp(whole)
            log_own[p] = jnp.sum(whole * eye, axis=0, keepdims=True)
            w = dt * jnp.exp(suffix)
            hi = w.astype(BF16).astype(F32)
            wsplit[slot, q] = jnp.concatenate([hi, w - hi], axis=0).astype(BF16)

    def states(g):
        slot = lax.rem(g, lead_steps)

        @pl.when(me == n - 1)
        def _():
            for q in range(G):
                log_out[g * G + q] = log_own[g * G + q]
            last_log_left(g)
            log_copy(g).start()

        for q in range(G):
            p = g * G + q
            wide = lax.dot_general(
                wsplit[slot, q],
                expand[...],
                (((0,), (0,)), ((), ())),
                preferred_element_type=F32,
            )

            def mixed(c, a, b):
                s = slice(c, c + 128)
                t = jnp.zeros((b - a, 128), F32)
                for j in range(CONV):
                    r = 8 - (CONV - 1) + j
                    t = t + pad[slot, q, r + a : r + b, s] * taps[j : j + 1, s]
                return silu(t).astype(BF16).astype(F32)

            columns = range(0, C, 128)
            later = [mixed(c, 8, L) for c in columns]
            if q == 0:
                for k in halo_parts:

                    @pl.when((g == k) & (me > 0))
                    def _(k=k):
                        halo_copy(k).wait_recv()

            r = q * (CONV - 1)
            pad[slot, q, 8 - (CONV - 1) : 8, :] = halo_in[g, r : r + CONV - 1, :].astype(F32)
            whole = [
                jnp.concatenate([mixed(c, 0, 8), late], axis=0)
                for c, late in zip(columns, later)
            ]
            in_map = whole[-1].astype(BF16)
            for c in range(0, F, 128):
                weighted = (whole[c // 128] * wide[:, c : c + 128]).astype(BF16)
                share = lax.dot_general(
                    weighted, in_map, (((0,), (0,)), ((), ())), preferred_element_type=F32
                ).astype(BF16)
                for hh in range(128 // P_SIZE):
                    h = c // P_SIZE + hh
                    for d in range(n):
                        b = hh * P_SIZE + d * R
                        own[p, d, h * R : (h + 1) * R, :] = share[b : b + R]

            @pl.when(me == 0)
            def _(q=q):
                send_prompt(g, q, 0, True)

            @pl.when(me == n - 1)
            def _(q=q):
                send_prompt(g, q, n - 1, False)

    def later_factor(p):
        row = jnp.sum(eye * log_in[p], axis=1, keepdims=True)
        return jnp.exp(jnp.broadcast_to(row, (heads, 128)))

    def sum_right(g, q, s):
        p = g * G + q
        message(p, s - 1, True, FAR).wait_recv()
        factor = decay[p]
        for d in reversed(range(s + 1, n)):
            for h in range(heads):
                z = (p, d, slice(h * R, (h + 1) * R))
                got = from_left[z].astype(F32) * factor[h : h + 1, :]
                own[z] = (own[z].astype(F32) + got).astype(BF16)
        send_prompt(g, q, s, True)

    def sum_left(g, q, s):
        p = g * G + q
        message(p, s + 1, False, FAR).wait_recv()
        factor = later_factor(p)
        for d in range(s):
            for h in range(heads):
                z = (p, d, slice(h * R, (h + 1) * R))
                mine = own[z].astype(F32) * factor[h : h + 1, :]
                own[z] = (from_right[z].astype(F32) + mine).astype(BF16)
        send_prompt(g, q, s, False)

    def pass_log(g):
        log_copy(g).wait_recv()
        last_log_left(g)
        for q in range(G):
            log_out[g * G + q] = log_in[g * G + q] + log_own[g * G + q]
        log_copy(g).start()

    def relay(g, outer):
        for s in range(1, n - 1):

            @pl.when(me == s)
            def _(s=s):
                for q in range(G):
                    if outer == (s < n - 1 - s):
                        sum_right(g, q, s)
                    else:
                        sum_left(g, q, s)

    off_load.wait()
    lax.fori_loop(0, lead_steps, lambda g, carry: (project(g), carry)[1], 0)
    @pl.when(me == 0)
    def _():
        halo_in[...] = jnp.zeros_like(halo_in)

    relay_lag = min(RELAY_LAG, steps)

    def step(g, carry):
        states(g)

        @pl.when(g + lead_steps < steps)
        def _():
            project(g + lead_steps)

        if n > 2:

            for s in range(1, n - 1):

                @pl.when((g == min(FORWARD_AT * (n - 1 - s), steps - 1)) & (me == s))
                def _():
                    newest_copy().wait_recv()
                    newest_copy().start()

        for s in range(1, n - 1):

            @pl.when((me == s) & (g >= n - 2 - s))
            def _(s=s):
                pass_log(g - (n - 2 - s))

        @pl.when(g >= relay_lag)
        def _():
            relay(g - relay_lag, True)

        @pl.when(g >= relay_lag + 1)
        def _():
            relay(g - relay_lag - 1, False)

        return carry

    lax.fori_loop(0, steps, step, 0)
    head_cols = ones_where((HEADS, RH), lambda i, l: i == lead + lax.div(l, R))
    local_cols = ones_where((128, RH), lambda i, l: i == lax.div(l, R))
    local = ones_where((HEADS, 128), lambda i, c: (i == lead + c) & (c < heads))
    pick = ones_where(
        (F, RH), lambda c, l: c == lax.div(l, R) * P_SIZE + me * R + lax.rem(l, R), BF16
    )
    row_pick = ones_where((P_SIZE, RH), lambda c, l: c == me * R + lax.rem(l, R))
    gate_load.wait()
    gate = jnp.dot(edge[S], wg[...], preferred_element_type=F32).astype(BF16)
    gate_here = silu(jnp.dot(gate, pick, preferred_element_type=F32))
    gain_here = jnp.sum(exact_dot(gain_ref[...], row_pick) * head_cols, axis=0, keepdims=True)
    skip_here = exact_dot(skip_ref[...], head_cols)
    new_step = jnp.dot(edge[S], wall[:, 0:128], preferred_element_type=F32).astype(BF16)
    new_dt = softplus(new_step.astype(F32) + exact_dot(bias, local))
    dt_here = exact_dot(new_dt, local_cols)
    keep_here = jnp.exp(-exact_dot(exact_dot(speed, local) * new_dt, local_cols))

    @pl.when(me == 0)
    def _():
        newest_copy().wait_recv()

    new_mixed = silu(newest[...] + new_raw * taps[CONV - 1 : CONV, :]).astype(BF16)
    new_input = jnp.dot(new_mixed[:, 0:F], pick, preferred_element_type=F32)
    new_in = new_mixed[:, F:C].astype(F32)
    new_out = new_mixed[:, C : C + STATE]
    both = jnp.sum(new_in * new_out.astype(F32), axis=1, keepdims=True)
    where_row = lax.broadcasted_iota(jnp.int32, (SP, RH), 0)

    def rest(outer):
        for s in range(n):
            for right in (True, False):
                if outer == (is_end(s, right) or (s < n - 1 - s) == right):

                    @pl.when(me == s)
                    def _(s=s, right=right):
                        send_rest(s, right)

    def arrivals(g, s, right):
        if FINAL in kinds(s, right):
            for q in range(G):
                message(g * G + q, s, right, FINAL).wait_recv()
        elif NEAR in kinds(s, right):
            message(g, s, right, NEAR).wait_recv()

    def finish(g, y):
        for s in range(n):

            @pl.when(me == s)
            def _(s=s):
                if s > 0:
                    arrivals(g, s - 1, True)
                if s == 0:
                    log_copy(g).wait_recv()
                if s < n - 1:
                    arrivals(g, s + 1, False)

        for q in range(G):
            p = g * G + q
            before, after = decay[p], later_factor(p)
            kept = []
            for h in range(heads):
                z = (p, me, slice(h * R, (h + 1) * R))
                t = own[z].astype(F32) + from_left[z].astype(F32) * before[h : h + 1, :]
                t = t * after[h : h + 1, :] + from_right[z].astype(F32)
                kept.append(t.astype(BF16))
            kept = jnp.concatenate(kept, axis=0)
            cache_ref[p] = kept
            part = lax.dot_general(
                new_out, kept, (((1,), (1,)), ((), ())), preferred_element_type=F32
            )
            y = jnp.where(where_row == p, part, y)
        return y

    for s in range(1, n - 2):

        @pl.when(me == s)
        def _(s=s):
            for g in range(max(0, steps - (n - 2 - s)), steps):
                pass_log(g)

    for g in range(steps - relay_lag, steps):
        relay(g, True)
        if g > 0:
            relay(g - 1, False)
    rest(True)
    relay(steps - 1, False)
    rest(False)
    y = lax.fori_loop(0, steps, finish, jnp.zeros((SP, RH), F32))

    readout = keep_here * y + dt_here * new_input * both + skip_here * new_input
    gated = readout * gate_here
    square_sum = jnp.broadcast_to(jnp.sum(gated * gated, axis=1, keepdims=True), (SP, 128))
    diagonal = ones_where((SP, 128), lambda i, c: i == c)
    sq = jnp.sum(square_sum * diagonal, axis=0, keepdims=True)
    sq_out[...] = sq

    def sq_copy(i):
        a, b = peers[i]
        return pltpu.make_async_remote_copy(
            sq_out, sq_in.at[i], sq_sem.at[0], sq_sem.at[1], device_id=at(a, b), device_id_type=MESH
        )

    all_squares = pltpu.make_async_remote_copy(
        sq_in, sq_in, sq_sem.at[0], sq_sem.at[1], device_id=at(1), device_id_type=MESH
    )
    for i in range(len(peers)):
        sq_copy(i).start()
    for s in range(n):

        @pl.when(me == s)
        def _(s=s):
            drain(s, True)
            drain(s, False)
            if s > 0:
                log_copy(steps - 1).wait_send()

    @pl.when(me < n - 1)
    def _():
        for k in halo_parts:
            halo_copy(k).wait_send()

    @pl.when(me > 0)
    def _():
        newest_copy().wait_send()

    all_squares.wait_recv()
    for i in range(len(peers)):
        sq = sq + sq_in[i]
    mean = jnp.sum(diagonal * sq, axis=1, keepdims=True) / (HEADS * P_SIZE)
    scale = lax.rsqrt(mean + epsilon)
    read_ref[...] = (gated * scale * gain_here).astype(BF16)[0:S]

    all_squares.wait_send()


def on_chip(array):
    return pltpu.with_memory_space_constraint(array, pltpu.VMEM)


def emit_kernel(dims, cache_ref, read_ref, cache_hbm, out_hbm, out, sem):
    heads, R = dims
    S, RH = read_ref.shape
    copies = [
        pltpu.make_async_copy(cache_ref, cache_hbm, sem.at[0]),
        pltpu.make_async_copy(out, out_hbm, sem.at[1]),
    ]
    copies[0].start()
    spread = ones_where((heads, RH), lambda h, l: h == lax.div(l, R))
    pick = ones_where((RH, R), lambda l, r: lax.rem(l, R) == r, BF16)
    value = read_ref[...].astype(F32)
    rows = jnp.concatenate([value[p : p + 1] * spread for p in range(S)], axis=0).astype(BF16)
    picked = jnp.dot(rows, pick, preferred_element_type=F32)
    out[...] = picked.reshape(S, heads, R).astype(BF16)
    copies[1].start()
    for c in copies:
        c.wait()


LEAD, RELAY_LAG, FORWARD_AT = 1, 1, 2
FAR, NEAR, FINAL = 0, 1, 2
SMALL = (1, 7, 8, 9, 10, 11, 12, 13)
RING, END_NEARS = 2, 2
END_BEHIND, MID_BEHIND = 5, 1


def fused(*args):
    x, wv, wk = args[0], args[2], args[4]
    S, L, D = x.shape
    n, m = lax.axis_size("sp"), lax.axis_size("tp")
    F = wv.shape[1]
    heads = F // P_SIZE
    R = P_SIZE // n
    G = next(g for g in (2, 3, 1) if S % g == 0)
    steps = S // G
    slots = min(LEAD, steps)
    halo_rows = -(-G * (CONV - 1) // 8) * 8
    C, RH, SP = F + STATE, heads * R, 16
    dims = (n, m, S, L, heads, R, G)
    flat = list(args)
    for i in (10, 11, 12):
        flat[i] = args[i].reshape(1, HEADS)
    flat[6] = args[6].T
    flat[14] = jnp.swapaxes(args[14], 1, 2)
    hbm, vmem = pl.BlockSpec(memory_space=pl.ANY), pl.BlockSpec(memory_space=pltpu.VMEM)
    specs = [hbm] * len(flat)
    dma = pltpu.SemaphoreType.DMA
    cache, read = pl.pallas_call(
        lambda *refs: mixer_kernel(dims, *refs),
        out_shape=(
            pltpu.VMEM((S, RH, STATE), BF16),
            pltpu.VMEM((S, RH), BF16),
        ),
        in_specs=specs,
        out_specs=(vmem, vmem),
        scratch_shapes=[
            *[pltpu.VMEM(flat[i].shape, flat[i].dtype) for i in SMALL],
            pltpu.VMEM((S, L, D), BF16),
            pltpu.VMEM((S + 1, 16, D), BF16),
            pltpu.VMEM(((S + 1) * 16, C + STATE), F32),
            pltpu.VMEM((D, 128 + C + STATE), BF16),
            pltpu.VMEM((heads, D), BF16),
            pltpu.VMEM((D, F), BF16),
            pltpu.VMEM((S, heads, L), F32),
            pltpu.VMEM((CONV, C + STATE), F32),
            pltpu.VMEM((slots, G, 8 + L, C), F32),
            pltpu.VMEM((slots, G, 2 * heads, L), BF16),
            pltpu.VMEM((steps, halo_rows, C), BF16),
            pltpu.VMEM((steps, halo_rows, C), BF16),
            pltpu.VMEM((SP, C + STATE), F32),
            pltpu.VMEM((2, HEADS, 128), F32),
            pltpu.VMEM((S, heads, 128), F32),
            pltpu.VMEM((S, 1, 128), F32),
            pltpu.VMEM((S, 1, 128), F32),
            pltpu.VMEM((S, 1, 128), F32),
            pltpu.VMEM((S, n, RH, STATE), BF16),
            pltpu.VMEM((S, n, RH, STATE), BF16),
            pltpu.VMEM((S, n, RH, STATE), BF16),
            pltpu.VMEM((1, 128), F32),
            pltpu.VMEM((n * m - 1, 1, 128), F32),
            pltpu.VMEM((2 * heads, F), BF16),
            dma((16,)),
            dma((2, 2)),
            dma((2,)),
            dma((3, RING)),
            dma((2, S)),
            dma((2, steps)),
            dma((1,)),
            dma((steps,)),
            dma((2,)),
        ],
        compiler_params=pltpu.CompilerParams(
            collective_id=0, has_side_effects=True, vmem_limit_bytes=56 * 1024 * 1024
        ),
    )(*flat)
    cache, read = pl.pallas_call(
        lambda *refs: emit_kernel((heads, R), *refs),
        out_shape=(
            jax.ShapeDtypeStruct((S, RH, STATE), BF16),
            jax.ShapeDtypeStruct((S, heads, R), BF16),
        ),
        in_specs=[vmem, vmem],
        out_specs=(pl.BlockSpec(memory_space=pltpu.HBM),) * 2,
        scratch_shapes=[pltpu.VMEM((S, heads, R), BF16), dma((2,))],
    )(on_chip(cache), on_chip(read))
    return cache.reshape(S, heads, R, STATE), read


def fits(n, m, shapes):
    (S, L), F = shapes
    heads, R = F // P_SIZE, P_SIZE // n
    return (
        n > 1
        and F % 128 == 0
        and heads % 8 == 0
        and R % 16 == 0
        and (heads * R) % 128 == 0
        and S <= 16
        and L % 16 == 0
        and L == 128
        and (HEADS // GROUPS) % heads == 0
    )


def part(*args):
    shapes = (args[0].shape[:2], args[2].shape[1])
    if fits(lax.axis_size("sp"), lax.axis_size("tp"), shapes):
        return fused(*args)
    return shards(*args)


def solution(mesh):
    in_specs = (
        P("grp", "sp", None),
        P("grp", None),
        P(None, "tp"),
        P(None, "tp"),
        P(),
        P(),
        P(),
        P(),
        P(),
        P(),
        P(),
        P(),
        P(),
        P(),
        P("grp", "sp", None),
    )
    out_specs = (P("grp", "tp", "sp", None), P("grp", "tp", "sp"))
    return jax.shard_map(part, mesh=mesh, in_specs=in_specs, out_specs=out_specs, check_vma=False)
```
